32 devices in a mesh: ep: 8 (over z, core), tp: 4 (over y, x).
Axes of the slice: x: 2, y: 2, z: 4, core: 2. Of those that a mesh axis runs over, the one named last changes fastest.
Arguments:
- query_maps: bfloat16 [2048, 4096], P('ep', 'tp'), may hold values from -40 to 40
- key_maps: bfloat16 [2048, 4096], P('ep', 'tp'), may hold values from -40 to 40
- value_rows: bfloat16 [2048, 4096], P('ep', 'tp'), may hold values from -6 to 6
- head_lambda: float32 [16], P('tp'), may hold values from 0.3 to 0.8
- head_gain: float32 [256], replicated, may hold values from 0.1 to 1.9
- out_weight: bfloat16 [4096, 2048], P('tp'), may hold values from -0.125 to 0.125
- expert_rows: bfloat16 [1024, 2048], P('ep'), may hold values from -6 to 6
- expert_gain: float32 [2048], replicated, may hold values from 0.1 to 1.9
- routes: int32 [1024, 2], P('ep'), may hold values from 0 to 7, all different within a row; in each aligned block of 128 rows (0 to 127, 128 to 255, ...) at most 48 rows name the same one
- route_weights: float32 [1024, 2], P('ep'), may hold values from 0.2 to 1
- gate_weight: bfloat16 [8, 2048, 4096], P('ep', None, 'tp'), may hold values from -0.125 to 0.125
- up_weight: bfloat16 [8, 2048, 4096], P('ep', None, 'tp'), may hold values from -0.125 to 0.125
- down_weight: bfloat16 [8, 4096, 2048], P('ep', 'tp'), may hold values from -0.125 to 0.125
Outputs:
- mixed: bfloat16 [2048, 2048], P('ep', 'tp')
- expert_out: bfloat16 [1024, 2048], P('ep', 'tp')
The draws below stay inside these ranges and needn't reach their ends.
Inputs may be any that keep to these rules, and one draw needn't show every extreme that they name: `routes`: within the rows of one device (aligned blocks of 128 rows) no expert is named more than 48 times, and the 2 experts of a row differ.
All inputs are finite; a program needn't handle non-finite values.
Results may differ from the reference program's by a relative error of at most 0.018.
Values may be sent and summed in bfloat16 or wider, within the bound.
A program may use at most 128 MiB of HBM per device.

```python
import math
import jax
import jax.numpy as jnp
import numpy as np
from jax import lax

D = 2048
HEADS = 16
HEAD = 128
VHEAD = 256
FF = 4096
TOPK = 2
MOE_DEV = 128
TOKENS = 2048
MOE_TOK = 1024
EXPERTS = 8
CAP = 48
N_EP = 8
N_TP = 4


def draw_query_maps(key, part):
    base = jnp.clip(1.3 * jax.random.normal(jax.random.fold_in(key, 1), (TOKENS, HEADS * 2 * HEAD), jnp.float32), -7.8, 7.8)
    return base.astype(jnp.bfloat16)


def draw_key_maps(key, part):
    base = jnp.clip(1.3 * jax.random.normal(jax.random.fold_in(key, 2), (TOKENS, HEADS * 2 * HEAD), jnp.float32), -7.8, 7.8)
    base = base.reshape(TOKENS, HEADS, 2, HEAD)
    return base.reshape(TOKENS, HEADS * 2 * HEAD).astype(jnp.bfloat16)


def spiked(result, own_key, source, target, shards_of, factor):
    owner, partner = [(jnp.arange(result.shape[axis_at]) // (result.shape[axis_at] // shards_of)).reshape([-1 if axis == axis_at else 1 for axis in range(result.ndim)]) for axis_at in (source, target)]
    chosen = jax.random.permutation(own_key, shards_of)[partner]
    strong = (owner == chosen) | (owner == (partner + shards_of // 2) % shards_of)
    return jnp.where(strong, factor * result, result)


def level_of(stream_key, dims, cuts, low, top_value):
    loudness = 1.0
    for axis_at, blocks in cuts:
        steps = jax.random.uniform(jax.random.fold_in(jax.random.fold_in(stream_key, 6), axis_at), (blocks,), jnp.float32, low / len(cuts), top_value / len(cuts))
        loudness = loudness * jnp.repeat(jnp.exp(steps), dims[axis_at] // blocks).reshape((-1,) + (1,) * (len(dims) - 1 - axis_at))
    return loudness


def routed_block(stream_key, own, number, rows, amount, top, most, skew):
    order = jax.random.permutation(stream_key, amount)
    heavy_load, ordinary = load_shares(amount, rows * top, most, skew, True), load_shares(amount, rows * top, most, skew, False)
    places = jnp.arange(amount)

    def named(sizes, turn):
        used = int((sizes > 0).sum())
        fixed = max(1, used // 4)
        passed = fixed + (places - fixed + turn * (used - fixed)) % max(1, amount - fixed)
        return jnp.zeros((amount,), jnp.int32).at[order[jnp.where(places < fixed, places, passed)]].set(jnp.asarray(sizes, jnp.int32))

    sizes = jnp.where(number % 4 == 0, named(heavy_load, number // 4), named(ordinary, number - number // 4 - 1))
    mixed = jax.random.permutation(jax.random.fold_in(own, 3), amount)
    source_of, receiver = mixed[0:amount // 2 * 2:2], mixed[1:amount // 2 * 2:2]
    room = jnp.minimum(sizes[source_of] - 1, most - sizes[receiver]) // 2
    room = jnp.where((source_of == order[0]) | (receiver == order[0]) | (sizes[receiver] == 0), 0, jnp.maximum(room, 0))
    passed = jax.random.randint(jax.random.fold_in(own, 4), (amount // 2,), 0, 1 << 20) % (room + 1)
    sizes = sizes.at[source_of].add(-passed).at[receiver].add(passed)
    labels = jnp.searchsorted(jnp.cumsum(sizes), jnp.arange(rows * top), side="right").astype(jnp.int32)
    table = labels.reshape(top, rows).T
    table = table[jax.random.permutation(jax.random.fold_in(own, 1), rows)]
    turn = jax.random.randint(jax.random.fold_in(own, 2), (rows, 1), 0, top)
    return jnp.take_along_axis(table, (jnp.arange(top)[None, :] + turn) % top, axis=1)


def load_shares(number_of, total, bound, lean, full):
    portions = [(1 << 20) // math.isqrt(standing ** lean) + 1 for standing in range(1, number_of + 1)]
    largest = bound if full else min(bound, max(-(-total // number_of), total * portions[0] // sum(portions)))
    least = 1 if total - largest >= number_of - 1 else 0
    holding, surplus = [largest] + [least] * (number_of - 1), total - largest - least * (number_of - 1)
    while surplus > 0:
        free = [i for i in range(1, number_of) if holding[i] < largest] or [i for i in range(1, number_of) if holding[i] < bound]
        mass, budget = sum([portions[i] for i in free]), surplus
        for i in free:
            extra = min(bound - holding[i], max(1, budget * portions[i] // mass), surplus)
            holding[i] = holding[i] + extra
            surplus = surplus - extra
    return np.array(holding)


def centred(rng, extent, spread, bound, cuts=(), kind=jnp.bfloat16):
    array = spread * jax.random.normal(rng, extent, jnp.float32)
    if cuts:
        array = array * level_of(rng, extent, cuts, -0.22, 0.18)
    return jnp.clip(array, -bound, bound).astype(kind)


def heavy_noise(rng, extent, scale, most, split, heavy, kind=jnp.bfloat16):
    array = scale * jax.random.normal(rng, extent, jnp.float32)
    if split:
        array = array * level_of(rng, extent, split, -0.22, 0.18)
    return jnp.clip(spiked(array, jax.random.fold_in(rng, 3), *heavy), -most, most).astype(kind)


def setup_inputs(seed: int = 0) -> dict:
    key_list = jax.random.split(jax.random.key(seed), 14)
    query_maps = draw_query_maps(jax.random.fold_in(key_list[13], 71), 0)
    key_maps = draw_key_maps(jax.random.fold_in(key_list[13], 71), 0)
    value_rows = centred(key_list[2], (TOKENS, HEADS * VHEAD), 1.0, 6.0, ((0, 8), (1, 4)))
    head_lambda = jnp.clip(0.3 + 0.5 * jax.random.uniform(key_list[3], (HEADS,), jnp.float32) ** level_of(key_list[3], (HEADS,), ((0, 4),), -0.2, 0.2), 0.3, 0.8)
    head_gain = jnp.clip(1.0 + 0.18 * jax.random.normal(key_list[4], (VHEAD,), jnp.float32), 0.1, 1.9)
    out_weight = heavy_noise(key_list[5], (HEADS * VHEAD, D), (HEADS * VHEAD) ** -0.5, 0.125, ((0, 4),), (0, 1, 4, 2.0))
    expert_rows = centred(key_list[6], (MOE_TOK, D), 1.0, 6.0, ((0, 8),))
    expert_gain = jnp.clip(1.0 + 0.18 * jax.random.normal(key_list[7], (D,), jnp.float32), 0.1, 1.9)
    routes_keys = jax.random.split(jax.random.fold_in(key_list[8], 1), MOE_TOK // MOE_DEV)
    routes_turns = jax.random.permutation(jax.random.fold_in(key_list[8], 3), MOE_TOK // MOE_DEV)
    routes = jax.vmap(lambda own, number: routed_block(jax.random.fold_in(key_list[8], 2), own, number, MOE_DEV, EXPERTS, TOPK, CAP, 2))(routes_keys, routes_turns).reshape((MOE_TOK, TOPK))
    route_weights = jnp.clip(0.2 + 0.8 * jax.random.uniform(key_list[9], (MOE_TOK, TOPK), jnp.float32) ** level_of(key_list[9], (MOE_TOK, TOPK), ((0, 8),), -0.2, 0.2), 0.2, 1.0)
    gate_weight = centred(key_list[10], (EXPERTS, D, FF), D ** -0.5, 0.125, ((0, 8), (2, 4)))
    up_weight = centred(key_list[11], (EXPERTS, D, FF), D ** -0.5, 0.125, ((0, 8), (2, 4)))
    down_weight = heavy_noise(key_list[12], (EXPERTS, FF, D), FF ** -0.5, 0.125, ((0, 8), (1, 4)), (1, 2, 4, 2.0))
    return dict(query_maps=query_maps, key_maps=key_maps, value_rows=value_rows, head_lambda=head_lambda, head_gain=head_gain, out_weight=out_weight, expert_rows=expert_rows, expert_gain=expert_gain, routes=routes, route_weights=route_weights, gate_weight=gate_weight, up_weight=up_weight, down_weight=down_weight)


norm_eps = 1e-06
rope_base = 10000.0

def rope_turn(inputs, positions):
    half_dim = inputs.shape[-1] // 2
    inverse = rope_base ** (-2.0 * jnp.arange(half_dim, dtype=jnp.float32) / inputs.shape[-1])
    angles = positions.astype(jnp.float32)[:, None] * inverse[None, :]
    cos_table = jnp.cos(angles)[:, None, None, :]
    sin_table = jnp.sin(angles)[:, None, None, :]
    first_half = inputs[..., :half_dim]
    second_half = inputs[..., half_dim:]
    return jnp.concatenate([first_half * cos_table - second_half * sin_table, second_half * cos_table + first_half * sin_table], axis=-1)

def mixer_half(query_maps, key_maps, value_rows, head_lambda, head_gain, out_weight):
    positions = jnp.arange(TOKENS, dtype=jnp.int32)
    rotated_q = rope_turn(query_maps.astype(jnp.float32).reshape(TOKENS, HEADS, 2, HEAD), positions).astype(jnp.bfloat16)
    rotated_k = rope_turn(key_maps.astype(jnp.float32).reshape(TOKENS, HEADS, 2, HEAD), positions).astype(jnp.bfloat16)
    values_all = value_rows.reshape(TOKENS, HEADS, VHEAD)
    block_size = math.gcd(512, TOKENS)
    score_scale = HEAD ** (-0.5)

    def one_head(head_index):
        head_q = rotated_q[:, head_index].astype(jnp.float32)
        head_k = rotated_k[:, head_index].astype(jnp.float32)
        head_v = values_all[:, head_index].astype(jnp.float32)
        key_pos = jnp.arange(TOKENS, dtype=jnp.int32)

        def one_block(block_index):
            first_row = (block_index * block_size).astype(jnp.int32)
            block_q = lax.dynamic_slice_in_dim(head_q, first_row, block_size, 0)
            query_pos = first_row + jnp.arange(block_size, dtype=jnp.int32)
            scores = jnp.einsum('qmd,kmd->mqk', block_q, head_k) * score_scale
            causal = (key_pos[None, :] <= query_pos[:, None])[None]
            masked = jnp.where(causal, scores, -jnp.inf)
            peak = lax.optimization_barrier(jnp.max(masked, axis=-1, keepdims=True))
            expd = jnp.where(causal, jnp.exp(masked - peak), 0.0)
            probs = expd / lax.optimization_barrier(jnp.sum(expd, axis=-1, keepdims=True))
            rounded = lax.optimization_barrier(probs.astype(jnp.bfloat16))
            map_out = jnp.einsum('mqk,ke->mqe', rounded.astype(jnp.float32), head_v)
            difference = map_out[0] - head_lambda[head_index] * map_out[1]
            normed = difference * lax.rsqrt(lax.optimization_barrier(jnp.mean(difference * difference, axis=-1, keepdims=True)) + norm_eps) * head_gain
            return normed.astype(jnp.bfloat16)
        blocks = lax.map(one_block, jnp.arange(TOKENS // block_size, dtype=jnp.int32))
        return blocks.reshape(TOKENS, VHEAD)
    per_head = lax.map(one_head, jnp.arange(HEADS, dtype=jnp.int32))
    group_size = HEADS // N_TP
    grouped = per_head.reshape(N_TP, group_size, TOKENS, VHEAD)
    weight_groups = out_weight.reshape(N_TP, group_size, VHEAD, D)

    def add_group(running, pieces):
        group_heads, group_weight = pieces
        partial_value = jnp.einsum('hte,hed->td', group_heads.astype(jnp.float32), group_weight.astype(jnp.float32))
        rounded = lax.optimization_barrier(partial_value.astype(jnp.bfloat16))
        return (running + rounded.astype(jnp.float32), None)
    summed, _ = lax.scan(add_group, jnp.zeros((TOKENS, D), jnp.float32), (grouped, weight_groups))
    return summed.astype(jnp.bfloat16)

def expert_half(expert_rows, expert_gain, routes, route_weights, gate_weight, up_weight, down_weight):
    inputs = expert_rows.astype(jnp.float32)
    normed = (inputs * lax.rsqrt(lax.optimization_barrier(jnp.mean(inputs * inputs, axis=-1, keepdims=True)) + norm_eps) * expert_gain).astype(jnp.bfloat16)
    expert_ids = routes.reshape(N_EP, MOE_DEV * TOPK)
    one_hot = (expert_ids[..., None] == jnp.arange(EXPERTS, dtype=jnp.int32)).astype(jnp.int32)
    slot_index = lax.optimization_barrier(jnp.sum((jnp.cumsum(one_hot, axis=1) - one_hot) * one_hot, axis=-1)).astype(jnp.int32)
    source_block = jnp.zeros_like(expert_ids) + jnp.arange(N_EP, dtype=jnp.int32)[:, None]
    repeated = jnp.repeat(normed.reshape(N_EP, MOE_DEV, D), TOPK, axis=1)
    buffer = jnp.zeros((EXPERTS, N_EP, CAP, D), normed.dtype).at[expert_ids, source_block, slot_index].set(repeated)
    group_width = FF // N_TP

    def run_one(pieces):
        slots, gate_one, up_one, down_one = pieces
        flat_rows = slots.reshape(N_EP * CAP, D)
        gate_values = jnp.dot(flat_rows, gate_one, preferred_element_type=jnp.float32)
        up_values = jnp.dot(flat_rows, up_one, preferred_element_type=jnp.float32)
        hidden = (jax.nn.silu(gate_values) * up_values).astype(jnp.bfloat16)
        hidden_groups = jnp.transpose(hidden.reshape(N_EP * CAP, N_TP, group_width), (1, 0, 2))
        down_groups = down_one.reshape(N_TP, group_width, D)

        def add_group(running, pieces_inner):
            hidden_part, down_part = pieces_inner
            partial_value = jnp.dot(hidden_part, down_part, preferred_element_type=jnp.float32)
            rounded = lax.optimization_barrier(partial_value.astype(jnp.bfloat16))
            return (running + rounded.astype(jnp.float32), None)
        summed, _ = lax.scan(add_group, jnp.zeros((N_EP * CAP, D), jnp.float32), (hidden_groups, down_groups))
        return summed.astype(jnp.bfloat16).reshape(N_EP, CAP, D)
    results = lax.map(run_one, (buffer, gate_weight, up_weight, down_weight))
    picked = results[expert_ids, source_block, slot_index].reshape(MOE_TOK, TOPK, D)
    combined = lax.optimization_barrier(jnp.sum(route_weights[..., None] * picked.astype(jnp.float32), axis=1))
    return combined.astype(jnp.bfloat16)

def reference(query_maps, key_maps, value_rows, head_lambda, head_gain, out_weight, expert_rows, expert_gain, routes, route_weights, gate_weight, up_weight, down_weight):
    mixed = mixer_half(query_maps, key_maps, value_rows, head_lambda, head_gain, out_weight)
    expert_out = expert_half(expert_rows, expert_gain, routes, route_weights, gate_weight, up_weight, down_weight)
    return (mixed, expert_out)
```

```python
import functools

import jax
import jax.numpy as jnp
from jax import lax
from jax.experimental import pallas as pl
from jax.experimental.pallas import tpu as pltpu
from jax.sharding import PartitionSpec as P

norm_eps = 1e-06
rope_base = 10000.0


def rope_turn(inputs, positions):
    half_dim = inputs.shape[-1] // 2
    inverse = rope_base ** (-2.0 * jnp.arange(half_dim, dtype=jnp.float32) / inputs.shape[-1])
    angles = positions.astype(jnp.float32)[:, None] * inverse[None, :]
    cos_table = jnp.cos(angles)[:, None, None, :]
    sin_table = jnp.sin(angles)[:, None, None, :]
    first_half = inputs[..., :half_dim]
    second_half = inputs[..., half_dim:]
    return jnp.concatenate(
        [
            first_half * cos_table - second_half * sin_table,
            second_half * cos_table + first_half * sin_table,
        ],
        axis=-1,
    )


def mixer_half(query_maps, key_maps, value_rows, head_lambda, head_gain, out_weight):
    row_count = query_maps.shape[0]
    head_count = head_lambda.shape[0]
    head_dim = query_maps.shape[1] // (2 * head_count)
    value_dim = value_rows.shape[1] // head_count
    model_width = out_weight.shape[1]
    score_scale = head_dim ** (-0.5)
    offset = lax.axis_index("ep") * row_count
    positions = offset + jnp.arange(row_count, dtype=jnp.int32)
    last_row = offset + row_count - 1
    rotated_q = rope_turn(
        query_maps.astype(jnp.float32).reshape(row_count, head_count, 2, head_dim), positions
    ).astype(jnp.bfloat16)
    rotated_k = rope_turn(
        key_maps.astype(jnp.float32).reshape(row_count, head_count, 2, head_dim), positions
    ).astype(jnp.bfloat16)
    rotated_k = rotated_k.reshape(row_count, head_count * 2 * head_dim)
    initial = (
        jnp.full((head_count, 2, row_count), -1e30, jnp.float32),
        jnp.zeros((head_count, 2, row_count), jnp.float32),
        jnp.zeros((head_count, 2, row_count, value_dim), jnp.float32),
    )
    piece_k = lax.all_gather(rotated_k, "ep", axis=0, tiled=True)
    piece_v = lax.all_gather(value_rows, "ep", axis=0, tiled=True)
    piece_len = piece_k.shape[0]
    block_size = 1024

    def attend(state):

        def fold_step(inner, block_index):
            block_start = block_index * block_size
            block_k = lax.dynamic_slice_in_dim(piece_k, block_start, block_size, 0).reshape(
                block_size, head_count, 2, head_dim
            )
            block_v = lax.dynamic_slice_in_dim(piece_v, block_start, block_size, 0).reshape(
                block_size, head_count, value_dim
            )
            scores = (
                jnp.einsum(
                    "qhmd,khmd->hmqk", rotated_q, block_k, preferred_element_type=jnp.float32
                )
                * score_scale
            )
            key_pos = block_start + jnp.arange(block_size, dtype=jnp.int32)
            causal = key_pos[None, :] <= positions[:, None]
            masked = jnp.where(causal, scores, -1e30)
            run_max, run_sum, run_acc = inner
            new_max = jnp.maximum(run_max, jnp.max(masked, axis=-1))
            expd = jnp.where(causal, jnp.exp(masked - new_max[..., None]), 0.0)
            rescale = jnp.exp(run_max - new_max)
            new_sum = run_sum * rescale + jnp.sum(expd, axis=-1)
            new_acc = run_acc * rescale[..., None] + jnp.einsum(
                "hmqk,khe->hmqe",
                expd.astype(jnp.bfloat16),
                block_v,
                preferred_element_type=jnp.float32,
            )
            return ((new_max, new_sum, new_acc), None)

        result, _ = lax.scan(fold_step, state, jnp.arange(piece_len // block_size, dtype=jnp.int32))
        return result

    def skip_piece(state):
        return state

    run_max, run_sum, run_acc = lax.cond(jnp.int32(0) <= last_row, attend, skip_piece, initial)
    first_map = run_acc[:, 0] / run_sum[:, 0][..., None]
    second_map = run_acc[:, 1] / run_sum[:, 1][..., None]
    difference = first_map - head_lambda[:, None, None] * second_map
    head_out = (
        difference
        * lax.rsqrt(jnp.mean(difference * difference, axis=-1, keepdims=True) + norm_eps)
        * head_gain
    ).astype(jnp.bfloat16)
    partial_value = jnp.einsum(
        "hqe,hed->qd",
        head_out,
        out_weight.reshape(head_count, value_dim, model_width),
        preferred_element_type=jnp.float32,
    )
    return lax.psum_scatter(
        partial_value.astype(jnp.bfloat16), "tp", scatter_dimension=1, tiled=True
    )


def expert_half(
    expert_rows, expert_gain, routes, route_weights, gate_weight, up_weight, down_weight
):
    ep_count = lax.axis_size("ep")
    tp_count = lax.axis_size("tp")
    row_count, model_width = expert_rows.shape
    pick_count = routes.shape[1]
    capacity = 3 * row_count * pick_count // (2 * ep_count)
    column_count = model_width // tp_count
    inputs = expert_rows.astype(jnp.float32)
    normed = (
        inputs
        * lax.rsqrt(jnp.mean(inputs * inputs, axis=-1, keepdims=True) + norm_eps)
        * expert_gain
    ).astype(jnp.bfloat16)
    expert_ids = routes.reshape(-1)
    one_hot = (expert_ids[:, None] == jnp.arange(ep_count, dtype=jnp.int32)[None, :]).astype(
        jnp.int32
    )
    slot_index = jnp.sum((jnp.cumsum(one_hot, axis=0) - one_hot) * one_hot, axis=1)
    source_row = jnp.arange(row_count * pick_count, dtype=jnp.int32) // pick_count
    empty = jnp.zeros((ep_count, capacity, normed.shape[1]), jnp.bfloat16)
    arrived = lax.all_to_all(
        empty.at[expert_ids, slot_index].set(normed[source_row]),
        "ep",
        split_axis=0,
        concat_axis=0,
        tiled=True,
    )
    slot_count = arrived.shape[1]
    flat_rows = arrived.reshape(ep_count * slot_count, model_width)
    gate_values = jnp.dot(flat_rows, gate_weight[0], preferred_element_type=jnp.float32)
    up_values = jnp.dot(flat_rows, up_weight[0], preferred_element_type=jnp.float32)
    hidden = (jax.nn.silu(gate_values) * up_values).astype(jnp.bfloat16)
    partial_value = jnp.dot(hidden, down_weight[0], preferred_element_type=jnp.float32).reshape(
        ep_count, slot_count, model_width
    )
    summed = lax.psum_scatter(
        partial_value.astype(jnp.bfloat16), "tp", scatter_dimension=2, tiled=True
    )
    returned = lax.all_to_all(summed, "ep", split_axis=0, concat_axis=0, tiled=True)
    picked = returned[expert_ids, slot_index].reshape(row_count, pick_count, column_count)
    combined = jnp.sum(route_weights[..., None] * picked.astype(jnp.float32), axis=1)
    return combined.astype(jnp.bfloat16)


MESH = pl.DeviceIdType.MESH


def remote(source, target, send_sem, recv_sem, device):
    return pltpu.make_async_remote_copy(
        src_ref=source,
        dst_ref=target,
        send_sem=send_sem,
        recv_sem=recv_sem,
        device_id=device,
        device_id_type=MESH,
    )


def layer_kernel(
    n_ep,
    n_tp,
    rows_ref,
    norm_gain_ref,
    routes_ref,
    route_weights_ref,
    query_ref,
    key_ref,
    value_ref,
    cos_ref,
    sin_ref,
    lambda_ref,
    gain_ref,
    gate_hbm,
    up_hbm,
    down_hbm,
    weight_hbm,
    expert_ref,
    mixed_ref,
    slots_ref,
    packed_q,
    packed_kv,
    own_q,
    own_kv,
    below_kv,
    lower_kv,
    upper_q,
    own_stat,
    upper_stat,
    low_stat,
    back_stat,
    own_maps,
    own_part,
    own_diff,
    low_part,
    low_diff,
    gathered,
    gate_vmem,
    up_vmem,
    down_vmem,
    hidden,
    partial,
    arrived,
    summed,
    returned,
    weight_vmem,
    heads,
    mixed_partial,
    mixed_arrived,
    weight_sem,
    local_sem,
    disp_send,
    disp_recv,
    gath_send,
    gath_recv,
    part_send,
    part_recv,
    ret_send,
    ret_recv,
    swap_send,
    swap_recv,
    below_send,
    below_recv,
    lower_send,
    lower_recv,
    upper_send,
    upper_recv,
    stat_send,
    stat_recv,
    back_send,
    back_recv,
    diff_send,
    diff_recv,
    cross_send,
    cross_recv,
    mixed_send,
    mixed_recv,
):
    ep = lax.axis_index("ep")
    tp = lax.axis_index("tp")
    n_z = n_ep // 2
    middle = n_z // 2
    z, core = ep // 2, lax.rem(ep, 2)
    odd = lax.rem(z, 2)
    asks = [z >= middle, odd == 1]
    host = [middle - 1, z - 1]
    seat = [lax.rem(z, middle), 0]
    partner = {"ep": ep + 1 - 2 * core}
    capacity, width = slots_ref.shape[1:]
    rows = n_ep * capacity
    head_count, row_count, head_width = packed_q.shape
    share = head_count // 2
    half = head_width // 2
    first = core * share
    weights = [
        pltpu.make_async_copy(gate_hbm, gate_vmem, weight_sem.at[0]),
        pltpu.make_async_copy(up_hbm, up_vmem, weight_sem.at[1]),
        pltpu.make_async_copy(down_hbm, down_vmem, weight_sem.at[2]),
        pltpu.make_async_copy(weight_hbm, weight_vmem, weight_sem.at[3]),
    ]
    for copy in weights:
        copy.start()
    peers = [{"ep": lax.rem(ep + d, n_ep)} for d in range(1, n_ep)]
    peers += [{"tp": lax.rem(tp + d, n_tp)} for d in range(1, n_tp)]
    barrier = pltpu.get_barrier_semaphore()
    for device in peers:
        pl.semaphore_signal(barrier, inc=1, device_id=device, device_id_type=MESH)

    token_count = rows_ref.shape[0]
    picks = routes_ref.shape[0]
    entries = rows_ref[...].astype(jnp.float32)
    inverse_norm = lax.rsqrt(jnp.mean(entries * entries, axis=1, keepdims=True) + norm_eps)
    own = pl.ds(pl.multiple_of(tp * width, width), width)
    normed = rows_ref[:, own].astype(jnp.float32) * inverse_norm * norm_gain_ref[:, own]
    normed = normed.astype(jnp.bfloat16)
    named_rows = -(-n_ep // 16) * 16
    label = lax.broadcasted_iota(jnp.int32, (named_rows, token_count), 0)
    named = [
        jnp.where(label == routes_ref[k : k + 1, :], 1.0, 0.0).astype(jnp.float32)
        for k in range(picks)
    ]
    before = lax.broadcasted_iota(jnp.int32, (token_count, token_count), 0)
    after = lax.broadcasted_iota(jnp.int32, (token_count, token_count), 1)
    earlier = jnp.dot(
        sum(named).astype(jnp.bfloat16),
        jnp.where(before < after, 1.0, 0.0).astype(jnp.bfloat16),
        preferred_element_type=jnp.float32,
    )
    slot_of = lax.broadcasted_iota(jnp.int32, (rows, token_count), 0)
    select = []
    for k in range(picks):
        rank = jnp.sum(named[k] * earlier, axis=0, keepdims=True).astype(jnp.int32)
        place = routes_ref[k : k + 1, :] * capacity + rank
        select.append(jnp.where(slot_of == place, 1.0, 0.0).astype(jnp.float32))
    slots_ref[...] = (
        jnp.dot(
            sum(select).astype(jnp.bfloat16), normed, preferred_element_type=jnp.float32
        )
        .astype(jnp.bfloat16)
        .reshape(n_ep, capacity, width)
    )
    with jax.named_scope("barrier"):
        pl.semaphore_wait(barrier, len(peers))
    mine = tp * n_ep + ep
    dispatch = [pltpu.make_async_copy(slots_ref.at[ep], gathered.at[mine], local_sem.at[0])]
    for d in range(1, n_ep):
        target = lax.rem(ep + d, n_ep)
        dispatch.append(
            remote(
                slots_ref.at[target],
                gathered.at[mine],
                disp_send.at[d],
                disp_recv.at[d],
                {"ep": target},
            )
        )
    for copy in dispatch:
        copy.start()

    for head in range(head_count):
        for m in range(2):
            at = head * head_width + m * half
            to = slice(m * half, (m + 1) * half)
            for ref, packed in ((query_ref, packed_q), (key_ref, packed_kv)):
                entry = ref[:, at : at + half].astype(jnp.float32)
                turned = entry * cos_ref[...] + pltpu.roll(entry, half // 2, 1) * sin_ref[...]
                packed[head, :, to] = turned.astype(jnp.bfloat16)
        packed_kv[head, :, head_width:] = value_ref[
            :, head * head_width : (head + 1) * head_width
        ]
    other = share - first
    swaps = []
    for j in range(share):
        swaps += [
            remote(
                packed_q.at[other + j],
                own_q.at[j, core],
                swap_send.at[0, j],
                swap_recv.at[0, j],
                partner,
            ),
            remote(
                packed_kv.at[other + j],
                own_kv.at[j, core],
                swap_send.at[1, j],
                swap_recv.at[1, j],
                partner,
            ),
        ]
    keeps = []
    for j in range(share):
        keeps += [
            pltpu.make_async_copy(packed_q.at[first + j], own_q.at[j, core], local_sem.at[3 + j]),
            pltpu.make_async_copy(
                packed_kv.at[first + j], own_kv.at[j, core], local_sem.at[3 + share + j]
            ),
        ]
    for copy in swaps + keeps:
        copy.start()

    def lift(side):
        return remote(
            packed_kv.at[side * share],
            below_kv.at[0, core],
            below_send.at[side],
            below_recv.at[core],
            {"ep": lax.rem(ep - core + 2 + side, n_ep)},
        )

    def lift_far(side):
        return remote(
            packed_kv.at[side * share + 1],
            lower_kv.at[0, 2 * lax.rem(z, middle) + core],
            lower_send.at[side],
            lower_recv.at[2 * lax.rem(z, middle) + core],
            {"ep": 2 * middle + side},
        )

    def ask(side, j):
        return remote(
            packed_q.at[side * share + j],
            upper_q.at[seat[j], core],
            upper_send.at[side, j],
            upper_recv.at[seat[j], core],
            {"ep": 2 * host[j] + side},
        )

    def wait_landed(ref, sem):
        pltpu.make_async_copy(ref, ref, sem).wait()

    spread = []
    with jax.named_scope("wait_disp"):
        for d in range(n_ep):
            source = lax.rem(ep + n_ep - d, n_ep)
            if d == 0:
                dispatch[0].wait()
            else:
                dispatch[d].wait_recv()
            slot = gathered.at[tp * n_ep + source]
            for t in range(1, n_tp):
                copy = remote(
                    slot,
                    slot,
                    gath_send.at[d * n_tp + t],
                    gath_recv.at[d * n_tp + t],
                    {"tp": lax.rem(tp + t, n_tp)},
                )
                copy.start()
                spread.append(copy)

    for j in range(share):
        for side in range(2):

            @pl.when(asks[j])
            def _():
                ask(side, j).start()

    for side in range(2):

        @pl.when(odd == 0)
        def _():
            lift(side).start()

    for side in range(2):

        @pl.when(z < middle)
        def _():
            lift_far(side).start()

    row = lax.broadcasted_iota(jnp.int32, (row_count, row_count), 0)
    column = lax.broadcasted_iota(jnp.int32, (row_count, row_count), 1)
    causal = column <= row
    wide = lax.broadcasted_iota(jnp.int32, (row_count, 2 * row_count), 0) + row_count
    wide_causal = lax.broadcasted_iota(jnp.int32, (row_count, 2 * row_count), 1) <= wide
    diagonal = column == row
    scale = half ** (-0.5)
    stat_row = lax.broadcasted_iota(jnp.int32, (8, row_count), 0)

    def as_column(values):
        return jnp.sum(jnp.where(diagonal, values, 0.0), axis=1, keepdims=True)

    def as_row(values):
        return jnp.sum(jnp.where(diagonal, values, 0.0), axis=0, keepdims=True)

    def as_stats(levels):
        return jnp.where(stat_row == 0, as_row(levels[0]), as_row(levels[1]))

    def head_weight(j):
        lanes = lax.broadcasted_iota(jnp.int32, lambda_ref.shape, 1)
        return jnp.sum(
            jnp.where(lanes == first + j, lambda_ref[...], 0.0), axis=1, keepdims=True
        )

    def fold(query_of, pieces, m):
        scores = []
        for keys_of, values_of, mask in pieces:
            piece = lax.dot_general(
                query_of(m), keys_of(m), (((1,), (1,)), ((), ())), preferred_element_type=jnp.float32
            )
            piece = piece * scale
            if mask is not None:
                piece = jnp.where(mask, piece, -1e30)
            scores.append(piece)
        peak = functools.reduce(
            jnp.maximum, [jnp.max(piece, axis=1, keepdims=True) for piece in scores]
        )
        total = jnp.zeros((row_count, 1), jnp.float32)
        outcome = jnp.zeros((row_count, head_width), jnp.float32)
        for piece, (keys_of, values_of, mask) in zip(scores, pieces):
            expd = jnp.exp(piece - peak)
            total += jnp.sum(expd, axis=1, keepdims=True)
            outcome += jnp.dot(
                expd.astype(jnp.bfloat16), values_of(), preferred_element_type=jnp.float32
            )
        return peak, total, outcome

    def piece_of(ref, j, count, mask):
        def keys_of(m):
            keys = ref[j, :count, :, m * half : (m + 1) * half]
            return keys.reshape(count * row_count, half)

        def values_of():
            return ref[j, :count, :, head_width:].reshape(count * row_count, head_width)

        return keys_of, values_of, mask

    def keep_diff(j, block, difference):
        @pl.when(core == block)
        def _():
            own_diff[first + j] = difference.astype(jnp.bfloat16)

        @pl.when(core != block)
        def _():
            own_part[j] = difference.astype(jnp.bfloat16)
            send_diff(j).start()

    def send_diff(j):
        return remote(
            own_part.at[j], own_diff.at[first + j], diff_send.at[j], diff_recv.at[first + j], partner
        )

    def send_stat(j):
        return remote(
            own_stat.at[j],
            upper_stat.at[seat[j]],
            stat_send.at[j],
            stat_recv.at[seat[j]],
            {"ep": 2 * host[j] + core},
        )

    def local_head(j, pieces):
        swaps[2 * j].wait_recv()
        swaps[2 * j + 1].wait_recv()
        keeps[2 * j].wait()
        keeps[2 * j + 1].wait()
        for block in range(2):
            mask = wide_causal if block else causal
            parts = pieces + [piece_of(own_kv, j, block + 1, mask)]
            maps, levels = [], []
            for m in range(2):
                peak, total, outcome = fold(
                    lambda m: own_q[j, block, :, m * half : (m + 1) * half], parts, m
                )
                maps.append(outcome / total)
                levels.append(peak + jnp.log(total))

            @pl.when(asks[j])
            def _():
                own_maps[j, block, 0] = maps[0]
                own_maps[j, block, 1] = maps[1]
                own_stat[j, block] = as_stats(levels)

            @pl.when(jnp.logical_not(asks[j]))
            def _():
                keep_diff(j, block, maps[0] - head_weight(j) * maps[1])

        @pl.when(asks[j])
        def _():
            send_stat(j).start()

    def send_cross(up, j, block, target):
        return remote(
            low_part.at[up, block],
            low_diff.at[first + j],
            cross_send.at[up, block],
            cross_recv.at[first + j],
            {"ep": 2 * target + block},
        )

    def send_back(up, j, block, target):
        return remote(
            low_stat.at[up, block],
            back_stat.at[j, block],
            back_send.at[up, block],
            back_recv.at[j, block],
            {"ep": 2 * target + core},
        )

    def cross_head(j, count, base, pieces):
        def step(index, carry):
            up, block = index // 2, lax.rem(index, 2)
            target = base + up
            wait_landed(upper_q.at[up, block], upper_recv.at[up, block])

            @pl.when(block == 0)
            def _():
                wait_landed(upper_stat.at[up], stat_recv.at[up])

            maps, levels = [], []
            for m in range(2):
                peak, total, outcome = fold(
                    lambda m: upper_q[up, block, :, m * half : (m + 1) * half], pieces, m
                )
                level = peak + jnp.log(total)
                above = as_column(upper_stat[up, block, m : m + 1, :])
                whole = jnp.maximum(level, above) + jnp.log(1.0 + jnp.exp(-jnp.abs(level - above)))
                maps.append(outcome * jnp.exp(peak - whole))
                levels.append(level)
            low_stat[up, block] = as_stats(levels)
            send_back(up, j, block, target).start()
            low_part[up, block] = (maps[0] - head_weight(j) * maps[1]).astype(jnp.bfloat16)
            send_cross(up, j, block, target).start()
            return carry

        lax.fori_loop(0, 2 * count, step, 0)

    def finish_upper(j):
        for block in range(2):
            wait_landed(back_stat.at[j, block], back_recv.at[j, block])
            maps = []
            for m in range(2):
                below = as_column(back_stat[j, block, m : m + 1, :])
                level = as_column(own_stat[j, block, m : m + 1, :])
                maps.append(own_maps[j, block, m] / (1.0 + jnp.exp(below - level)))
            keep_diff(j, block, maps[0] - head_weight(j) * maps[1])

    below_piece = piece_of(below_kv, 0, 2, None)
    lower_piece = piece_of(lower_kv, 0, 2 * middle, None)

    @pl.when(z != middle)
    def _():
        with jax.named_scope("own1"):
            local_head(1, [])

    @pl.when(odd == 0)
    def _():
        with jax.named_scope("own0"):
            local_head(0, [])

    with jax.named_scope("wait_gath"):
        for copy in spread:
            copy.wait_recv()
    weights[0].wait()
    weights[1].wait()
    tile = 256

    def hidden_tile(j, carry):
        columns = pl.ds(pl.multiple_of(j * tile, tile), tile)
        gate = jnp.zeros((rows, tile), jnp.float32)
        up = jnp.zeros((rows, tile), jnp.float32)
        for i in range(n_tp):
            block = gathered[i * n_ep : (i + 1) * n_ep].reshape(rows, width)
            gate += jnp.dot(
                block,
                gate_vmem[0, i * width : (i + 1) * width, columns],
                preferred_element_type=jnp.float32,
            )
            up += jnp.dot(
                block,
                up_vmem[0, i * width : (i + 1) * width, columns],
                preferred_element_type=jnp.float32,
            )
        hidden[:, columns] = (gate / (1.0 + jnp.exp(-gate)) * up).astype(jnp.bfloat16)
        return carry

    with jax.named_scope("gateup"):
        lax.fori_loop(0, hidden.shape[1] // tile, hidden_tile, 0)
    weights[2].wait()
    scatter = []
    with jax.named_scope("down"):
        for d in list(range(1, n_tp)) + [0]:
            target = lax.rem(tp + d, n_tp)
            columns = pl.ds(pl.multiple_of(target * width, width), width)
            partial[d] = jnp.dot(
                hidden[...], down_vmem[0, :, columns], preferred_element_type=jnp.float32
            ).astype(jnp.bfloat16)
            if d:
                copy = remote(
                    partial.at[d], arrived.at[d], part_send.at[d], part_recv.at[d], {"tp": target}
                )
                copy.start()
                scatter.append(copy)

    @pl.when(odd == 1)
    def _():
        with jax.named_scope("odd0"):
            for source in range(2):
                wait_landed(below_kv.at[0, source], below_recv.at[source])
            local_head(0, [below_piece])

    @pl.when(z == 0)
    def _():
        with jax.named_scope("cross0"):
            cross_head(1, 1, 1, [piece_of(own_kv, 1, 2, None)])

    @pl.when(z == middle - 1)
    def _():
        with jax.named_scope("cross1"):
            cross_head(0, middle, middle, [below_piece, piece_of(own_kv, 0, 2, None)])

    @pl.when(z == middle)
    def _():
        with jax.named_scope("cross2"):
            for source in range(2 * middle):
                wait_landed(lower_kv.at[0, source], lower_recv.at[source])
            local_head(1, [lower_piece])
            cross_head(1, 1, middle + 1, [lower_piece, piece_of(own_kv, 1, 2, None)])

    for j in range(share):

        @pl.when(asks[j])
        def _():
            with jax.named_scope("finish"):
                finish_upper(j)

        @pl.when(jnp.logical_not(asks[j]))
        def _():
            for side in range(2):
                low_diff[side * share + j] = jnp.zeros((row_count, head_width), jnp.bfloat16)

    total = partial[0].astype(jnp.float32)
    with jax.named_scope("wait_part"):
        for d in range(1, n_tp):
            scatter[d - 1].wait_recv()
            total += arrived[d].astype(jnp.float32)
    summed[...] = total.astype(jnp.bfloat16).reshape(n_ep, capacity, width)
    back = [pltpu.make_async_copy(summed.at[ep], returned.at[ep], local_sem.at[2])]
    for d in range(1, n_ep):
        target = lax.rem(ep + d, n_ep)
        back.append(
            remote(
                summed.at[target],
                returned.at[ep],
                ret_send.at[d],
                ret_recv.at[d],
                {"ep": target},
            )
        )
    for copy in back:
        copy.start()

    with jax.named_scope("wait_heads"):
        for j in range(share):
            wait_landed(own_diff.at[other + j], diff_recv.at[other + j])

        for j in range(share):

            @pl.when(asks[j])
            def _():
                for side in range(2):
                    at = side * share + j
                    wait_landed(low_diff.at[at], cross_recv.at[at])

    for head in range(head_count):
        difference = own_diff[head].astype(jnp.float32) + low_diff[head].astype(jnp.float32)
        mean = jnp.mean(difference * difference, axis=1, keepdims=True)
        heads[head] = (difference * lax.rsqrt(mean + norm_eps) * gain_ref[...]).astype(
            jnp.bfloat16
        )
    weights[3].wait()
    mixed_scatter = []
    for d in list(range(1, n_tp)) + [0]:
        target = lax.rem(tp + d, n_tp)
        columns = pl.ds(pl.multiple_of(target * width, width), width)
        product = jnp.zeros((row_count, width), jnp.float32)
        for h in range(head_count):
            product += jnp.dot(
                heads[h],
                weight_vmem[h * head_width : (h + 1) * head_width, columns],
                preferred_element_type=jnp.float32,
            )
        mixed_partial[d] = product.astype(jnp.bfloat16)
        if d:
            copy = remote(
                mixed_partial.at[d], mixed_arrived.at[d], mixed_send.at[d], mixed_recv.at[d], {"tp": target}
            )
            copy.start()
            mixed_scatter.append(copy)
    with jax.named_scope("wait_back"):
        back[0].wait()
        for copy in back[1:]:
            copy.wait_recv()
    flat = returned[...].reshape(rows, width)
    result = jnp.zeros(expert_ref.shape, jnp.float32)
    for k in range(picks):
        picked = lax.dot_general(
            select[k].astype(jnp.bfloat16),
            flat,
            (((0,), (0,)), ((), ())),
            preferred_element_type=jnp.float32,
        )
        spread_out = jnp.where(before == after, route_weights_ref[k : k + 1, :], 0.0)
        result += jnp.sum(spread_out, axis=1, keepdims=True) * picked
    expert_ref[...] = result.astype(expert_ref.dtype)
    total = mixed_partial[0].astype(jnp.float32)
    with jax.named_scope("wait_mixed"):
        for d in range(1, n_tp):
            mixed_scatter[d - 1].wait_recv()
            total += mixed_arrived[d].astype(jnp.float32)
    mixed_ref[...] = total.astype(jnp.bfloat16)
    for copy in dispatch[1:] + swaps + spread + scatter + back[1:] + mixed_scatter:
        copy.wait_send()
    for j in range(share):
        send_diff(j).wait_send()

        @pl.when(asks[j])
        def _():
            send_stat(j).wait_send()
            for side in range(2):
                ask(side, j).wait_send()

    for side in range(2):

        @pl.when(odd == 0)
        def _():
            lift(side).wait_send()

        @pl.when(z < middle)
        def _():
            lift_far(side).wait_send()

        @pl.when(z <= middle)
        def _():
            send_cross(0, 0, side, z + 1).wait_send()
            send_back(0, 0, side, z + 1).wait_send()

        @pl.when(z == middle - 1)
        def _():
            send_cross(1, 0, side, z + 2).wait_send()
            send_back(1, 0, side, z + 2).wait_send()


def fused(
    query_maps,
    key_maps,
    value_rows,
    head_lambda,
    head_gain,
    out_weight,
    expert_rows,
    expert_gain,
    routes,
    route_weights,
    gate_weight,
    up_weight,
    down_weight,
):
    n_ep = lax.axis_size("ep")
    n_tp = lax.axis_size("tp")
    n_z = n_ep // 2
    ep = lax.axis_index("ep")
    row_count = query_maps.shape[0]
    head_width = query_maps.shape[1] // n_z
    head_dim = head_width // 2
    token_count, model_width = expert_rows.shape
    capacity = 3 * token_count * routes.shape[1] // (2 * n_ep)
    width = model_width // n_tp
    hidden_width = gate_weight.shape[2]
    slot_rows = n_ep * capacity

    positions = ep * row_count + jnp.arange(row_count, dtype=jnp.int32)
    half_dim = head_dim // 2
    inverse = rope_base ** (-2.0 * jnp.arange(half_dim, dtype=jnp.float32) / head_dim)
    angles = positions.astype(jnp.float32)[:, None] * inverse[None, :]
    cosine, sine = jnp.cos(angles), jnp.sin(angles)
    cos_table = jnp.concatenate([cosine, cosine], axis=1)
    sin_table = jnp.concatenate([-sine, sine], axis=1)

    vmem = pl.BlockSpec(memory_space=pltpu.VMEM)
    hbm = pl.BlockSpec(memory_space=pl.ANY)
    dma = pltpu.SemaphoreType.DMA
    bf16, f32 = jnp.bfloat16, jnp.float32
    share = n_z // 2
    expert_out, mixed = pl.pallas_call(
        functools.partial(layer_kernel, n_ep, n_tp),
        out_shape=(
            jax.ShapeDtypeStruct((token_count, width), bf16),
            jax.ShapeDtypeStruct((row_count, width), bf16),
        ),
        in_specs=[vmem] * 11 + [hbm] * 4,
        out_specs=(vmem, vmem),
        scratch_shapes=[
            pltpu.VMEM((n_ep, capacity, width), bf16),
            pltpu.VMEM((n_z, row_count, head_width), bf16),
            pltpu.VMEM((n_z, row_count, 2 * head_width), bf16),
            pltpu.VMEM((share, 2, row_count, head_width), bf16),
            pltpu.VMEM((share, 2, row_count, 2 * head_width), bf16),
            pltpu.VMEM((1, 2, row_count, 2 * head_width), bf16),
            pltpu.VMEM((1, n_z, row_count, 2 * head_width), bf16),
            pltpu.VMEM((share, 2, row_count, head_width), bf16),
            pltpu.VMEM((share, 2, 8, row_count), f32),
            pltpu.VMEM((share, 2, 8, row_count), f32),
            pltpu.VMEM((share, 2, 8, row_count), f32),
            pltpu.VMEM((share, 2, 8, row_count), f32),
            pltpu.VMEM((share, 2, 2, row_count, head_width), f32),
            pltpu.VMEM((share, row_count, head_width), bf16),
            pltpu.VMEM((n_z, row_count, head_width), bf16),
            pltpu.VMEM((share, 2, row_count, head_width), bf16),
            pltpu.VMEM((n_z, row_count, head_width), bf16),
            pltpu.VMEM((n_tp * n_ep, capacity, width), bf16),
            pltpu.VMEM(gate_weight.shape, bf16),
            pltpu.VMEM(up_weight.shape, bf16),
            pltpu.VMEM(down_weight.shape, bf16),
            pltpu.VMEM((slot_rows, hidden_width), bf16),
            pltpu.VMEM((n_tp, slot_rows, width), bf16),
            pltpu.VMEM((n_tp, slot_rows, width), bf16),
            pltpu.VMEM((n_ep, capacity, width), bf16),
            pltpu.VMEM((n_ep, capacity, width), bf16),
            pltpu.VMEM(out_weight.shape, bf16),
            pltpu.VMEM((n_z, row_count, head_width), bf16),
            pltpu.VMEM((n_tp, row_count, width), bf16),
            pltpu.VMEM((n_tp, row_count, width), bf16),
            dma((4,)),
            dma((3 + n_z,)),
            dma((n_ep,)),
            dma((n_ep,)),
            dma((n_ep * n_tp,)),
            dma((n_ep * n_tp,)),
            dma((n_tp,)),
            dma((n_tp,)),
            dma((n_ep,)),
            dma((n_ep,)),
            dma((2, share)),
            dma((2, share)),
            dma((2,)),
            dma((2,)),
            dma((2,)),
            dma((n_z,)),
            dma((2, share)),
            dma((share, 2)),
            dma((share,)),
            dma((share,)),
            dma((share, 2)),
            dma((share, 2)),
            dma((share,)),
            dma((n_z,)),
            dma((share, 2)),
            dma((n_z,)),
            dma((n_tp,)),
            dma((n_tp,)),
        ],
        compiler_params=pltpu.CompilerParams(
            collective_id=0, has_side_effects=True, vmem_limit_bytes=60 * 1024 * 1024
        ),
        name="layer",
    )(
        expert_rows,
        expert_gain.reshape(1, model_width),
        routes.T,
        route_weights.T,
        query_maps,
        key_maps,
        value_rows,
        cos_table,
        sin_table,
        head_lambda.reshape(1, n_z),
        head_gain.reshape(1, head_width),
        gate_weight,
        up_weight,
        down_weight,
        out_weight,
    )
    return (mixed, expert_out)


def on_device(
    query_maps,
    key_maps,
    value_rows,
    head_lambda,
    head_gain,
    out_weight,
    expert_rows,
    expert_gain,
    routes,
    route_weights,
    gate_weight,
    up_weight,
    down_weight,
):
    n_ep = lax.axis_size("ep")
    head_count = head_lambda.shape[0]
    capacity = 3 * expert_rows.shape[0] * routes.shape[1] // (2 * n_ep)
    if (
        2 * head_count == n_ep
        and head_count == 4
        and capacity % 16 == 0
        and value_rows.shape[1] == query_maps.shape[1] == 256 * head_count
    ):
        return fused(
            query_maps,
            key_maps,
            value_rows,
            head_lambda,
            head_gain,
            out_weight,
            expert_rows,
            expert_gain,
            routes,
            route_weights,
            gate_weight,
            up_weight,
            down_weight,
        )
    mixed = mixer_half(query_maps, key_maps, value_rows, head_lambda, head_gain, out_weight)
    expert_out = expert_half(
        expert_rows, expert_gain, routes, route_weights, gate_weight, up_weight, down_weight
    )
    return (mixed, expert_out)


def solution(mesh):
    placed = (
        P("ep", "tp"),
        P("ep", "tp"),
        P("ep", "tp"),
        P("tp"),
        P(),
        P("tp", None),
        P("ep", None),
        P(),
        P("ep", None),
        P("ep", None),
        P("ep", None, "tp"),
        P("ep", None, "tp"),
        P("ep", "tp", None),
    )
    return jax.shard_map(
        on_device,
        mesh=mesh,
        in_specs=placed,
        out_specs=(P("ep", "tp"), P("ep", "tp")),
        check_vma=False,
    )
```

```python
import functools

import jax
import jax.numpy as jnp
import numpy as np
from jax import lax
from jax.experimental import pallas as pl
from jax.experimental.pallas import tpu as pltpu
from jax.sharding import PartitionSpec as P

norm_eps = 1e-06
rope_base = 10000.0


def rope_turn(inputs, positions):
    half_dim = inputs.shape[-1] // 2
    inverse = rope_base ** (-2.0 * jnp.arange(half_dim, dtype=jnp.float32) / inputs.shape[-1])
    angles = positions.astype(jnp.float32)[:, None] * inverse[None, :]
    cos_table = jnp.cos(angles)[:, None, None, :]
    sin_table = jnp.sin(angles)[:, None, None, :]
    first_half = inputs[..., :half_dim]
    second_half = inputs[..., half_dim:]
    return jnp.concatenate(
        [
            first_half * cos_table - second_half * sin_table,
            second_half * cos_table + first_half * sin_table,
        ],
        axis=-1,
    )


def mixer_half(query_maps, key_maps, value_rows, head_lambda, head_gain, out_weight):
    row_count = query_maps.shape[0]
    head_count = head_lambda.shape[0]
    head_dim = query_maps.shape[1] // (2 * head_count)
    value_dim = value_rows.shape[1] // head_count
    model_width = out_weight.shape[1]
    score_scale = head_dim ** (-0.5)
    offset = lax.axis_index("ep") * row_count
    positions = offset + jnp.arange(row_count, dtype=jnp.int32)
    last_row = offset + row_count - 1
    rotated_q = rope_turn(
        query_maps.astype(jnp.float32).reshape(row_count, head_count, 2, head_dim), positions
    ).astype(jnp.bfloat16)
    rotated_k = rope_turn(
        key_maps.astype(jnp.float32).reshape(row_count, head_count, 2, head_dim), positions
    ).astype(jnp.bfloat16)
    rotated_k = rotated_k.reshape(row_count, head_count * 2 * head_dim)
    initial = (
        jnp.full((head_count, 2, row_count), -1e30, jnp.float32),
        jnp.zeros((head_count, 2, row_count), jnp.float32),
        jnp.zeros((head_count, 2, row_count, value_dim), jnp.float32),
    )
    piece_k = lax.all_gather(rotated_k, "ep", axis=0, tiled=True)
    piece_v = lax.all_gather(value_rows, "ep", axis=0, tiled=True)
    piece_len = piece_k.shape[0]
    block_size = 1024

    def attend(state):

        def fold_step(inner, block_index):
            block_start = block_index * block_size
            block_k = lax.dynamic_slice_in_dim(piece_k, block_start, block_size, 0).reshape(
                block_size, head_count, 2, head_dim
            )
            block_v = lax.dynamic_slice_in_dim(piece_v, block_start, block_size, 0).reshape(
                block_size, head_count, value_dim
            )
            scores = (
                jnp.einsum(
                    "qhmd,khmd->hmqk", rotated_q, block_k, preferred_element_type=jnp.float32
                )
                * score_scale
            )
            key_pos = block_start + jnp.arange(block_size, dtype=jnp.int32)
            causal = key_pos[None, :] <= positions[:, None]
            masked = jnp.where(causal, scores, -1e30)
            run_max, run_sum, run_acc = inner
            new_max = jnp.maximum(run_max, jnp.max(masked, axis=-1))
            expd = jnp.where(causal, jnp.exp(masked - new_max[..., None]), 0.0)
            rescale = jnp.exp(run_max - new_max)
            new_sum = run_sum * rescale + jnp.sum(expd, axis=-1)
            new_acc = run_acc * rescale[..., None] + jnp.einsum(
                "hmqk,khe->hmqe",
                expd.astype(jnp.bfloat16),
                block_v,
                preferred_element_type=jnp.float32,
            )
            return ((new_max, new_sum, new_acc), None)

        result, _ = lax.scan(fold_step, state, jnp.arange(piece_len // block_size, dtype=jnp.int32))
        return result

    def skip_piece(state):
        return state

    run_max, run_sum, run_acc = lax.cond(jnp.int32(0) <= last_row, attend, skip_piece, initial)
    first_map = run_acc[:, 0] / run_sum[:, 0][..., None]
    second_map = run_acc[:, 1] / run_sum[:, 1][..., None]
    difference = first_map - head_lambda[:, None, None] * second_map
    head_out = (
        difference
        * lax.rsqrt(jnp.mean(difference * difference, axis=-1, keepdims=True) + norm_eps)
        * head_gain
    ).astype(jnp.bfloat16)
    partial_value = jnp.einsum(
        "hqe,hed->qd",
        head_out,
        out_weight.reshape(head_count, value_dim, model_width),
        preferred_element_type=jnp.float32,
    )
    return lax.psum_scatter(
        partial_value.astype(jnp.bfloat16), "tp", scatter_dimension=1, tiled=True
    )


def expert_half(
    expert_rows, expert_gain, routes, route_weights, gate_weight, up_weight, down_weight
):
    ep_count = lax.axis_size("ep")
    tp_count = lax.axis_size("tp")
    row_count, model_width = expert_rows.shape
    pick_count = routes.shape[1]
    capacity = 3 * row_count * pick_count // (2 * ep_count)
    column_count = model_width // tp_count
    inputs = expert_rows.astype(jnp.float32)
    normed = (
        inputs
        * lax.rsqrt(jnp.mean(inputs * inputs, axis=-1, keepdims=True) + norm_eps)
        * expert_gain
    ).astype(jnp.bfloat16)
    expert_ids = routes.reshape(-1)
    one_hot = (expert_ids[:, None] == jnp.arange(ep_count, dtype=jnp.int32)[None, :]).astype(
        jnp.int32
    )
    slot_index = jnp.sum((jnp.cumsum(one_hot, axis=0) - one_hot) * one_hot, axis=1)
    source_row = jnp.arange(row_count * pick_count, dtype=jnp.int32) // pick_count
    empty = jnp.zeros((ep_count, capacity, normed.shape[1]), jnp.bfloat16)
    arrived = lax.all_to_all(
        empty.at[expert_ids, slot_index].set(normed[source_row]),
        "ep",
        split_axis=0,
        concat_axis=0,
        tiled=True,
    )
    slot_count = arrived.shape[1]
    flat_rows = arrived.reshape(ep_count * slot_count, model_width)
    gate_values = jnp.dot(flat_rows, gate_weight[0], preferred_element_type=jnp.float32)
    up_values = jnp.dot(flat_rows, up_weight[0], preferred_element_type=jnp.float32)
    hidden = (jax.nn.silu(gate_values) * up_values).astype(jnp.bfloat16)
    partial_value = jnp.dot(hidden, down_weight[0], preferred_element_type=jnp.float32).reshape(
        ep_count, slot_count, model_width
    )
    summed = lax.psum_scatter(
        partial_value.astype(jnp.bfloat16), "tp", scatter_dimension=2, tiled=True
    )
    returned = lax.all_to_all(summed, "ep", split_axis=0, concat_axis=0, tiled=True)
    picked = returned[expert_ids, slot_index].reshape(row_count, pick_count, column_count)
    combined = jnp.sum(route_weights[..., None] * picked.astype(jnp.float32), axis=1)
    return combined.astype(jnp.bfloat16)


MESH = pl.DeviceIdType.MESH


def remote(source, target, send_sem, recv_sem, device):
    return pltpu.make_async_remote_copy(
        src_ref=source,
        dst_ref=target,
        send_sem=send_sem,
        recv_sem=recv_sem,
        device_id=device,
        device_id_type=MESH,
    )


def layer_kernel(
    n_ep,
    n_tp,
    rows_ref,
    norm_gain_ref,
    routes_ref,
    route_weights_ref,
    query_ref,
    key_ref,
    value_ref,
    turn_ref,
    offset_ref,
    lambda_ref,
    gain_ref,
    gate_hbm,
    up_hbm,
    down_hbm,
    weight_hbm,
    expert_ref,
    mixed_ref,
    slots_ref,
    packed_q,
    packed_kv,
    own_q,
    own_kv,
    below_kv,
    lower_kv,
    upper_q,
    own_stat,
    upper_stat,
    low_stat,
    back_stat,
    own_maps,
    own_part,
    own_diff,
    low_part,
    low_diff,
    gathered,
    gate_vmem,
    up_vmem,
    down_vmem,
    hidden,
    partial,
    arrived,
    summed,
    returned,
    weight_vmem,
    heads,
    mixed_partial,
    mixed_arrived,
    weight_sem,
    local_sem,
    disp_send,
    disp_recv,
    gath_send,
    gath_recv,
    part_send,
    part_recv,
    ret_send,
    ret_recv,
    swap_send,
    swap_recv,
    below_send,
    below_recv,
    lower_send,
    lower_recv,
    upper_send,
    upper_recv,
    stat_send,
    stat_recv,
    back_send,
    back_recv,
    diff_send,
    diff_recv,
    cross_send,
    cross_recv,
    mixed_send,
    mixed_recv,
    hold_sem,
):
    ep = lax.axis_index("ep")
    tp = lax.axis_index("tp")
    n_z = n_ep // 2
    middle = n_z // 2
    z, core = ep // 2, lax.rem(ep, 2)
    odd = lax.rem(z, 2)
    asks = [z >= middle, odd == 1]
    host = [middle - 1, z - 1]
    seat = [lax.rem(z, middle), 0]
    partner = {"ep": ep + 1 - 2 * core}
    capacity, width = slots_ref.shape[1:]
    rows = n_ep * capacity
    head_count, row_count, head_width = packed_q.shape
    share = head_count // 2
    half = head_width // 2
    first = core * share
    weights = [
        pltpu.make_async_copy(gate_hbm, gate_vmem, weight_sem.at[0]),
        pltpu.make_async_copy(up_hbm, up_vmem, weight_sem.at[1]),
        pltpu.make_async_copy(down_hbm, down_vmem, weight_sem.at[2]),
        pltpu.make_async_copy(weight_hbm, weight_vmem, weight_sem.at[3]),
    ]
    for copy in weights:
        copy.start()
    peers = [{"ep": lax.rem(ep + d, n_ep)} for d in range(1, n_ep)]
    peers += [{"tp": lax.rem(tp + d, n_tp)} for d in range(1, n_tp)]
    barrier = pltpu.get_barrier_semaphore()
    for device in peers:
        pl.semaphore_signal(barrier, inc=1, device_id=device, device_id_type=MESH)

    token_count = rows_ref.shape[0]
    picks = routes_ref.shape[0]
    entries = rows_ref[...].astype(jnp.float32)
    inverse_norm = lax.rsqrt(jnp.mean(entries * entries, axis=1, keepdims=True) + norm_eps)
    own = pl.ds(pl.multiple_of(tp * width, width), width)
    normed = rows_ref[:, own].astype(jnp.float32) * inverse_norm * norm_gain_ref[:, own]
    normed = normed.astype(jnp.bfloat16)
    named_rows = -(-n_ep // 16) * 16
    label = lax.broadcasted_iota(jnp.int32, (named_rows, token_count), 0)
    named = [
        jnp.where(label == routes_ref[k : k + 1, :], 1.0, 0.0).astype(jnp.float32)
        for k in range(picks)
    ]
    before = lax.broadcasted_iota(jnp.int32, (token_count, token_count), 0)
    after = lax.broadcasted_iota(jnp.int32, (token_count, token_count), 1)
    earlier = jnp.dot(
        sum(named).astype(jnp.bfloat16),
        jnp.where(before < after, 1.0, 0.0).astype(jnp.bfloat16),
        preferred_element_type=jnp.float32,
    )
    slot_of = lax.broadcasted_iota(jnp.int32, (rows, token_count), 0)
    select = []
    for k in range(picks):
        rank = jnp.sum(named[k] * earlier, axis=0, keepdims=True).astype(jnp.int32)
        place = routes_ref[k : k + 1, :] * capacity + rank
        select.append(jnp.where(slot_of == place, 1.0, 0.0).astype(jnp.float32))
    slots_ref[...] = (
        jnp.dot(
            sum(select).astype(jnp.bfloat16), normed, preferred_element_type=jnp.float32
        )
        .astype(jnp.bfloat16)
        .reshape(n_ep, capacity, width)
    )
    with jax.named_scope("barrier"):
        pl.semaphore_wait(barrier, len(peers))
    across, along = tp + 1 - 2 * lax.rem(tp, 2), lax.rem(tp + 2, n_tp)
    corner = n_tp - 1 - tp
    dispatch = [pltpu.make_async_copy(slots_ref.at[ep], gathered.at[tp, 0], local_sem.at[0])]
    for d in range(1, n_ep):
        target = lax.rem(ep + d, n_ep)
        dispatch.append(
            remote(
                slots_ref.at[target],
                gathered.at[tp, d],
                disp_send.at[d],
                disp_recv.at[d],
                {"ep": target},
            )
        )
    for copy in dispatch:
        copy.start()

    cos_off, sin_off = offset_ref[0, pl.ds(ep, 1), :], offset_ref[1, pl.ds(ep, 1), :]
    cosine = turn_ref[0] * cos_off - turn_ref[1] * sin_off
    sine = turn_ref[1] * cos_off + turn_ref[0] * sin_off
    sine = jnp.where(lax.broadcasted_iota(jnp.int32, sine.shape, 1) < half // 2, -sine, sine)
    for head in range(head_count):
        for m in range(2):
            at = head * head_width + m * half
            to = slice(m * half, (m + 1) * half)
            for ref, packed in ((query_ref, packed_q), (key_ref, packed_kv)):
                entry = ref[:, at : at + half].astype(jnp.float32)
                turned = entry * cosine + pltpu.roll(entry, half // 2, 1) * sine
                packed[head, :, to] = turned.astype(jnp.bfloat16)
        packed_kv[head, :, head_width:] = value_ref[
            :, head * head_width : (head + 1) * head_width
        ]
    other = share - first
    swaps = []
    for j in range(share):
        swaps += [
            remote(
                packed_q.at[other + j],
                own_q.at[j, core],
                swap_send.at[0, j],
                swap_recv.at[0, j],
                partner,
            ),
            remote(
                packed_kv.at[other + j],
                own_kv.at[j, core],
                swap_send.at[1, j],
                swap_recv.at[1, j],
                partner,
            ),
        ]
    keeps = []
    for j in range(share):
        keeps += [
            pltpu.make_async_copy(packed_q.at[first + j], own_q.at[j, core], local_sem.at[3 + j]),
            pltpu.make_async_copy(
                packed_kv.at[first + j], own_kv.at[j, core], local_sem.at[3 + share + j]
            ),
        ]
    for copy in swaps + keeps:
        copy.start()

    def lift(side):
        return remote(
            packed_kv.at[side * share],
            below_kv.at[0, core],
            below_send.at[side],
            below_recv.at[core],
            {"ep": lax.rem(ep - core + 2 + side, n_ep)},
        )

    def lift_far(side):
        return remote(
            packed_kv.at[side * share + 1],
            lower_kv.at[0, 2 * lax.rem(z, middle) + core],
            lower_send.at[side],
            lower_recv.at[2 * lax.rem(z, middle) + core],
            {"ep": 2 * middle + side},
        )

    def ask(side, j):
        return remote(
            packed_q.at[side * share + j],
            upper_q.at[seat[j], core],
            upper_send.at[side, j],
            upper_recv.at[seat[j], core],
            {"ep": 2 * host[j] + side},
        )

    def wait_landed(ref, sem):
        pltpu.make_async_copy(ref, ref, sem).wait()

    spread = []
    with jax.named_scope("wait_disp"):
        for d in range(n_ep):
            if d == 0:
                dispatch[0].wait()
            else:
                dispatch[d].wait_recv()
            slot = gathered.at[tp, d]
            for way, device in enumerate((across, along)):
                copy = remote(
                    slot, slot, gath_send.at[way, d], gath_recv.at[way, d], {"tp": device}
                )
                copy.start()
                spread.append(copy)

    for j in range(share):
        for side in range(2):

            @pl.when(asks[j])
            def _():
                ask(side, j).start()

    for side in range(2):

        @pl.when(odd == 0)
        def _():
            lift(side).start()

    for side in range(2):

        @pl.when(z < middle)
        def _():
            lift_far(side).start()

    row = lax.broadcasted_iota(jnp.int32, (row_count, row_count), 0)
    column = lax.broadcasted_iota(jnp.int32, (row_count, row_count), 1)
    causal = column <= row
    wide = lax.broadcasted_iota(jnp.int32, (row_count, 2 * row_count), 0) + row_count
    wide_causal = lax.broadcasted_iota(jnp.int32, (row_count, 2 * row_count), 1) <= wide
    diagonal = column == row
    scale = half ** (-0.5)
    stat_row = lax.broadcasted_iota(jnp.int32, (8, row_count), 0)

    def as_column(values):
        return jnp.sum(jnp.where(diagonal, values, 0.0), axis=1, keepdims=True)

    def as_row(values):
        return jnp.sum(jnp.where(diagonal, values, 0.0), axis=0, keepdims=True)

    def as_stats(levels):
        return jnp.where(stat_row == 0, as_row(levels[0]), as_row(levels[1]))

    def head_weight(j):
        lanes = lax.broadcasted_iota(jnp.int32, lambda_ref.shape, 1)
        return jnp.sum(
            jnp.where(lanes == first + j, lambda_ref[...], 0.0), axis=1, keepdims=True
        )

    def fold(query_of, pieces, m):
        scores = []
        for keys_of, values_of, mask in pieces:
            piece = lax.dot_general(
                query_of(m), keys_of(m), (((1,), (1,)), ((), ())), preferred_element_type=jnp.float32
            )
            piece = piece * scale
            if mask is not None:
                piece = jnp.where(mask, piece, -1e30)
            scores.append(piece)
        peak = functools.reduce(
            jnp.maximum, [jnp.max(piece, axis=1, keepdims=True) for piece in scores]
        )
        total = jnp.zeros((row_count, 1), jnp.float32)
        outcome = jnp.zeros((row_count, head_width), jnp.float32)
        for piece, (keys_of, values_of, mask) in zip(scores, pieces):
            expd = jnp.exp(piece - peak)
            total += jnp.sum(expd, axis=1, keepdims=True)
            outcome += jnp.dot(
                expd.astype(jnp.bfloat16), values_of(), preferred_element_type=jnp.float32
            )
        return peak, total, outcome

    def piece_of(ref, j, count, mask):
        def keys_of(m):
            keys = ref[j, :count, :, m * half : (m + 1) * half]
            return keys.reshape(count * row_count, half)

        def values_of():
            return ref[j, :count, :, head_width:].reshape(count * row_count, head_width)

        return keys_of, values_of, mask

    def keep_diff(j, block, difference):
        @pl.when(core == block)
        def _():
            own_diff[first + j] = difference.astype(jnp.bfloat16)

        @pl.when(core != block)
        def _():
            own_part[j] = difference.astype(jnp.bfloat16)
            send_diff(j).start()

    def send_diff(j):
        return remote(
            own_part.at[j], own_diff.at[first + j], diff_send.at[j], diff_recv.at[first + j], partner
        )

    def send_stat(j):
        return remote(
            own_stat.at[j],
            upper_stat.at[seat[j]],
            stat_send.at[j],
            stat_recv.at[seat[j]],
            {"ep": 2 * host[j] + core},
        )

    def wait_own(j):
        swaps[2 * j].wait_recv()
        swaps[2 * j + 1].wait_recv()
        keeps[2 * j].wait()
        keeps[2 * j + 1].wait()

    def local_head(j, pieces):
        for block in range(2):
            mask = wide_causal if block else causal
            parts = pieces + [piece_of(own_kv, j, block + 1, mask)]
            maps, levels = [], []
            for m in range(2):
                peak, total, outcome = fold(
                    lambda m: own_q[j, block, :, m * half : (m + 1) * half], parts, m
                )
                maps.append(outcome / total)
                levels.append(peak + jnp.log(total))

            @pl.when(asks[j])
            def _():
                own_maps[j, block, 0] = maps[0]
                own_maps[j, block, 1] = maps[1]
                own_stat[j, block] = as_stats(levels)

            @pl.when(jnp.logical_not(asks[j]))
            def _():
                keep_diff(j, block, maps[0] - head_weight(j) * maps[1])

        @pl.when(asks[j])
        def _():
            send_stat(j).start()

    def send_cross(up, j, block, target):
        return remote(
            low_part.at[up, block],
            low_diff.at[first + j],
            cross_send.at[up, block],
            cross_recv.at[first + j],
            {"ep": 2 * target + block},
        )

    def send_back(up, j, block, target):
        return remote(
            low_stat.at[up, block],
            back_stat.at[j, block],
            back_send.at[up, block],
            back_recv.at[j, block],
            {"ep": 2 * target + core},
        )

    def cross_head(j, count, base, pieces):
        def step(index, carry):
            up, block = index // 2, lax.rem(index, 2)
            target = base + up
            wait_landed(upper_q.at[up, block], upper_recv.at[up, block])

            @pl.when(block == 0)
            def _():
                wait_landed(upper_stat.at[up], stat_recv.at[up])

            maps, levels = [], []
            for m in range(2):
                peak, total, outcome = fold(
                    lambda m: upper_q[up, block, :, m * half : (m + 1) * half], pieces, m
                )
                level = peak + jnp.log(total)
                above = as_column(upper_stat[up, block, m : m + 1, :])
                whole = jnp.maximum(level, above) + jnp.log(1.0 + jnp.exp(-jnp.abs(level - above)))
                maps.append(outcome * jnp.exp(peak - whole))
                levels.append(level)
            low_stat[up, block] = as_stats(levels)
            send_back(up, j, block, target).start()
            low_part[up, block] = (maps[0] - head_weight(j) * maps[1]).astype(jnp.bfloat16)
            send_cross(up, j, block, target).start()
            return carry

        lax.fori_loop(0, 2 * count, step, 0)

    def finish_upper(j):
        for block in range(2):
            wait_landed(back_stat.at[j, block], back_recv.at[j, block])
            maps = []
            for m in range(2):
                below = as_column(back_stat[j, block, m : m + 1, :])
                level = as_column(own_stat[j, block, m : m + 1, :])
                maps.append(own_maps[j, block, m] / (1.0 + jnp.exp(below - level)))
            keep_diff(j, block, maps[0] - head_weight(j) * maps[1])

    below_piece = piece_of(below_kv, 0, 2, None)
    lower_piece = piece_of(lower_kv, 0, 2 * middle, None)

    @pl.when(z != middle)
    def _():
        with jax.named_scope("own1"):
            wait_own(1)
            local_head(1, [])

    @pl.when(odd == 0)
    def _():
        with jax.named_scope("own0"):
            wait_own(0)
            local_head(0, [])

    with jax.named_scope("forward"):
        for d in range(n_ep):
            way = d % 2
            slot = gathered.at[(across, along)[way], d]
            wait_landed(slot, gath_recv.at[way, d])
            copy = remote(
                slot, slot, gath_send.at[2, d], gath_recv.at[2, d], {"tp": (along, across)[way]}
            )
            copy.start()
            spread.append(copy)
    tile = 256
    part_count = n_ep // 2
    part_rows = part_count * capacity
    scatter = []
    for part in range(2):
        lead = part * part_count
        with jax.named_scope(f"wait_gath#p={part}"):
            for d in range(lead, lead + part_count):
                way = 1 - d % 2
                wait_landed(gathered.at[(across, along)[way], d], gath_recv.at[way, d])
                wait_landed(gathered.at[corner, d], gath_recv.at[2, d])
        if part == 0:
            weights[0].wait()
            weights[1].wait()

        def hidden_tile(j, carry):
            columns = pl.ds(pl.multiple_of(j * tile, tile), tile)
            gate = jnp.zeros((part_rows, tile), jnp.float32)
            up = jnp.zeros((part_rows, tile), jnp.float32)
            for i in range(n_tp):
                block = gathered[i, lead : lead + part_count].reshape(part_rows, width)
                gate += jnp.dot(
                    block,
                    gate_vmem[0, i * width : (i + 1) * width, columns],
                    preferred_element_type=jnp.float32,
                )
                up += jnp.dot(
                    block,
                    up_vmem[0, i * width : (i + 1) * width, columns],
                    preferred_element_type=jnp.float32,
                )
            hidden[part, :, columns] = (gate / (1.0 + jnp.exp(-gate)) * up).astype(jnp.bfloat16)
            return carry

        with jax.named_scope(f"gateup#p={part}"):
            lax.fori_loop(0, hidden.shape[2] // tile, hidden_tile, 0)
        if part == 0:
            weights[2].wait()
        with jax.named_scope(f"down#p={part}"):
            for d in list(range(1, n_tp)) + [0]:
                target = lax.rem(tp + d, n_tp)
                columns = pl.ds(pl.multiple_of(target * width, width), width)
                partial[part, d] = jnp.dot(
                    hidden[part], down_vmem[0, :, columns], preferred_element_type=jnp.float32
                ).astype(jnp.bfloat16)
                if d:
                    copy = remote(
                        partial.at[part, d],
                        arrived.at[part, d],
                        part_send.at[part, d],
                        part_recv.at[part, d],
                        {"tp": target},
                    )
                    copy.start()
                    scatter.append(copy)

    @pl.when(odd == 1)
    def _():
        with jax.named_scope("odd0"):
            for source in range(2):
                wait_landed(below_kv.at[0, source], below_recv.at[source])
            wait_own(0)
            local_head(0, [below_piece])

    @pl.when(z == 0)
    def _():
        with jax.named_scope("cross0"):
            cross_head(1, 1, 1, [piece_of(own_kv, 1, 2, None)])

    @pl.when(z == middle - 1)
    def _():
        with jax.named_scope("cross1"):
            cross_head(0, middle, middle, [below_piece, piece_of(own_kv, 0, 2, None)])

    def project():
        with jax.named_scope("wait_heads"):
            for j in range(share):
                wait_landed(own_diff.at[other + j], diff_recv.at[other + j])

                @pl.when(asks[j])
                def _():
                    for side in range(2):
                        at = side * share + j
                        wait_landed(low_diff.at[at], cross_recv.at[at])

        for head in range(head_count):
            difference = own_diff[head].astype(jnp.float32) + low_diff[head].astype(jnp.float32)
            mean = jnp.mean(difference * difference, axis=1, keepdims=True)
            heads[head] = (difference * lax.rsqrt(mean + norm_eps) * gain_ref[...]).astype(
                jnp.bfloat16
            )
        weights[3].wait()
        for d in list(range(1, n_tp)) + [0]:
            target = lax.rem(tp + d, n_tp)
            columns = pl.ds(pl.multiple_of(target * width, width), width)
            product = jnp.zeros((row_count, width), jnp.float32)
            for h in range(head_count):
                product += jnp.dot(
                    heads[h],
                    weight_vmem[h * head_width : (h + 1) * head_width, columns],
                    preferred_element_type=jnp.float32,
                )
            mixed_partial[d] = product.astype(jnp.bfloat16)
            if d:
                mixed_copy(d).start()

    def mixed_copy(d):
        return remote(
            mixed_partial.at[d],
            mixed_arrived.at[d],
            mixed_send.at[d],
            mixed_recv.at[d],
            {"tp": lax.rem(tp + d, n_tp)},
        )

    back = []
    for d in range(n_ep):
        if d == 0:
            copy = pltpu.make_async_copy(summed.at[0], returned.at[ep], local_sem.at[2])
        else:
            copy = remote(
                summed.at[d],
                returned.at[ep],
                ret_send.at[d],
                ret_recv.at[d],
                {"ep": lax.rem(ep + n_ep - d, n_ep)},
            )
        back.append(copy)

    def sum_part(part):
        lead = part * part_count
        total = partial[part, 0].astype(jnp.float32)
        with jax.named_scope(f"wait_part#p={part}"):
            for d in range(1, n_tp):
                scatter[part * (n_tp - 1) + d - 1].wait_recv()
                total += arrived[part, d].astype(jnp.float32)
        summed[lead : lead + part_count] = total.astype(jnp.bfloat16).reshape(
            part_count, capacity, width
        )

    for j in range(share):

        @pl.when(jnp.logical_not(asks[j]))
        def _():
            for side in range(2):
                low_diff[side * share + j] = jnp.zeros((row_count, head_width), jnp.bfloat16)

    @pl.when(z == middle - 1)
    def _():
        with jax.named_scope("finish"):
            finish_upper(1)

    @pl.when(z < middle)
    def _():
        with jax.named_scope("project_low"):
            project()

    sum_part(0)

    @pl.when(z >= middle)
    def _():
        for copy in back[:part_count]:
            copy.start()

    @pl.when(z == middle)
    def _():
        with jax.named_scope("cross2"):
            for source in range(2 * middle):
                wait_landed(lower_kv.at[0, source], lower_recv.at[source])
            wait_own(1)
            cross_head(1, 1, middle + 1, [lower_piece, piece_of(own_kv, 1, 2, None)])
            local_head(1, [lower_piece])

    sum_part(1)

    @pl.when(z < middle)
    def _():
        targets = [lax.rem(ep + n_ep - d, n_ep) for d in range(n_ep)]
        for target, copy in zip(targets, back):

            @pl.when(target < 2 * middle)
            def _():
                copy.start()

        with jax.named_scope("hold"):

            @pl.when(z == middle - 1)
            def _():
                for up in range(middle):
                    for side in range(2):
                        send_cross(up, 0, side, middle + up).wait_send()
                pl.semaphore_signal(
                    hold_sem,
                    inc=1,
                    device_id={"ep": lax.rem(ep + n_ep - 2, n_ep)},
                    device_id_type=MESH,
                )

            @pl.when(z != middle - 1)
            def _():
                pl.semaphore_wait(hold_sem, 1)

        for target, copy in zip(targets, back):

            @pl.when(target >= 2 * middle)
            def _():
                copy.start()

    @pl.when(z >= middle)
    def _():
        for copy in back[part_count:]:
            copy.start()

        with jax.named_scope("finish"):
            finish_upper(0)

        @pl.when(odd == 1)
        def _():
            with jax.named_scope("finish"):
                finish_upper(1)

        with jax.named_scope("project_up"):
            project()

    with jax.named_scope("wait_back"):
        back[0].wait()
        for copy in back[1:]:
            copy.wait_recv()
    flat = returned[...].reshape(rows, width)
    result = jnp.zeros(expert_ref.shape, jnp.float32)
    for k in range(picks):
        picked = lax.dot_general(
            select[k].astype(jnp.bfloat16),
            flat,
            (((0,), (0,)), ((), ())),
            preferred_element_type=jnp.float32,
        )
        spread_out = jnp.where(before == after, route_weights_ref[k : k + 1, :], 0.0)
        result += jnp.sum(spread_out, axis=1, keepdims=True) * picked
    expert_ref[...] = result.astype(expert_ref.dtype)
    total = mixed_partial[0].astype(jnp.float32)
    with jax.named_scope("wait_mixed"):
        for d in range(1, n_tp):
            mixed_copy(d).wait_recv()
            total += mixed_arrived[d].astype(jnp.float32)
    mixed_ref[...] = total.astype(jnp.bfloat16)
    for copy in dispatch[1:] + swaps + spread + scatter + back[1:]:
        copy.wait_send()
    for d in range(1, n_tp):
        mixed_copy(d).wait_send()
    for j in range(share):
        send_diff(j).wait_send()

        @pl.when(asks[j])
        def _():
            send_stat(j).wait_send()
            for side in range(2):
                ask(side, j).wait_send()

    for side in range(2):

        @pl.when(odd == 0)
        def _():
            lift(side).wait_send()

        @pl.when(z < middle)
        def _():
            lift_far(side).wait_send()

        @pl.when(z <= middle)
        def _():
            send_back(0, 0, side, z + 1).wait_send()

            @pl.when(z != middle - 1)
            def _():
                send_cross(0, 0, side, z + 1).wait_send()

        @pl.when(z == middle - 1)
        def _():
            send_back(1, 0, side, z + 2).wait_send()


def hand_over(expert_ref, mixed_ref, expert_out, mixed_out):
    expert_out[...] = expert_ref[...]
    mixed_out[...] = mixed_ref[...]


def fused(
    query_maps,
    key_maps,
    value_rows,
    head_lambda,
    head_gain,
    out_weight,
    expert_rows,
    expert_gain,
    routes,
    route_weights,
    gate_weight,
    up_weight,
    down_weight,
):
    n_ep = lax.axis_size("ep")
    n_tp = lax.axis_size("tp")
    n_z = n_ep // 2
    row_count = query_maps.shape[0]
    head_width = query_maps.shape[1] // n_z
    head_dim = head_width // 2
    token_count, model_width = expert_rows.shape
    capacity = 3 * token_count * routes.shape[1] // (2 * n_ep)
    width = model_width // n_tp
    hidden_width = gate_weight.shape[2]
    slot_rows = n_ep * capacity

    half_dim = head_dim // 2
    inverse = rope_base ** (-2.0 * np.arange(half_dim) / head_dim)
    inverse = np.concatenate([inverse, inverse])
    turns = np.arange(row_count)[:, None] * inverse
    offsets = (row_count * np.arange(n_ep))[:, None] * inverse
    turns = jnp.asarray(np.stack([np.cos(turns), np.sin(turns)]), jnp.float32)
    offsets = jnp.asarray(np.stack([np.cos(offsets), np.sin(offsets)]), jnp.float32)

    vmem = pl.BlockSpec(memory_space=pltpu.VMEM)
    hbm = pl.BlockSpec(memory_space=pl.ANY)
    dma = pltpu.SemaphoreType.DMA
    bf16, f32 = jnp.bfloat16, jnp.float32
    share = n_z // 2
    expert_out, mixed = pl.pallas_call(
        functools.partial(layer_kernel, n_ep, n_tp),
        out_shape=(
            jax.ShapeDtypeStruct((token_count, width), bf16),
            jax.ShapeDtypeStruct((row_count, width), bf16),
        ),
        in_specs=[vmem] * 11 + [hbm] * 4,
        out_specs=(vmem, vmem),
        scratch_shapes=[
            pltpu.VMEM((n_ep, capacity, width), bf16),
            pltpu.VMEM((n_z, row_count, head_width), bf16),
            pltpu.VMEM((n_z, row_count, 2 * head_width), bf16),
            pltpu.VMEM((share, 2, row_count, head_width), bf16),
            pltpu.VMEM((share, 2, row_count, 2 * head_width), bf16),
            pltpu.VMEM((1, 2, row_count, 2 * head_width), bf16),
            pltpu.VMEM((1, n_z, row_count, 2 * head_width), bf16),
            pltpu.VMEM((share, 2, row_count, head_width), bf16),
            pltpu.VMEM((share, 2, 8, row_count), f32),
            pltpu.VMEM((share, 2, 8, row_count), f32),
            pltpu.VMEM((share, 2, 8, row_count), f32),
            pltpu.VMEM((share, 2, 8, row_count), f32),
            pltpu.VMEM((share, 2, 2, row_count, head_width), f32),
            pltpu.VMEM((share, row_count, head_width), bf16),
            pltpu.VMEM((n_z, row_count, head_width), bf16),
            pltpu.VMEM((share, 2, row_count, head_width), bf16),
            pltpu.VMEM((n_z, row_count, head_width), bf16),
            pltpu.VMEM((n_tp, n_ep, capacity, width), bf16),
            pltpu.VMEM(gate_weight.shape, bf16),
            pltpu.VMEM(up_weight.shape, bf16),
            pltpu.VMEM(down_weight.shape, bf16),
            pltpu.VMEM((2, slot_rows // 2, hidden_width), bf16),
            pltpu.VMEM((2, n_tp, slot_rows // 2, width), bf16),
            pltpu.VMEM((2, n_tp, slot_rows // 2, width), bf16),
            pltpu.VMEM((n_ep, capacity, width), bf16),
            pltpu.VMEM((n_ep, capacity, width), bf16),
            pltpu.VMEM(out_weight.shape, bf16),
            pltpu.VMEM((n_z, row_count, head_width), bf16),
            pltpu.VMEM((n_tp, row_count, width), bf16),
            pltpu.VMEM((n_tp, row_count, width), bf16),
            dma((4,)),
            dma((3 + n_z,)),
            dma((n_ep,)),
            dma((n_ep,)),
            dma((3, n_ep)),
            dma((3, n_ep)),
            dma((2, n_tp)),
            dma((2, n_tp)),
            dma((n_ep,)),
            dma((n_ep,)),
            dma((2, share)),
            dma((2, share)),
            dma((2,)),
            dma((2,)),
            dma((2,)),
            dma((n_z,)),
            dma((2, share)),
            dma((share, 2)),
            dma((share,)),
            dma((share,)),
            dma((share, 2)),
            dma((share, 2)),
            dma((share,)),
            dma((n_z,)),
            dma((share, 2)),
            dma((n_z,)),
            dma((n_tp,)),
            dma((n_tp,)),
            pltpu.SemaphoreType.REGULAR,
        ],
        compiler_params=pltpu.CompilerParams(
            collective_id=0, has_side_effects=True, vmem_limit_bytes=60 * 1024 * 1024
        ),
        name="layer",
    )(
        expert_rows,
        expert_gain.reshape(1, model_width),
        routes.T,
        route_weights.T,
        query_maps,
        key_maps,
        value_rows,
        turns,
        offsets,
        head_lambda.reshape(1, n_z),
        head_gain.reshape(1, head_width),
        gate_weight,
        up_weight,
        down_weight,
        out_weight,
    )
    expert_out, mixed = pl.pallas_call(
        hand_over,
        out_shape=(
            jax.ShapeDtypeStruct((token_count, width), bf16),
            jax.ShapeDtypeStruct((row_count, width), bf16),
        ),
        in_specs=[vmem] * 2,
        out_specs=(vmem, vmem),
        name="hand_over",
    )(expert_out, mixed)
    return (mixed, expert_out)


def on_device(
    query_maps,
    key_maps,
    value_rows,
    head_lambda,
    head_gain,
    out_weight,
    expert_rows,
    expert_gain,
    routes,
    route_weights,
    gate_weight,
    up_weight,
    down_weight,
):
    n_ep = lax.axis_size("ep")
    head_count = head_lambda.shape[0]
    capacity = 3 * expert_rows.shape[0] * routes.shape[1] // (2 * n_ep)
    if (
        2 * head_count == n_ep
        and head_count == lax.axis_size("tp") == 4
        and capacity % 16 == 0
        and value_rows.shape[1] == query_maps.shape[1] == 256 * head_count
    ):
        return fused(
            query_maps,
            key_maps,
            value_rows,
            head_lambda,
            head_gain,
            out_weight,
            expert_rows,
            expert_gain,
            routes,
            route_weights,
            gate_weight,
            up_weight,
            down_weight,
        )
    mixed = mixer_half(query_maps, key_maps, value_rows, head_lambda, head_gain, out_weight)
    expert_out = expert_half(
        expert_rows, expert_gain, routes, route_weights, gate_weight, up_weight, down_weight
    )
    return (mixed, expert_out)


def solution(mesh):
    placed = (
        P("ep", "tp"),
        P("ep", "tp"),
        P("ep", "tp"),
        P("tp"),
        P(),
        P("tp", None),
        P("ep", None),
        P(),
        P("ep", None),
        P("ep", None),
        P("ep", None, "tp"),
        P("ep", None, "tp"),
        P("ep", "tp", None),
    )
    return jax.shard_map(
        on_device,
        mesh=mesh,
        in_specs=placed,
        out_specs=(P("ep", "tp"), P("ep", "tp")),
        check_vma=False,
    )
```

```python
import functools

import jax
import jax.numpy as jnp
import numpy as np
from jax import lax
from jax.experimental import pallas as pl
from jax.experimental.pallas import tpu as pltpu
from jax.sharding import PartitionSpec as P

norm_eps = 1e-06
rope_base = 10000.0


def rope_turn(inputs, positions):
    half_dim = inputs.shape[-1] // 2
    inverse = rope_base ** (-2.0 * jnp.arange(half_dim, dtype=jnp.float32) / inputs.shape[-1])
    angles = positions.astype(jnp.float32)[:, None] * inverse[None, :]
    cos_table = jnp.cos(angles)[:, None, None, :]
    sin_table = jnp.sin(angles)[:, None, None, :]
    first_half = inputs[..., :half_dim]
    second_half = inputs[..., half_dim:]
    return jnp.concatenate(
        [
            first_half * cos_table - second_half * sin_table,
            second_half * cos_table + first_half * sin_table,
        ],
        axis=-1,
    )


def mixer_half(query_maps, key_maps, value_rows, head_lambda, head_gain, out_weight):
    row_count = query_maps.shape[0]
    head_count = head_lambda.shape[0]
    head_dim = query_maps.shape[1] // (2 * head_count)
    value_dim = value_rows.shape[1] // head_count
    model_width = out_weight.shape[1]
    score_scale = head_dim ** (-0.5)
    offset = lax.axis_index("ep") * row_count
    positions = offset + jnp.arange(row_count, dtype=jnp.int32)
    last_row = offset + row_count - 1
    rotated_q = rope_turn(
        query_maps.astype(jnp.float32).reshape(row_count, head_count, 2, head_dim), positions
    ).astype(jnp.bfloat16)
    rotated_k = rope_turn(
        key_maps.astype(jnp.float32).reshape(row_count, head_count, 2, head_dim), positions
    ).astype(jnp.bfloat16)
    rotated_k = rotated_k.reshape(row_count, head_count * 2 * head_dim)
    initial = (
        jnp.full((head_count, 2, row_count), -1e30, jnp.float32),
        jnp.zeros((head_count, 2, row_count), jnp.float32),
        jnp.zeros((head_count, 2, row_count, value_dim), jnp.float32),
    )
    piece_k = lax.all_gather(rotated_k, "ep", axis=0, tiled=True)
    piece_v = lax.all_gather(value_rows, "ep", axis=0, tiled=True)
    piece_len = piece_k.shape[0]
    block_size = 1024

    def attend(state):

        def fold_step(inner, block_index):
            block_start = block_index * block_size
            block_k = lax.dynamic_slice_in_dim(piece_k, block_start, block_size, 0).reshape(
                block_size, head_count, 2, head_dim
            )
            block_v = lax.dynamic_slice_in_dim(piece_v, block_start, block_size, 0).reshape(
                block_size, head_count, value_dim
            )
            scores = (
                jnp.einsum(
                    "qhmd,khmd->hmqk", rotated_q, block_k, preferred_element_type=jnp.float32
                )
                * score_scale
            )
            key_pos = block_start + jnp.arange(block_size, dtype=jnp.int32)
            causal = key_pos[None, :] <= positions[:, None]
            masked = jnp.where(causal, scores, -1e30)
            run_max, run_sum, run_acc = inner
            new_max = jnp.maximum(run_max, jnp.max(masked, axis=-1))
            expd = jnp.where(causal, jnp.exp(masked - new_max[..., None]), 0.0)
            rescale = jnp.exp(run_max - new_max)
            new_sum = run_sum * rescale + jnp.sum(expd, axis=-1)
            new_acc = run_acc * rescale[..., None] + jnp.einsum(
                "hmqk,khe->hmqe",
                expd.astype(jnp.bfloat16),
                block_v,
                preferred_element_type=jnp.float32,
            )
            return ((new_max, new_sum, new_acc), None)

        result, _ = lax.scan(fold_step, state, jnp.arange(piece_len // block_size, dtype=jnp.int32))
        return result

    def skip_piece(state):
        return state

    run_max, run_sum, run_acc = lax.cond(jnp.int32(0) <= last_row, attend, skip_piece, initial)
    first_map = run_acc[:, 0] / run_sum[:, 0][..., None]
    second_map = run_acc[:, 1] / run_sum[:, 1][..., None]
    difference = first_map - head_lambda[:, None, None] * second_map
    head_out = (
        difference
        * lax.rsqrt(jnp.mean(difference * difference, axis=-1, keepdims=True) + norm_eps)
        * head_gain
    ).astype(jnp.bfloat16)
    partial_value = jnp.einsum(
        "hqe,hed->qd",
        head_out,
        out_weight.reshape(head_count, value_dim, model_width),
        preferred_element_type=jnp.float32,
    )
    return lax.psum_scatter(
        partial_value.astype(jnp.bfloat16), "tp", scatter_dimension=1, tiled=True
    )


def expert_half(
    expert_rows, expert_gain, routes, route_weights, gate_weight, up_weight, down_weight
):
    ep_count = lax.axis_size("ep")
    tp_count = lax.axis_size("tp")
    row_count, model_width = expert_rows.shape
    pick_count = routes.shape[1]
    capacity = 3 * row_count * pick_count // (2 * ep_count)
    column_count = model_width // tp_count
    inputs = expert_rows.astype(jnp.float32)
    normed = (
        inputs
        * lax.rsqrt(jnp.mean(inputs * inputs, axis=-1, keepdims=True) + norm_eps)
        * expert_gain
    ).astype(jnp.bfloat16)
    expert_ids = routes.reshape(-1)
    one_hot = (expert_ids[:, None] == jnp.arange(ep_count, dtype=jnp.int32)[None, :]).astype(
        jnp.int32
    )
    slot_index = jnp.sum((jnp.cumsum(one_hot, axis=0) - one_hot) * one_hot, axis=1)
    source_row = jnp.arange(row_count * pick_count, dtype=jnp.int32) // pick_count
    empty = jnp.zeros((ep_count, capacity, normed.shape[1]), jnp.bfloat16)
    arrived = lax.all_to_all(
        empty.at[expert_ids, slot_index].set(normed[source_row]),
        "ep",
        split_axis=0,
        concat_axis=0,
        tiled=True,
    )
    slot_count = arrived.shape[1]
    flat_rows = arrived.reshape(ep_count * slot_count, model_width)
    gate_values = jnp.dot(flat_rows, gate_weight[0], preferred_element_type=jnp.float32)
    up_values = jnp.dot(flat_rows, up_weight[0], preferred_element_type=jnp.float32)
    hidden = (jax.nn.silu(gate_values) * up_values).astype(jnp.bfloat16)
    partial_value = jnp.dot(hidden, down_weight[0], preferred_element_type=jnp.float32).reshape(
        ep_count, slot_count, model_width
    )
    summed = lax.psum_scatter(
        partial_value.astype(jnp.bfloat16), "tp", scatter_dimension=2, tiled=True
    )
    returned = lax.all_to_all(summed, "ep", split_axis=0, concat_axis=0, tiled=True)
    picked = returned[expert_ids, slot_index].reshape(row_count, pick_count, column_count)
    combined = jnp.sum(route_weights[..., None] * picked.astype(jnp.float32), axis=1)
    return combined.astype(jnp.bfloat16)


MESH = pl.DeviceIdType.MESH


def remote(source, target, send_sem, recv_sem, device):
    return pltpu.make_async_remote_copy(
        src_ref=source,
        dst_ref=target,
        send_sem=send_sem,
        recv_sem=recv_sem,
        device_id=device,
        device_id_type=MESH,
    )


def layer_kernel(
    n_ep,
    n_tp,
    rows_ref,
    norm_gain_ref,
    routes_ref,
    route_weights_ref,
    query_ref,
    key_ref,
    value_ref,
    turn_ref,
    offset_ref,
    lambda_ref,
    gain_ref,
    gate_hbm,
    up_hbm,
    down_hbm,
    weight_hbm,
    expert_ref,
    mixed_ref,
    slots_ref,
    packed_q,
    packed_kv,
    own_q,
    own_kv,
    below_kv,
    lower_kv,
    upper_q,
    own_stat,
    upper_stat,
    low_stat,
    back_stat,
    own_maps,
    own_part,
    own_diff,
    low_part,
    low_diff,
    gathered,
    gate_vmem,
    up_vmem,
    down_vmem,
    hidden,
    partial,
    arrived,
    summed,
    returned,
    weight_vmem,
    heads,
    mixed_partial,
    mixed_arrived,
    mixed_sum,
    weight_sem,
    local_sem,
    disp_send,
    disp_recv,
    gath_send,
    gath_recv,
    part_send,
    part_recv,
    ret_send,
    ret_recv,
    swap_send,
    swap_recv,
    below_send,
    below_recv,
    lower_send,
    lower_recv,
    upper_send,
    upper_recv,
    stat_send,
    stat_recv,
    back_send,
    back_recv,
    diff_send,
    diff_recv,
    cross_send,
    cross_recv,
    mixed_send,
    mixed_recv,
    hold_sem,
):
    ep = lax.axis_index("ep")
    tp = lax.axis_index("tp")
    n_z = n_ep // 2
    middle = n_z // 2
    z, core = ep // 2, lax.rem(ep, 2)
    odd = lax.rem(z, 2)
    asks = [z >= middle, odd == 1]
    host = [middle - 1, z - 1]
    seat = [lax.rem(z, middle), 0]
    partner = {"ep": ep + 1 - 2 * core}
    capacity, width = slots_ref.shape[1:]
    rows = n_ep * capacity
    head_count, row_count, head_width = packed_q.shape
    share = head_count // 2
    half = head_width // 2
    first = core * share
    weights = [
        pltpu.make_async_copy(gate_hbm, gate_vmem, weight_sem.at[0]),
        pltpu.make_async_copy(up_hbm, up_vmem, weight_sem.at[1]),
        pltpu.make_async_copy(down_hbm, down_vmem, weight_sem.at[2]),
        pltpu.make_async_copy(weight_hbm, weight_vmem, weight_sem.at[3]),
    ]
    for copy in weights:
        copy.start()
    peers = [{"ep": lax.rem(ep + d, n_ep)} for d in range(1, n_ep)]
    peers += [{"tp": lax.rem(tp + d, n_tp)} for d in range(1, n_tp)]
    barrier = pltpu.get_barrier_semaphore()
    for device in peers:
        pl.semaphore_signal(barrier, inc=1, device_id=device, device_id_type=MESH)

    token_count = rows_ref.shape[0]
    picks = routes_ref.shape[0]
    entries = rows_ref[...].astype(jnp.float32)
    inverse_norm = lax.rsqrt(jnp.mean(entries * entries, axis=1, keepdims=True) + norm_eps)
    own = pl.ds(pl.multiple_of(tp * width, width), width)
    normed = rows_ref[:, own].astype(jnp.float32) * inverse_norm * norm_gain_ref[:, own]
    normed = normed.astype(jnp.bfloat16)
    named_rows = -(-n_ep // 16) * 16
    label = lax.broadcasted_iota(jnp.int32, (named_rows, token_count), 0)
    named = [
        jnp.where(label == routes_ref[k : k + 1, :], 1.0, 0.0).astype(jnp.float32)
        for k in range(picks)
    ]
    before = lax.broadcasted_iota(jnp.int32, (token_count, token_count), 0)
    after = lax.broadcasted_iota(jnp.int32, (token_count, token_count), 1)
    earlier = jnp.dot(
        sum(named).astype(jnp.bfloat16),
        jnp.where(before < after, 1.0, 0.0).astype(jnp.bfloat16),
        preferred_element_type=jnp.float32,
    )
    slot_of = lax.broadcasted_iota(jnp.int32, (rows, token_count), 0)
    select = []
    for k in range(picks):
        rank = jnp.sum(named[k] * earlier, axis=0, keepdims=True).astype(jnp.int32)
        place = routes_ref[k : k + 1, :] * capacity + rank
        select.append(jnp.where(slot_of == place, 1.0, 0.0).astype(jnp.float32))
    slots_ref[...] = (
        jnp.dot(
            sum(select).astype(jnp.bfloat16), normed, preferred_element_type=jnp.float32
        )
        .astype(jnp.bfloat16)
        .reshape(n_ep, capacity, width)
    )
    with jax.named_scope("barrier"):
        pl.semaphore_wait(barrier, len(peers))
    across, along = tp + 1 - 2 * lax.rem(tp, 2), lax.rem(tp + 2, n_tp)
    corner = n_tp - 1 - tp
    dispatch = [pltpu.make_async_copy(slots_ref.at[ep], gathered.at[tp, 0], local_sem.at[0])]
    for d in range(1, n_ep):
        target = lax.rem(ep + d, n_ep)
        dispatch.append(
            remote(
                slots_ref.at[target],
                gathered.at[tp, d],
                disp_send.at[d],
                disp_recv.at[d],
                {"ep": target},
            )
        )
    for copy in dispatch:
        copy.start()

    cos_off, sin_off = offset_ref[0, pl.ds(ep, 1), :], offset_ref[1, pl.ds(ep, 1), :]
    cosine = turn_ref[0] * cos_off - turn_ref[1] * sin_off
    sine = turn_ref[1] * cos_off + turn_ref[0] * sin_off
    sine = jnp.where(lax.broadcasted_iota(jnp.int32, sine.shape, 1) < half // 2, -sine, sine)
    for head in range(head_count):
        for m in range(2):
            at = head * head_width + m * half
            to = slice(m * half, (m + 1) * half)
            for ref, packed in ((query_ref, packed_q), (key_ref, packed_kv)):
                entry = ref[:, at : at + half].astype(jnp.float32)
                turned = entry * cosine + pltpu.roll(entry, half // 2, 1) * sine
                packed[head, :, to] = turned.astype(jnp.bfloat16)
        packed_kv[head, :, head_width:] = value_ref[
            :, head * head_width : (head + 1) * head_width
        ]
    other = share - first
    swaps = []
    for j in range(share):
        swaps += [
            remote(
                packed_q.at[other + j],
                own_q.at[j, core],
                swap_send.at[0, j],
                swap_recv.at[0, j],
                partner,
            ),
            remote(
                packed_kv.at[other + j],
                own_kv.at[j, core],
                swap_send.at[1, j],
                swap_recv.at[1, j],
                partner,
            ),
        ]
    keeps = []
    for j in range(share):
        keeps += [
            pltpu.make_async_copy(packed_q.at[first + j], own_q.at[j, core], local_sem.at[3 + j]),
            pltpu.make_async_copy(
                packed_kv.at[first + j], own_kv.at[j, core], local_sem.at[3 + share + j]
            ),
        ]
    for copy in swaps + keeps:
        copy.start()

    def lift(side):
        return remote(
            packed_kv.at[side * share],
            below_kv.at[0, core],
            below_send.at[side],
            below_recv.at[core],
            {"ep": lax.rem(ep - core + 2 + side, n_ep)},
        )

    def lift_far(side):
        return remote(
            packed_kv.at[side * share + 1],
            lower_kv.at[0, 2 * lax.rem(z, middle) + core],
            lower_send.at[side],
            lower_recv.at[2 * lax.rem(z, middle) + core],
            {"ep": 2 * middle + side},
        )

    def ask(side, j):
        return remote(
            packed_q.at[side * share + j],
            upper_q.at[seat[j], core],
            upper_send.at[side, j],
            upper_recv.at[seat[j], core],
            {"ep": 2 * host[j] + side},
        )

    def wait_landed(ref, sem):
        pltpu.make_async_copy(ref, ref, sem).wait()

    spread = []
    with jax.named_scope("wait_disp"):
        for d in range(n_ep):
            if d == 0:
                dispatch[0].wait()
            else:
                dispatch[d].wait_recv()
            slot = gathered.at[tp, d]
            for way, device in enumerate((across, along)):
                copy = remote(
                    slot, slot, gath_send.at[way, d], gath_recv.at[way, d], {"tp": device}
                )
                copy.start()
                spread.append(copy)

    for j in range(share):
        for side in range(2):

            @pl.when(asks[j])
            def _():
                ask(side, j).start()

    for side in range(2):

        @pl.when(odd == 0)
        def _():
            lift(side).start()

    for side in range(2):

        @pl.when(z < middle)
        def _():
            lift_far(side).start()

    row = lax.broadcasted_iota(jnp.int32, (row_count, row_count), 0)
    column = lax.broadcasted_iota(jnp.int32, (row_count, row_count), 1)
    causal = column <= row
    wide = lax.broadcasted_iota(jnp.int32, (row_count, 2 * row_count), 0) + row_count
    wide_causal = lax.broadcasted_iota(jnp.int32, (row_count, 2 * row_count), 1) <= wide
    diagonal = column == row
    scale = half ** (-0.5)
    stat_row = lax.broadcasted_iota(jnp.int32, (8, row_count), 0)

    def as_column(values):
        return jnp.sum(jnp.where(diagonal, values, 0.0), axis=1, keepdims=True)

    def as_row(values):
        return jnp.sum(jnp.where(diagonal, values, 0.0), axis=0, keepdims=True)

    def as_stats(levels):
        return jnp.where(stat_row == 0, as_row(levels[0]), as_row(levels[1]))

    def head_weight(j):
        lanes = lax.broadcasted_iota(jnp.int32, lambda_ref.shape, 1)
        return jnp.sum(
            jnp.where(lanes == first + j, lambda_ref[...], 0.0), axis=1, keepdims=True
        )

    def fold(query_of, pieces, m):
        scores = []
        for keys_of, values_of, mask in pieces:
            piece = lax.dot_general(
                query_of(m), keys_of(m), (((1,), (1,)), ((), ())), preferred_element_type=jnp.float32
            )
            piece = piece * scale
            if mask is not None:
                piece = jnp.where(mask, piece, -1e30)
            scores.append(piece)
        peak = functools.reduce(
            jnp.maximum, [jnp.max(piece, axis=1, keepdims=True) for piece in scores]
        )
        total = jnp.zeros((row_count, 1), jnp.float32)
        outcome = jnp.zeros((row_count, head_width), jnp.float32)
        for piece, (keys_of, values_of, mask) in zip(scores, pieces):
            expd = jnp.exp(piece - peak)
            total += jnp.sum(expd, axis=1, keepdims=True)
            outcome += jnp.dot(
                expd.astype(jnp.bfloat16), values_of(), preferred_element_type=jnp.float32
            )
        return peak, total, outcome

    def piece_of(ref, j, count, mask):
        def keys_of(m):
            keys = ref[j, :count, :, m * half : (m + 1) * half]
            return keys.reshape(count * row_count, half)

        def values_of():
            return ref[j, :count, :, head_width:].reshape(count * row_count, head_width)

        return keys_of, values_of, mask

    def keep_diff(j, block, difference):
        @pl.when(core == block)
        def _():
            own_diff[first + j] = difference.astype(jnp.bfloat16)

        @pl.when(core != block)
        def _():
            own_part[j] = difference.astype(jnp.bfloat16)
            send_diff(j).start()

    def send_diff(j):
        return remote(
            own_part.at[j], own_diff.at[first + j], diff_send.at[j], diff_recv.at[first + j], partner
        )

    def send_stat(j):
        return remote(
            own_stat.at[j],
            upper_stat.at[seat[j]],
            stat_send.at[j],
            stat_recv.at[seat[j]],
            {"ep": 2 * host[j] + core},
        )

    def wait_own(j):
        swaps[2 * j].wait_recv()
        swaps[2 * j + 1].wait_recv()
        keeps[2 * j].wait()
        keeps[2 * j + 1].wait()

    def local_head(j, pieces):
        for block in range(2):
            mask = wide_causal if block else causal
            parts = pieces + [piece_of(own_kv, j, block + 1, mask)]
            maps, levels = [], []
            for m in range(2):
                peak, total, outcome = fold(
                    lambda m: own_q[j, block, :, m * half : (m + 1) * half], parts, m
                )
                maps.append(outcome / total)
                levels.append(peak + jnp.log(total))

            @pl.when(asks[j])
            def _():
                own_maps[j, block, 0] = maps[0]
                own_maps[j, block, 1] = maps[1]
                own_stat[j, block] = as_stats(levels)

            @pl.when(jnp.logical_not(asks[j]))
            def _():
                keep_diff(j, block, maps[0] - head_weight(j) * maps[1])

        @pl.when(asks[j])
        def _():
            send_stat(j).start()

    def send_cross(up, j, block, target):
        return remote(
            low_part.at[up, block],
            low_diff.at[first + j],
            cross_send.at[up, block],
            cross_recv.at[first + j],
            {"ep": 2 * target + block},
        )

    def send_back(up, j, block, target):
        return remote(
            low_stat.at[up, block],
            back_stat.at[j, block],
            back_send.at[up, block],
            back_recv.at[j, block],
            {"ep": 2 * target + core},
        )

    def cross_head(j, count, base, pieces):
        def step(index, carry):
            up, block = index // 2, lax.rem(index, 2)
            target = base + up
            wait_landed(upper_q.at[up, block], upper_recv.at[up, block])

            @pl.when(block == 0)
            def _():
                wait_landed(upper_stat.at[up], stat_recv.at[up])

            maps, levels = [], []
            for m in range(2):
                peak, total, outcome = fold(
                    lambda m: upper_q[up, block, :, m * half : (m + 1) * half], pieces, m
                )
                level = peak + jnp.log(total)
                above = as_column(upper_stat[up, block, m : m + 1, :])
                whole = jnp.maximum(level, above) + jnp.log(1.0 + jnp.exp(-jnp.abs(level - above)))
                maps.append(outcome * jnp.exp(peak - whole))
                levels.append(level)
            low_stat[up, block] = as_stats(levels)
            send_back(up, j, block, target).start()
            low_part[up, block] = (maps[0] - head_weight(j) * maps[1]).astype(jnp.bfloat16)
            send_cross(up, j, block, target).start()
            return carry

        lax.fori_loop(0, 2 * count, step, 0)

    def finish_upper(j):
        for block in range(2):
            wait_landed(back_stat.at[j, block], back_recv.at[j, block])
            maps = []
            for m in range(2):
                below = as_column(back_stat[j, block, m : m + 1, :])
                level = as_column(own_stat[j, block, m : m + 1, :])
                maps.append(own_maps[j, block, m] / (1.0 + jnp.exp(below - level)))
            keep_diff(j, block, maps[0] - head_weight(j) * maps[1])

    below_piece = piece_of(below_kv, 0, 2, None)
    lower_piece = piece_of(lower_kv, 0, 2 * middle, None)

    @pl.when(z != middle)
    def _():
        with jax.named_scope("own1"):
            wait_own(1)
            local_head(1, [])

    @pl.when(odd == 0)
    def _():
        with jax.named_scope("own0"):
            wait_own(0)
            local_head(0, [])

    with jax.named_scope("forward"):
        for d in range(n_ep):
            way = d % 2
            slot = gathered.at[(across, along)[way], d]
            wait_landed(slot, gath_recv.at[way, d])
            copy = remote(
                slot, slot, gath_send.at[2, d], gath_recv.at[2, d], {"tp": (along, across)[way]}
            )
            copy.start()
            spread.append(copy)
    tile = 256
    part_count = n_ep // 2
    part_rows = part_count * capacity
    scatter = []
    for part in range(2):
        lead = part * part_count
        with jax.named_scope(f"wait_gath#p={part}"):
            for d in range(lead, lead + part_count):
                way = 1 - d % 2
                wait_landed(gathered.at[(across, along)[way], d], gath_recv.at[way, d])
                wait_landed(gathered.at[corner, d], gath_recv.at[2, d])
        if part == 0:
            weights[0].wait()
            weights[1].wait()

        def hidden_tile(j, carry):
            columns = pl.ds(pl.multiple_of(j * tile, tile), tile)
            gate = jnp.zeros((part_rows, tile), jnp.float32)
            up = jnp.zeros((part_rows, tile), jnp.float32)
            for i in range(n_tp):
                block = gathered[i, lead : lead + part_count].reshape(part_rows, width)
                gate += jnp.dot(
                    block,
                    gate_vmem[0, i * width : (i + 1) * width, columns],
                    preferred_element_type=jnp.float32,
                )
                up += jnp.dot(
                    block,
                    up_vmem[0, i * width : (i + 1) * width, columns],
                    preferred_element_type=jnp.float32,
                )
            hidden[part, :, columns] = (gate / (1.0 + jnp.exp(-gate)) * up).astype(jnp.bfloat16)
            return carry

        with jax.named_scope(f"gateup#p={part}"):
            lax.fori_loop(0, hidden.shape[2] // tile, hidden_tile, 0)
        if part == 0:
            weights[2].wait()
        with jax.named_scope(f"down#p={part}"):
            for d in list(range(1, n_tp)) + [0]:
                target = lax.rem(tp + d, n_tp)
                columns = pl.ds(pl.multiple_of(target * width, width), width)
                partial[part, d] = jnp.dot(
                    hidden[part], down_vmem[0, :, columns], preferred_element_type=jnp.float32
                ).astype(jnp.bfloat16)
                if d:
                    copy = remote(
                        partial.at[part, d],
                        arrived.at[part, d],
                        part_send.at[part, d],
                        part_recv.at[part, d],
                        {"tp": target},
                    )
                    copy.start()
                    scatter.append(copy)

    @pl.when(odd == 1)
    def _():
        with jax.named_scope("odd0"):
            for source in range(2):
                wait_landed(below_kv.at[0, source], below_recv.at[source])
            wait_own(0)
            local_head(0, [below_piece])

    @pl.when(z == 0)
    def _():
        with jax.named_scope("cross0"):
            cross_head(1, 1, 1, [piece_of(own_kv, 1, 2, None)])

    @pl.when(z == middle - 1)
    def _():
        with jax.named_scope("cross1"):
            cross_head(0, middle, middle, [below_piece, piece_of(own_kv, 0, 2, None)])

    def project():
        with jax.named_scope("wait_heads"):
            for j in range(share):
                wait_landed(own_diff.at[other + j], diff_recv.at[other + j])

                @pl.when(asks[j])
                def _():
                    for side in range(2):
                        at = side * share + j
                        wait_landed(low_diff.at[at], cross_recv.at[at])

        for head in range(head_count):
            difference = own_diff[head].astype(jnp.float32) + low_diff[head].astype(jnp.float32)
            mean = jnp.mean(difference * difference, axis=1, keepdims=True)
            heads[head] = (difference * lax.rsqrt(mean + norm_eps) * gain_ref[...]).astype(
                jnp.bfloat16
            )
        weights[3].wait()
        for role, target in ((3, corner), (1, across), (2, along), (0, tp)):
            columns = pl.ds(pl.multiple_of(target * width, width), width)
            product = jnp.zeros((row_count, width), jnp.float32)
            for h in range(head_count):
                product += jnp.dot(
                    heads[h],
                    weight_vmem[h * head_width : (h + 1) * head_width, columns],
                    preferred_element_type=jnp.float32,
                )
            mixed_partial[role] = product.astype(jnp.bfloat16).reshape(
                2, row_count // 2, width
            )
            for part in range(2):
                if role == 3:
                    mixed_copy(1, part).start()
                elif role == 1 + part:
                    mixed_copy(0, part).start()

    ways = (across, along)

    def mixed_copy(kind, part):
        return remote(
            (mixed_partial.at[1 + part, part], mixed_partial.at[3, part], mixed_sum.at[part])[kind],
            mixed_arrived.at[kind, part],
            mixed_send.at[kind, part],
            mixed_recv.at[kind, part],
            {"tp": ways[1 - part if kind == 2 else part]},
        )

    def mixed_forward():
        with jax.named_scope("mixed_forward"):
            for part in range(2):
                mixed_copy(1, part).wait_recv()
                both = mixed_partial[2 - part, part].astype(jnp.float32)
                both += mixed_arrived[1, part].astype(jnp.float32)
                mixed_sum[part] = both.astype(jnp.bfloat16)
                mixed_copy(2, part).start()

    back = []
    for d in range(n_ep):
        if d == 0:
            copy = pltpu.make_async_copy(summed.at[0], returned.at[ep], local_sem.at[2])
        else:
            copy = remote(
                summed.at[d],
                returned.at[ep],
                ret_send.at[d],
                ret_recv.at[d],
                {"ep": lax.rem(ep + n_ep - d, n_ep)},
            )
        back.append(copy)

    def sum_part(part):
        lead = part * part_count
        total = partial[part, 0].astype(jnp.float32)
        with jax.named_scope(f"wait_part#p={part}"):
            for d in range(1, n_tp):
                scatter[part * (n_tp - 1) + d - 1].wait_recv()
                total += arrived[part, d].astype(jnp.float32)
        summed[lead : lead + part_count] = total.astype(jnp.bfloat16).reshape(
            part_count, capacity, width
        )

    for j in range(share):

        @pl.when(jnp.logical_not(asks[j]))
        def _():
            for side in range(2):
                low_diff[side * share + j] = jnp.zeros((row_count, head_width), jnp.bfloat16)

    @pl.when(z == middle - 1)
    def _():
        with jax.named_scope("finish"):
            finish_upper(1)

    @pl.when(z < middle)
    def _():
        with jax.named_scope("project_low"):
            project()

    sum_part(0)

    @pl.when(z < middle)
    def _():
        mixed_forward()

    @pl.when(z >= middle)
    def _():
        for copy in back[:part_count]:
            copy.start()

    @pl.when(z == middle)
    def _():
        with jax.named_scope("cross2"):
            for source in range(2 * middle):
                wait_landed(lower_kv.at[0, source], lower_recv.at[source])
            wait_own(1)
            cross_head(1, 1, middle + 1, [lower_piece, piece_of(own_kv, 1, 2, None)])
            local_head(1, [lower_piece])

    sum_part(1)

    def release():
        pl.semaphore_signal(
            hold_sem,
            inc=1,
            device_id={"ep": lax.rem(ep + n_ep - 2, n_ep)},
            device_id_type=MESH,
        )

    @pl.when(z < middle)
    def _():
        targets = [lax.rem(ep + n_ep - d, n_ep) for d in range(n_ep)]
        for target, copy in zip(targets, back):

            @pl.when(target < 2 * middle)
            def _():
                copy.start()

        with jax.named_scope("hold"):

            @pl.when(z == middle - 1)
            def _():
                for up in range(middle):
                    for side in range(2):
                        send_cross(up, 0, side, middle + up).wait_send()
                pl.semaphore_wait(hold_sem, 1)
                release()

            @pl.when(z != middle - 1)
            def _():
                pl.semaphore_wait(hold_sem, 1)

        for target, copy in zip(targets, back):

            @pl.when(target >= 2 * middle)
            def _():
                copy.start()

    @pl.when(z >= middle)
    def _():
        @pl.when(z != middle)
        def _():
            for copy in back[part_count:]:
                copy.start()

        with jax.named_scope("finish"):
            finish_upper(0)

        @pl.when(odd == 1)
        def _():
            with jax.named_scope("finish"):
                finish_upper(1)

        with jax.named_scope("project_up"):
            project()

        @pl.when(z == middle)
        def _():
            with jax.named_scope("held"):
                for side in range(2):
                    send_cross(0, 1, side, middle + 1).wait_send()
            release()
            for copy in back[part_count:]:
                copy.start()

        mixed_forward()

    with jax.named_scope("wait_back"):
        back[0].wait()
        for copy in back[1:]:
            copy.wait_recv()
    flat = returned[...].reshape(rows, width)
    result = jnp.zeros(expert_ref.shape, jnp.float32)
    for k in range(picks):
        picked = lax.dot_general(
            select[k].astype(jnp.bfloat16),
            flat,
            (((0,), (0,)), ((), ())),
            preferred_element_type=jnp.float32,
        )
        spread_out = jnp.where(before == after, route_weights_ref[k : k + 1, :], 0.0)
        result += jnp.sum(spread_out, axis=1, keepdims=True) * picked
    expert_ref[...] = result.astype(expert_ref.dtype)
    with jax.named_scope("wait_mixed"):
        for part in range(2):
            total = mixed_partial[0, part].astype(jnp.float32)
            for kind in (0, 2):
                mixed_copy(kind, part).wait_recv()
                total += mixed_arrived[kind, part].astype(jnp.float32)
            lines = slice(part * row_count // 2, (part + 1) * row_count // 2)
            mixed_ref[lines, :] = total.astype(jnp.bfloat16)
    for copy in dispatch[1:] + swaps + spread + scatter + back[1:]:
        copy.wait_send()
    for kind in range(3):
        for part in range(2):
            mixed_copy(kind, part).wait_send()
    for j in range(share):
        send_diff(j).wait_send()

        @pl.when(asks[j])
        def _():
            send_stat(j).wait_send()
            for side in range(2):
                ask(side, j).wait_send()

    for side in range(2):

        @pl.when(odd == 0)
        def _():
            lift(side).wait_send()

        @pl.when(z < middle)
        def _():
            lift_far(side).wait_send()

        @pl.when(z <= middle)
        def _():
            send_back(0, 0, side, z + 1).wait_send()

            @pl.when(z < middle - 1)
            def _():
                send_cross(0, 0, side, z + 1).wait_send()

        @pl.when(z == middle - 1)
        def _():
            send_back(1, 0, side, z + 2).wait_send()


def hand_over(expert_ref, mixed_ref, expert_out, mixed_out):
    expert_out[...] = expert_ref[...]
    mixed_out[...] = mixed_ref[...]


def fused(
    query_maps,
    key_maps,
    value_rows,
    head_lambda,
    head_gain,
    out_weight,
    expert_rows,
    expert_gain,
    routes,
    route_weights,
    gate_weight,
    up_weight,
    down_weight,
):
    n_ep = lax.axis_size("ep")
    n_tp = lax.axis_size("tp")
    n_z = n_ep // 2
    row_count = query_maps.shape[0]
    head_width = query_maps.shape[1] // n_z
    head_dim = head_width // 2
    token_count, model_width = expert_rows.shape
    capacity = 3 * token_count * routes.shape[1] // (2 * n_ep)
    width = model_width // n_tp
    hidden_width = gate_weight.shape[2]
    slot_rows = n_ep * capacity

    half_dim = head_dim // 2
    inverse = rope_base ** (-2.0 * np.arange(half_dim) / head_dim)
    inverse = np.concatenate([inverse, inverse])
    turns = np.arange(row_count)[:, None] * inverse
    offsets = (row_count * np.arange(n_ep))[:, None] * inverse
    turns = jnp.asarray(np.stack([np.cos(turns), np.sin(turns)]), jnp.float32)
    offsets = jnp.asarray(np.stack([np.cos(offsets), np.sin(offsets)]), jnp.float32)

    vmem = pl.BlockSpec(memory_space=pltpu.VMEM)
    hbm = pl.BlockSpec(memory_space=pl.ANY)
    dma = pltpu.SemaphoreType.DMA
    bf16, f32 = jnp.bfloat16, jnp.float32
    share = n_z // 2
    expert_out, mixed = pl.pallas_call(
        functools.partial(layer_kernel, n_ep, n_tp),
        out_shape=(
            jax.ShapeDtypeStruct((token_count, width), bf16),
            jax.ShapeDtypeStruct((row_count, width), bf16),
        ),
        in_specs=[vmem] * 11 + [hbm] * 4,
        out_specs=(vmem, vmem),
        scratch_shapes=[
            pltpu.VMEM((n_ep, capacity, width), bf16),
            pltpu.VMEM((n_z, row_count, head_width), bf16),
            pltpu.VMEM((n_z, row_count, 2 * head_width), bf16),
            pltpu.VMEM((share, 2, row_count, head_width), bf16),
            pltpu.VMEM((share, 2, row_count, 2 * head_width), bf16),
            pltpu.VMEM((1, 2, row_count, 2 * head_width), bf16),
            pltpu.VMEM((1, n_z, row_count, 2 * head_width), bf16),
            pltpu.VMEM((share, 2, row_count, head_width), bf16),
            pltpu.VMEM((share, 2, 8, row_count), f32),
            pltpu.VMEM((share, 2, 8, row_count), f32),
            pltpu.VMEM((share, 2, 8, row_count), f32),
            pltpu.VMEM((share, 2, 8, row_count), f32),
            pltpu.VMEM((share, 2, 2, row_count, head_width), f32),
            pltpu.VMEM((share, row_count, head_width), bf16),
            pltpu.VMEM((n_z, row_count, head_width), bf16),
            pltpu.VMEM((share, 2, row_count, head_width), bf16),
            pltpu.VMEM((n_z, row_count, head_width), bf16),
            pltpu.VMEM((n_tp, n_ep, capacity, width), bf16),
            pltpu.VMEM(gate_weight.shape, bf16),
            pltpu.VMEM(up_weight.shape, bf16),
            pltpu.VMEM(down_weight.shape, bf16),
            pltpu.VMEM((2, slot_rows // 2, hidden_width), bf16),
            pltpu.VMEM((2, n_tp, slot_rows // 2, width), bf16),
            pltpu.VMEM((2, n_tp, slot_rows // 2, width), bf16),
            pltpu.VMEM((n_ep, capacity, width), bf16),
            pltpu.VMEM((n_ep, capacity, width), bf16),
            pltpu.VMEM(out_weight.shape, bf16),
            pltpu.VMEM((n_z, row_count, head_width), bf16),
            pltpu.VMEM((n_tp, 2, row_count // 2, width), bf16),
            pltpu.VMEM((3, 2, row_count // 2, width), bf16),
            pltpu.VMEM((2, row_count // 2, width), bf16),
            dma((4,)),
            dma((3 + n_z,)),
            dma((n_ep,)),
            dma((n_ep,)),
            dma((3, n_ep)),
            dma((3, n_ep)),
            dma((2, n_tp)),
            dma((2, n_tp)),
            dma((n_ep,)),
            dma((n_ep,)),
            dma((2, share)),
            dma((2, share)),
            dma((2,)),
            dma((2,)),
            dma((2,)),
            dma((n_z,)),
            dma((2, share)),
            dma((share, 2)),
            dma((share,)),
            dma((share,)),
            dma((share, 2)),
            dma((share, 2)),
            dma((share,)),
            dma((n_z,)),
            dma((share, 2)),
            dma((n_z,)),
            dma((3, 2)),
            dma((3, 2)),
            pltpu.SemaphoreType.REGULAR,
        ],
        compiler_params=pltpu.CompilerParams(
            collective_id=0, has_side_effects=True, vmem_limit_bytes=60 * 1024 * 1024
        ),
        name="layer",
    )(
        expert_rows,
        expert_gain.reshape(1, model_width),
        routes.T,
        route_weights.T,
        query_maps,
        key_maps,
        value_rows,
        turns,
        offsets,
        head_lambda.reshape(1, n_z),
        head_gain.reshape(1, head_width),
        gate_weight,
        up_weight,
        down_weight,
        out_weight,
    )
    expert_out, mixed = pl.pallas_call(
        hand_over,
        out_shape=(
            jax.ShapeDtypeStruct((token_count, width), bf16),
            jax.ShapeDtypeStruct((row_count, width), bf16),
        ),
        in_specs=[vmem] * 2,
        out_specs=(vmem, vmem),
        name="hand_over",
    )(expert_out, mixed)
    return (mixed, expert_out)


def on_device(
    query_maps,
    key_maps,
    value_rows,
    head_lambda,
    head_gain,
    out_weight,
    expert_rows,
    expert_gain,
    routes,
    route_weights,
    gate_weight,
    up_weight,
    down_weight,
):
    n_ep = lax.axis_size("ep")
    head_count = head_lambda.shape[0]
    capacity = 3 * expert_rows.shape[0] * routes.shape[1] // (2 * n_ep)
    if (
        2 * head_count == n_ep
        and head_count == lax.axis_size("tp") == 4
        and capacity % 16 == 0
        and value_rows.shape[1] == query_maps.shape[1] == 256 * head_count
    ):
        return fused(
            query_maps,
            key_maps,
            value_rows,
            head_lambda,
            head_gain,
            out_weight,
            expert_rows,
            expert_gain,
            routes,
            route_weights,
            gate_weight,
            up_weight,
            down_weight,
        )
    mixed = mixer_half(query_maps, key_maps, value_rows, head_lambda, head_gain, out_weight)
    expert_out = expert_half(
        expert_rows, expert_gain, routes, route_weights, gate_weight, up_weight, down_weight
    )
    return (mixed, expert_out)


def solution(mesh):
    placed = (
        P("ep", "tp"),
        P("ep", "tp"),
        P("ep", "tp"),
        P("tp"),
        P(),
        P("tp", None),
        P("ep", None),
        P(),
        P("ep", None),
        P("ep", None),
        P("ep", None, "tp"),
        P("ep", None, "tp"),
        P("ep", "tp", None),
    )
    return jax.shard_map(
        on_device,
        mesh=mesh,
        in_specs=placed,
        out_specs=(P("ep", "tp"), P("ep", "tp")),
        check_vma=False,
    )
```

```python
import functools

import jax
import jax.numpy as jnp
import numpy as np
from jax import lax
from jax.experimental import pallas as pl
from jax.experimental.pallas import tpu as pltpu
from jax.sharding import PartitionSpec as P

norm_eps = 1e-06
rope_base = 10000.0


def rope_turn(inputs, positions):
    half_dim = inputs.shape[-1] // 2
    inverse = rope_base ** (-2.0 * jnp.arange(half_dim, dtype=jnp.float32) / inputs.shape[-1])
    angles = positions.astype(jnp.float32)[:, None] * inverse[None, :]
    cos_table = jnp.cos(angles)[:, None, None, :]
    sin_table = jnp.sin(angles)[:, None, None, :]
    first_half = inputs[..., :half_dim]
    second_half = inputs[..., half_dim:]
    return jnp.concatenate(
        [
            first_half * cos_table - second_half * sin_table,
            second_half * cos_table + first_half * sin_table,
        ],
        axis=-1,
    )


def mixer_half(query_maps, key_maps, value_rows, head_lambda, head_gain, out_weight):
    row_count = query_maps.shape[0]
    head_count = head_lambda.shape[0]
    head_dim = query_maps.shape[1] // (2 * head_count)
    value_dim = value_rows.shape[1] // head_count
    model_width = out_weight.shape[1]
    score_scale = head_dim ** (-0.5)
    offset = lax.axis_index("ep") * row_count
    positions = offset + jnp.arange(row_count, dtype=jnp.int32)
    last_row = offset + row_count - 1
    rotated_q = rope_turn(
        query_maps.astype(jnp.float32).reshape(row_count, head_count, 2, head_dim), positions
    ).astype(jnp.bfloat16)
    rotated_k = rope_turn(
        key_maps.astype(jnp.float32).reshape(row_count, head_count, 2, head_dim), positions
    ).astype(jnp.bfloat16)
    rotated_k = rotated_k.reshape(row_count, head_count * 2 * head_dim)
    initial = (
        jnp.full((head_count, 2, row_count), -1e30, jnp.float32),
        jnp.zeros((head_count, 2, row_count), jnp.float32),
        jnp.zeros((head_count, 2, row_count, value_dim), jnp.float32),
    )
    piece_k = lax.all_gather(rotated_k, "ep", axis=0, tiled=True)
    piece_v = lax.all_gather(value_rows, "ep", axis=0, tiled=True)
    piece_len = piece_k.shape[0]
    block_size = 1024

    def attend(state):

        def fold_step(inner, block_index):
            block_start = block_index * block_size
            block_k = lax.dynamic_slice_in_dim(piece_k, block_start, block_size, 0).reshape(
                block_size, head_count, 2, head_dim
            )
            block_v = lax.dynamic_slice_in_dim(piece_v, block_start, block_size, 0).reshape(
                block_size, head_count, value_dim
            )
            scores = (
                jnp.einsum(
                    "qhmd,khmd->hmqk", rotated_q, block_k, preferred_element_type=jnp.float32
                )
                * score_scale
            )
            key_pos = block_start + jnp.arange(block_size, dtype=jnp.int32)
            causal = key_pos[None, :] <= positions[:, None]
            masked = jnp.where(causal, scores, -1e30)
            run_max, run_sum, run_acc = inner
            new_max = jnp.maximum(run_max, jnp.max(masked, axis=-1))
            expd = jnp.where(causal, jnp.exp(masked - new_max[..., None]), 0.0)
            rescale = jnp.exp(run_max - new_max)
            new_sum = run_sum * rescale + jnp.sum(expd, axis=-1)
            new_acc = run_acc * rescale[..., None] + jnp.einsum(
                "hmqk,khe->hmqe",
                expd.astype(jnp.bfloat16),
                block_v,
                preferred_element_type=jnp.float32,
            )
            return ((new_max, new_sum, new_acc), None)

        result, _ = lax.scan(fold_step, state, jnp.arange(piece_len // block_size, dtype=jnp.int32))
        return result

    def skip_piece(state):
        return state

    run_max, run_sum, run_acc = lax.cond(jnp.int32(0) <= last_row, attend, skip_piece, initial)
    first_map = run_acc[:, 0] / run_sum[:, 0][..., None]
    second_map = run_acc[:, 1] / run_sum[:, 1][..., None]
    difference = first_map - head_lambda[:, None, None] * second_map
    head_out = (
        difference
        * lax.rsqrt(jnp.mean(difference * difference, axis=-1, keepdims=True) + norm_eps)
        * head_gain
    ).astype(jnp.bfloat16)
    partial_value = jnp.einsum(
        "hqe,hed->qd",
        head_out,
        out_weight.reshape(head_count, value_dim, model_width),
        preferred_element_type=jnp.float32,
    )
    return lax.psum_scatter(
        partial_value.astype(jnp.bfloat16), "tp", scatter_dimension=1, tiled=True
    )


def expert_half(
    expert_rows, expert_gain, routes, route_weights, gate_weight, up_weight, down_weight
):
    ep_count = lax.axis_size("ep")
    tp_count = lax.axis_size("tp")
    row_count, model_width = expert_rows.shape
    pick_count = routes.shape[1]
    capacity = 3 * row_count * pick_count // (2 * ep_count)
    column_count = model_width // tp_count
    inputs = expert_rows.astype(jnp.float32)
    normed = (
        inputs
        * lax.rsqrt(jnp.mean(inputs * inputs, axis=-1, keepdims=True) + norm_eps)
        * expert_gain
    ).astype(jnp.bfloat16)
    expert_ids = routes.reshape(-1)
    one_hot = (expert_ids[:, None] == jnp.arange(ep_count, dtype=jnp.int32)[None, :]).astype(
        jnp.int32
    )
    slot_index = jnp.sum((jnp.cumsum(one_hot, axis=0) - one_hot) * one_hot, axis=1)
    source_row = jnp.arange(row_count * pick_count, dtype=jnp.int32) // pick_count
    empty = jnp.zeros((ep_count, capacity, normed.shape[1]), jnp.bfloat16)
    arrived = lax.all_to_all(
        empty.at[expert_ids, slot_index].set(normed[source_row]),
        "ep",
        split_axis=0,
        concat_axis=0,
        tiled=True,
    )
    slot_count = arrived.shape[1]
    flat_rows = arrived.reshape(ep_count * slot_count, model_width)
    gate_values = jnp.dot(flat_rows, gate_weight[0], preferred_element_type=jnp.float32)
    up_values = jnp.dot(flat_rows, up_weight[0], preferred_element_type=jnp.float32)
    hidden = (jax.nn.silu(gate_values) * up_values).astype(jnp.bfloat16)
    partial_value = jnp.dot(hidden, down_weight[0], preferred_element_type=jnp.float32).reshape(
        ep_count, slot_count, model_width
    )
    summed = lax.psum_scatter(
        partial_value.astype(jnp.bfloat16), "tp", scatter_dimension=2, tiled=True
    )
    returned = lax.all_to_all(summed, "ep", split_axis=0, concat_axis=0, tiled=True)
    picked = returned[expert_ids, slot_index].reshape(row_count, pick_count, column_count)
    combined = jnp.sum(route_weights[..., None] * picked.astype(jnp.float32), axis=1)
    return combined.astype(jnp.bfloat16)


MESH = pl.DeviceIdType.MESH


def remote(source, target, send_sem, recv_sem, device):
    return pltpu.make_async_remote_copy(
        src_ref=source,
        dst_ref=target,
        send_sem=send_sem,
        recv_sem=recv_sem,
        device_id=device,
        device_id_type=MESH,
    )


def layer_kernel(
    n_ep,
    n_tp,
    norm_gain_ref,
    routes_ref,
    route_weights_ref,
    offset_ref,
    lambda_ref,
    gain_ref,
    rows_hbm,
    query_hbm,
    key_hbm,
    value_hbm,
    turn_hbm,
    gate_hbm,
    up_hbm,
    down_hbm,
    weight_hbm,
    expert_ref,
    mixed_ref,
    rows_ref,
    query_ref,
    key_ref,
    value_ref,
    turn_ref,
    slots_ref,
    packed_q,
    packed_kv,
    own_q,
    own_kv,
    below_kv,
    lower_kv,
    upper_q,
    own_stat,
    upper_stat,
    low_stat,
    back_stat,
    own_maps,
    own_part,
    own_diff,
    low_part,
    low_diff,
    gathered,
    gate_vmem,
    up_vmem,
    down_vmem,
    hidden,
    partial,
    arrived,
    summed,
    returned,
    weight_vmem,
    heads,
    mixed_partial,
    mixed_arrived,
    mixed_sum,
    input_sem,
    weight_sem,
    local_sem,
    disp_send,
    disp_recv,
    gath_send,
    gath_recv,
    part_send,
    part_recv,
    ret_send,
    ret_recv,
    swap_send,
    swap_recv,
    below_send,
    below_recv,
    lower_send,
    lower_recv,
    upper_send,
    upper_recv,
    stat_send,
    stat_recv,
    back_send,
    back_recv,
    diff_send,
    diff_recv,
    cross_send,
    cross_recv,
    mixed_send,
    mixed_recv,
    hold_sem,
):
    ep = lax.axis_index("ep")
    tp = lax.axis_index("tp")
    n_z = n_ep // 2
    middle = n_z // 2
    z, core = ep // 2, lax.rem(ep, 2)
    odd = lax.rem(z, 2)
    asks = [z >= middle, odd == 1]
    host = [middle - 1, z - 1]
    seat = [lax.rem(z, middle), 0]
    partner = {"ep": ep + 1 - 2 * core}
    capacity, width = slots_ref.shape[1:]
    rows = n_ep * capacity
    head_count, row_count, head_width = packed_q.shape
    share = head_count // 2
    half = head_width // 2
    first = core * share
    weights = [
        pltpu.make_async_copy(gate_hbm, gate_vmem, weight_sem.at[0]),
        pltpu.make_async_copy(up_hbm, up_vmem, weight_sem.at[1]),
        pltpu.make_async_copy(down_hbm, down_vmem, weight_sem.at[2]),
        pltpu.make_async_copy(weight_hbm, weight_vmem, weight_sem.at[3]),
    ]
    inputs = [
        pltpu.make_async_copy(rows_hbm, rows_ref, input_sem.at[0]),
        pltpu.make_async_copy(turn_hbm, turn_ref, input_sem.at[1]),
        pltpu.make_async_copy(query_hbm, query_ref, input_sem.at[2]),
        pltpu.make_async_copy(key_hbm, key_ref, input_sem.at[3]),
        pltpu.make_async_copy(value_hbm, value_ref, input_sem.at[4]),
    ]
    for copy in inputs:
        copy.start()
    peers = [{"ep": lax.rem(ep + d, n_ep)} for d in range(1, n_ep)]
    peers += [{"tp": lax.rem(tp + d, n_tp)} for d in range(1, n_tp)]
    barrier = pltpu.get_barrier_semaphore()
    for device in peers:
        pl.semaphore_signal(barrier, inc=1, device_id=device, device_id_type=MESH)

    token_count = rows_ref.shape[0]
    picks = routes_ref.shape[0]
    inputs[0].wait()
    for copy in weights:
        copy.start()
    entries = rows_ref[...].astype(jnp.float32)
    inverse_norm = lax.rsqrt(jnp.mean(entries * entries, axis=1, keepdims=True) + norm_eps)
    own = pl.ds(pl.multiple_of(tp * width, width), width)
    normed = rows_ref[:, own].astype(jnp.float32) * inverse_norm * norm_gain_ref[:, own]
    normed = normed.astype(jnp.bfloat16)
    named_rows = -(-n_ep // 16) * 16
    label = lax.broadcasted_iota(jnp.int32, (named_rows, token_count), 0)
    named = [
        jnp.where(label == routes_ref[k : k + 1, :], 1.0, 0.0).astype(jnp.float32)
        for k in range(picks)
    ]
    before = lax.broadcasted_iota(jnp.int32, (token_count, token_count), 0)
    after = lax.broadcasted_iota(jnp.int32, (token_count, token_count), 1)
    earlier = jnp.dot(
        sum(named).astype(jnp.bfloat16),
        jnp.where(before < after, 1.0, 0.0).astype(jnp.bfloat16),
        preferred_element_type=jnp.float32,
    )
    slot_of = lax.broadcasted_iota(jnp.int32, (rows, token_count), 0)
    select = []
    for k in range(picks):
        rank = jnp.sum(named[k] * earlier, axis=0, keepdims=True).astype(jnp.int32)
        place = routes_ref[k : k + 1, :] * capacity + rank
        select.append(jnp.where(slot_of == place, 1.0, 0.0).astype(jnp.float32))
    slots_ref[...] = (
        jnp.dot(
            sum(select).astype(jnp.bfloat16), normed, preferred_element_type=jnp.float32
        )
        .astype(jnp.bfloat16)
        .reshape(n_ep, capacity, width)
    )
    with jax.named_scope("barrier"):
        pl.semaphore_wait(barrier, len(peers))
    across, along = tp + 1 - 2 * lax.rem(tp, 2), lax.rem(tp + 2, n_tp)
    corner = n_tp - 1 - tp
    dispatch = [pltpu.make_async_copy(slots_ref.at[ep], gathered.at[tp, 0], local_sem.at[0])]
    for d in range(1, n_ep):
        target = lax.rem(ep + d, n_ep)
        dispatch.append(
            remote(
                slots_ref.at[target],
                gathered.at[tp, d],
                disp_send.at[d],
                disp_recv.at[d],
                {"ep": target},
            )
        )
    for copy in dispatch:
        copy.start()

    for copy in inputs[1:]:
        copy.wait()
    cos_off, sin_off = offset_ref[0, pl.ds(ep, 1), :], offset_ref[1, pl.ds(ep, 1), :]
    cosine = turn_ref[0] * cos_off - turn_ref[1] * sin_off
    sine = turn_ref[1] * cos_off + turn_ref[0] * sin_off
    sine = jnp.where(lax.broadcasted_iota(jnp.int32, sine.shape, 1) < half // 2, -sine, sine)
    for head in range(head_count):
        for m in range(2):
            at = head * head_width + m * half
            to = slice(m * half, (m + 1) * half)
            for ref, packed in ((query_ref, packed_q), (key_ref, packed_kv)):
                entry = ref[:, at : at + half].astype(jnp.float32)
                turned = entry * cosine + pltpu.roll(entry, half // 2, 1) * sine
                packed[head, :, to] = turned.astype(jnp.bfloat16)
        packed_kv[head, :, head_width:] = value_ref[
            :, head * head_width : (head + 1) * head_width
        ]
    other = share - first
    swaps = []
    for j in range(share):
        swaps += [
            remote(
                packed_q.at[other + j],
                own_q.at[j, core],
                swap_send.at[0, j],
                swap_recv.at[0, j],
                partner,
            ),
            remote(
                packed_kv.at[other + j],
                own_kv.at[j, core],
                swap_send.at[1, j],
                swap_recv.at[1, j],
                partner,
            ),
        ]
    keeps = []
    for j in range(share):
        keeps += [
            pltpu.make_async_copy(packed_q.at[first + j], own_q.at[j, core], local_sem.at[3 + j]),
            pltpu.make_async_copy(
                packed_kv.at[first + j], own_kv.at[j, core], local_sem.at[3 + share + j]
            ),
        ]
    for copy in swaps + keeps:
        copy.start()

    def lift(side):
        return remote(
            packed_kv.at[side * share],
            below_kv.at[0, core],
            below_send.at[side],
            below_recv.at[core],
            {"ep": lax.rem(ep - core + 2 + side, n_ep)},
        )

    def lift_far(side):
        return remote(
            packed_kv.at[side * share + 1],
            lower_kv.at[0, 2 * lax.rem(z, middle) + core],
            lower_send.at[side],
            lower_recv.at[2 * lax.rem(z, middle) + core],
            {"ep": 2 * middle + side},
        )

    def ask(side, j):
        return remote(
            packed_q.at[side * share + j],
            upper_q.at[seat[j], core],
            upper_send.at[side, j],
            upper_recv.at[seat[j], core],
            {"ep": 2 * host[j] + side},
        )

    def wait_landed(ref, sem):
        pltpu.make_async_copy(ref, ref, sem).wait()

    def leave():
        for j in range(share):
            for side in range(2):

                @pl.when(asks[j])
                def _():
                    ask(side, j).start()

        for side in range(2):

            @pl.when(odd == 0)
            def _():
                lift(side).start()

        for side in range(2):

            @pl.when(z < middle)
            def _():
                lift_far(side).start()

    spread = []
    with jax.named_scope("wait_disp"):
        for d in range(n_ep):
            if d == 5:
                leave()
            if d == 0:
                dispatch[0].wait()
            else:
                dispatch[d].wait_recv()
            slot = gathered.at[tp, d]
            for way, device in enumerate((across, along)):
                copy = remote(
                    slot, slot, gath_send.at[way, d], gath_recv.at[way, d], {"tp": device}
                )
                copy.start()
                spread.append(copy)

    row = lax.broadcasted_iota(jnp.int32, (row_count, row_count), 0)
    column = lax.broadcasted_iota(jnp.int32, (row_count, row_count), 1)
    causal = column <= row
    wide = lax.broadcasted_iota(jnp.int32, (row_count, 2 * row_count), 0) + row_count
    wide_causal = lax.broadcasted_iota(jnp.int32, (row_count, 2 * row_count), 1) <= wide
    diagonal = column == row
    scale = half ** (-0.5)
    stat_row = lax.broadcasted_iota(jnp.int32, (8, row_count), 0)

    def as_column(values):
        return jnp.sum(jnp.where(diagonal, values, 0.0), axis=1, keepdims=True)

    def as_row(values):
        return jnp.sum(jnp.where(diagonal, values, 0.0), axis=0, keepdims=True)

    def as_stats(levels):
        return jnp.where(stat_row == 0, as_row(levels[0]), as_row(levels[1]))

    def head_weight(j):
        lanes = lax.broadcasted_iota(jnp.int32, lambda_ref.shape, 1)
        return jnp.sum(
            jnp.where(lanes == first + j, lambda_ref[...], 0.0), axis=1, keepdims=True
        )

    def fold(query_of, pieces, m):
        scores = []
        for keys_of, values_of, mask in pieces:
            piece = lax.dot_general(
                query_of(m), keys_of(m), (((1,), (1,)), ((), ())), preferred_element_type=jnp.float32
            )
            piece = piece * scale
            if mask is not None:
                piece = jnp.where(mask, piece, -1e30)
            scores.append(piece)
        peak = functools.reduce(
            jnp.maximum, [jnp.max(piece, axis=1, keepdims=True) for piece in scores]
        )
        total = jnp.zeros((row_count, 1), jnp.float32)
        outcome = jnp.zeros((row_count, head_width), jnp.float32)
        for piece, (keys_of, values_of, mask) in zip(scores, pieces):
            expd = jnp.exp(piece - peak)
            total += jnp.sum(expd, axis=1, keepdims=True)
            outcome += jnp.dot(
                expd.astype(jnp.bfloat16), values_of(), preferred_element_type=jnp.float32
            )
        return peak, total, outcome

    def piece_of(ref, j, count, mask):
        def keys_of(m):
            keys = ref[j, :count, :, m * half : (m + 1) * half]
            return keys.reshape(count * row_count, half)

        def values_of():
            return ref[j, :count, :, head_width:].reshape(count * row_count, head_width)

        return keys_of, values_of, mask

    def keep_diff(j, block, difference):
        @pl.when(core == block)
        def _():
            own_diff[first + j] = difference.astype(jnp.bfloat16)

        @pl.when(core != block)
        def _():
            own_part[j] = difference.astype(jnp.bfloat16)
            send_diff(j).start()

    def send_diff(j):
        return remote(
            own_part.at[j], own_diff.at[first + j], diff_send.at[j], diff_recv.at[first + j], partner
        )

    def send_stat(j):
        return remote(
            own_stat.at[j],
            upper_stat.at[seat[j]],
            stat_send.at[j],
            stat_recv.at[seat[j]],
            {"ep": 2 * host[j] + core},
        )

    def wait_own(j):
        swaps[2 * j].wait_recv()
        swaps[2 * j + 1].wait_recv()
        keeps[2 * j].wait()
        keeps[2 * j + 1].wait()

    def local_head(j, pieces):
        for block in range(2):
            mask = wide_causal if block else causal
            parts = pieces + [piece_of(own_kv, j, block + 1, mask)]
            maps, levels = [], []
            for m in range(2):
                peak, total, outcome = fold(
                    lambda m: own_q[j, block, :, m * half : (m + 1) * half], parts, m
                )
                maps.append(outcome / total)
                levels.append(peak + jnp.log(total))

            @pl.when(asks[j])
            def _():
                own_maps[j, block, 0] = maps[0]
                own_maps[j, block, 1] = maps[1]
                own_stat[j, block] = as_stats(levels)

            @pl.when(jnp.logical_not(asks[j]))
            def _():
                keep_diff(j, block, maps[0] - head_weight(j) * maps[1])

        @pl.when(asks[j])
        def _():
            send_stat(j).start()

    def send_cross(up, j, block, target):
        return remote(
            low_part.at[up, block],
            low_diff.at[first + j],
            cross_send.at[up, block],
            cross_recv.at[first + j],
            {"ep": 2 * target + block},
        )

    def send_back(up, j, block, target):
        return remote(
            low_stat.at[up, block],
            back_stat.at[j, block],
            back_send.at[up, block],
            back_recv.at[j, block],
            {"ep": 2 * target + core},
        )

    def cross_head(j, count, base, pieces):
        def step(index, carry):
            up, block = index // 2, lax.rem(index, 2)
            target = base + up
            wait_landed(upper_q.at[up, block], upper_recv.at[up, block])

            @pl.when(block == 0)
            def _():
                wait_landed(upper_stat.at[up], stat_recv.at[up])

            maps, levels = [], []
            for m in range(2):
                peak, total, outcome = fold(
                    lambda m: upper_q[up, block, :, m * half : (m + 1) * half], pieces, m
                )
                level = peak + jnp.log(total)
                above = as_column(upper_stat[up, block, m : m + 1, :])
                whole = jnp.maximum(level, above) + jnp.log(1.0 + jnp.exp(-jnp.abs(level - above)))
                maps.append(outcome * jnp.exp(peak - whole))
                levels.append(level)
            low_stat[up, block] = as_stats(levels)
            send_back(up, j, block, target).start()
            low_part[up, block] = (maps[0] - head_weight(j) * maps[1]).astype(jnp.bfloat16)
            send_cross(up, j, block, target).start()
            return carry

        lax.fori_loop(0, 2 * count, step, 0)

    def finish_upper(j):
        for block in range(2):
            wait_landed(back_stat.at[j, block], back_recv.at[j, block])
            maps = []
            for m in range(2):
                below = as_column(back_stat[j, block, m : m + 1, :])
                level = as_column(own_stat[j, block, m : m + 1, :])
                maps.append(own_maps[j, block, m] / (1.0 + jnp.exp(below - level)))
            keep_diff(j, block, maps[0] - head_weight(j) * maps[1])

    below_piece = piece_of(below_kv, 0, 2, None)
    lower_piece = piece_of(lower_kv, 0, 2 * middle, None)

    @pl.when(z != middle)
    def _():
        with jax.named_scope("own1"):
            wait_own(1)
            local_head(1, [])

    @pl.when(odd == 0)
    def _():
        with jax.named_scope("own0"):
            wait_own(0)
            local_head(0, [])

    with jax.named_scope("forward"):
        for d in range(n_ep):
            way = d % 2
            slot = gathered.at[(across, along)[way], d]
            wait_landed(slot, gath_recv.at[way, d])
            copy = remote(
                slot, slot, gath_send.at[2, d], gath_recv.at[2, d], {"tp": (along, across)[way]}
            )
            copy.start()
            spread.append(copy)
    tile = 256
    part_count = n_ep // 2
    part_rows = part_count * capacity
    scatter = []
    for part in range(2):
        lead = part * part_count
        with jax.named_scope(f"wait_gath#p={part}"):
            for d in range(lead, lead + part_count):
                way = 1 - d % 2
                wait_landed(gathered.at[(across, along)[way], d], gath_recv.at[way, d])
                wait_landed(gathered.at[corner, d], gath_recv.at[2, d])
        if part == 0:
            weights[0].wait()
            weights[1].wait()

        def hidden_tile(j, carry):
            columns = pl.ds(pl.multiple_of(j * tile, tile), tile)
            gate = jnp.zeros((part_rows, tile), jnp.float32)
            up = jnp.zeros((part_rows, tile), jnp.float32)
            for i in range(n_tp):
                block = gathered[i, lead : lead + part_count].reshape(part_rows, width)
                gate += jnp.dot(
                    block,
                    gate_vmem[0, i * width : (i + 1) * width, columns],
                    preferred_element_type=jnp.float32,
                )
                up += jnp.dot(
                    block,
                    up_vmem[0, i * width : (i + 1) * width, columns],
                    preferred_element_type=jnp.float32,
                )
            hidden[part, :, columns] = (gate / (1.0 + jnp.exp(-gate)) * up).astype(jnp.bfloat16)
            return carry

        with jax.named_scope(f"gateup#p={part}"):
            lax.fori_loop(0, hidden.shape[2] // tile, hidden_tile, 0)
        if part == 0:
            weights[2].wait()
        with jax.named_scope(f"down#p={part}"):
            for d in list(range(1, n_tp)) + [0]:
                target = lax.rem(tp + d, n_tp)
                columns = pl.ds(pl.multiple_of(target * width, width), width)
                partial[part, d] = jnp.dot(
                    hidden[part], down_vmem[0, :, columns], preferred_element_type=jnp.float32
                ).astype(jnp.bfloat16)
                if d:
                    copy = remote(
                        partial.at[part, d],
                        arrived.at[part, d],
                        part_send.at[part, d],
                        part_recv.at[part, d],
                        {"tp": target},
                    )
                    copy.start()
                    scatter.append(copy)

    @pl.when(odd == 1)
    def _():
        with jax.named_scope("odd0"):
            for source in range(2):
                wait_landed(below_kv.at[0, source], below_recv.at[source])
            wait_own(0)
            local_head(0, [below_piece])

    @pl.when(z == 0)
    def _():
        with jax.named_scope("cross0"):
            cross_head(1, 1, 1, [piece_of(own_kv, 1, 2, None)])

    @pl.when(z == middle - 1)
    def _():
        with jax.named_scope("cross1"):
            cross_head(0, middle, middle, [below_piece, piece_of(own_kv, 0, 2, None)])

    def project():
        with jax.named_scope("wait_heads"):
            for j in range(share):
                wait_landed(own_diff.at[other + j], diff_recv.at[other + j])

                @pl.when(asks[j])
                def _():
                    for side in range(2):
                        at = side * share + j
                        wait_landed(low_diff.at[at], cross_recv.at[at])

        for head in range(head_count):
            difference = own_diff[head].astype(jnp.float32) + low_diff[head].astype(jnp.float32)
            mean = jnp.mean(difference * difference, axis=1, keepdims=True)
            heads[head] = (difference * lax.rsqrt(mean + norm_eps) * gain_ref[...]).astype(
                jnp.bfloat16
            )
        weights[3].wait()
        for role, target in ((3, corner), (1, across), (2, along), (0, tp)):
            columns = pl.ds(pl.multiple_of(target * width, width), width)
            product = jnp.zeros((row_count, width), jnp.float32)
            for h in range(head_count):
                product += jnp.dot(
                    heads[h],
                    weight_vmem[h * head_width : (h + 1) * head_width, columns],
                    preferred_element_type=jnp.float32,
                )
            mixed_partial[role] = product.astype(jnp.bfloat16).reshape(
                2, row_count // 2, width
            )
            for part in range(2):
                if role == 3:
                    mixed_copy(1, part).start()
                elif role == 1 + part:
                    mixed_copy(0, part).start()

    ways = (across, along)

    def mixed_copy(kind, part):
        return remote(
            (mixed_partial.at[1 + part, part], mixed_partial.at[3, part], mixed_sum.at[part])[kind],
            mixed_arrived.at[kind, part],
            mixed_send.at[kind, part],
            mixed_recv.at[kind, part],
            {"tp": ways[1 - part if kind == 2 else part]},
        )

    def mixed_forward():
        with jax.named_scope("mixed_forward"):
            for part in range(2):
                mixed_copy(1, part).wait_recv()
                both = mixed_partial[2 - part, part].astype(jnp.float32)
                both += mixed_arrived[1, part].astype(jnp.float32)
                mixed_sum[part] = both.astype(jnp.bfloat16)
                mixed_copy(2, part).start()

    back = []
    for d in range(n_ep):
        if d == 0:
            copy = pltpu.make_async_copy(summed.at[0], returned.at[ep], local_sem.at[2])
        else:
            copy = remote(
                summed.at[d],
                returned.at[ep],
                ret_send.at[d],
                ret_recv.at[d],
                {"ep": lax.rem(ep + n_ep - d, n_ep)},
            )
        back.append(copy)

    def sum_part(part):
        lead = part * part_count
        total = partial[part, 0].astype(jnp.float32)
        with jax.named_scope(f"wait_part#p={part}"):
            for d in range(1, n_tp):
                scatter[part * (n_tp - 1) + d - 1].wait_recv()
                total += arrived[part, d].astype(jnp.float32)
        summed[lead : lead + part_count] = total.astype(jnp.bfloat16).reshape(
            part_count, capacity, width
        )

    for j in range(share):

        @pl.when(jnp.logical_not(asks[j]))
        def _():
            for side in range(2):
                low_diff[side * share + j] = jnp.zeros((row_count, head_width), jnp.bfloat16)

    @pl.when(z == middle - 1)
    def _():
        with jax.named_scope("finish"):
            finish_upper(1)

    @pl.when(z < middle)
    def _():
        with jax.named_scope("project_low"):
            project()

    sum_part(0)

    @pl.when(z < middle)
    def _():
        mixed_forward()

    @pl.when(z >= middle)
    def _():
        for copy in back[:part_count]:
            copy.start()

    @pl.when(z == middle)
    def _():
        with jax.named_scope("cross2"):
            for source in range(2 * middle):
                wait_landed(lower_kv.at[0, source], lower_recv.at[source])
            wait_own(1)
            cross_head(1, 1, middle + 1, [lower_piece, piece_of(own_kv, 1, 2, None)])
            local_head(1, [lower_piece])

    sum_part(1)

    def release():
        pl.semaphore_signal(
            hold_sem,
            inc=1,
            device_id={"ep": lax.rem(ep + n_ep - 2, n_ep)},
            device_id_type=MESH,
        )

    @pl.when(z < middle)
    def _():
        targets = [lax.rem(ep + n_ep - d, n_ep) for d in range(n_ep)]
        for target, copy in zip(targets, back):

            @pl.when(target < 2 * middle)
            def _():
                copy.start()

        with jax.named_scope("hold"):

            @pl.when(z == middle - 1)
            def _():
                for up in range(middle):
                    for side in range(2):
                        send_cross(up, 0, side, middle + up).wait_send()
                pl.semaphore_wait(hold_sem, 1)
                release()

            @pl.when(z != middle - 1)
            def _():
                pl.semaphore_wait(hold_sem, 1)

        for target, copy in zip(targets, back):

            @pl.when(target >= 2 * middle)
            def _():
                copy.start()

    @pl.when(z >= middle)
    def _():
        @pl.when(z != middle)
        def _():
            for copy in back[part_count:]:
                copy.start()

        with jax.named_scope("finish"):
            finish_upper(0)

        @pl.when(odd == 1)
        def _():
            with jax.named_scope("finish"):
                finish_upper(1)

        with jax.named_scope("project_up"):
            project()

        @pl.when(z == middle)
        def _():
            with jax.named_scope("held"):
                for side in range(2):
                    send_cross(0, 1, side, middle + 1).wait_send()
            release()
            for copy in back[part_count:]:
                copy.start()

        mixed_forward()

    with jax.named_scope("wait_back"):
        back[0].wait()
        for copy in back[1:]:
            copy.wait_recv()
    flat = returned[...].reshape(rows, width)
    result = jnp.zeros(expert_ref.shape, jnp.float32)
    for k in range(picks):
        picked = lax.dot_general(
            select[k].astype(jnp.bfloat16),
            flat,
            (((0,), (0,)), ((), ())),
            preferred_element_type=jnp.float32,
        )
        spread_out = jnp.where(before == after, route_weights_ref[k : k + 1, :], 0.0)
        result += jnp.sum(spread_out, axis=1, keepdims=True) * picked
    expert_ref[...] = result.astype(expert_ref.dtype)
    with jax.named_scope("wait_mixed"):
        for part in range(2):
            total = mixed_partial[0, part].astype(jnp.float32)
            for kind in (0, 2):
                mixed_copy(kind, part).wait_recv()
                total += mixed_arrived[kind, part].astype(jnp.float32)
            lines = slice(part * row_count // 2, (part + 1) * row_count // 2)
            mixed_ref[lines, :] = total.astype(jnp.bfloat16)
    for copy in dispatch[1:] + swaps + spread + scatter + back[1:]:
        copy.wait_send()
    for kind in range(3):
        for part in range(2):
            mixed_copy(kind, part).wait_send()
    for j in range(share):
        send_diff(j).wait_send()

        @pl.when(asks[j])
        def _():
            send_stat(j).wait_send()
            for side in range(2):
                ask(side, j).wait_send()

    for side in range(2):

        @pl.when(odd == 0)
        def _():
            lift(side).wait_send()

        @pl.when(z < middle)
        def _():
            lift_far(side).wait_send()

        @pl.when(z <= middle)
        def _():
            send_back(0, 0, side, z + 1).wait_send()

            @pl.when(z < middle - 1)
            def _():
                send_cross(0, 0, side, z + 1).wait_send()

        @pl.when(z == middle - 1)
        def _():
            send_back(1, 0, side, z + 2).wait_send()


def hand_over(expert_ref, mixed_ref, expert_out, mixed_out):
    expert_out[...] = expert_ref[...]
    mixed_out[...] = mixed_ref[...]


def fused(
    query_maps,
    key_maps,
    value_rows,
    head_lambda,
    head_gain,
    out_weight,
    expert_rows,
    expert_gain,
    routes,
    route_weights,
    gate_weight,
    up_weight,
    down_weight,
):
    n_ep = lax.axis_size("ep")
    n_tp = lax.axis_size("tp")
    n_z = n_ep // 2
    row_count = query_maps.shape[0]
    head_width = query_maps.shape[1] // n_z
    head_dim = head_width // 2
    token_count, model_width = expert_rows.shape
    capacity = 3 * token_count * routes.shape[1] // (2 * n_ep)
    width = model_width // n_tp
    hidden_width = gate_weight.shape[2]
    slot_rows = n_ep * capacity

    half_dim = head_dim // 2
    inverse = rope_base ** (-2.0 * np.arange(half_dim) / head_dim)
    inverse = np.concatenate([inverse, inverse])
    turns = np.arange(row_count)[:, None] * inverse
    offsets = (row_count * np.arange(n_ep))[:, None] * inverse
    turns = jnp.asarray(np.stack([np.cos(turns), np.sin(turns)]), jnp.float32)
    offsets = jnp.asarray(np.stack([np.cos(offsets), np.sin(offsets)]), jnp.float32)

    vmem = pl.BlockSpec(memory_space=pltpu.VMEM)
    hbm = pl.BlockSpec(memory_space=pl.ANY)
    dma = pltpu.SemaphoreType.DMA
    bf16, f32 = jnp.bfloat16, jnp.float32
    share = n_z // 2
    expert_out, mixed = pl.pallas_call(
        functools.partial(layer_kernel, n_ep, n_tp),
        out_shape=(
            jax.ShapeDtypeStruct((token_count, width), bf16),
            jax.ShapeDtypeStruct((row_count, width), bf16),
        ),
        in_specs=[vmem] * 6 + [hbm] * 9,
        out_specs=(vmem, vmem),
        scratch_shapes=[
            pltpu.VMEM(expert_rows.shape, bf16),
            pltpu.VMEM(query_maps.shape, bf16),
            pltpu.VMEM(key_maps.shape, bf16),
            pltpu.VMEM(value_rows.shape, bf16),
            pltpu.VMEM(turns.shape, f32),
            pltpu.VMEM((n_ep, capacity, width), bf16),
            pltpu.VMEM((n_z, row_count, head_width), bf16),
            pltpu.VMEM((n_z, row_count, 2 * head_width), bf16),
            pltpu.VMEM((share, 2, row_count, head_width), bf16),
            pltpu.VMEM((share, 2, row_count, 2 * head_width), bf16),
            pltpu.VMEM((1, 2, row_count, 2 * head_width), bf16),
            pltpu.VMEM((1, n_z, row_count, 2 * head_width), bf16),
            pltpu.VMEM((share, 2, row_count, head_width), bf16),
            pltpu.VMEM((share, 2, 8, row_count), f32),
            pltpu.VMEM((share, 2, 8, row_count), f32),
            pltpu.VMEM((share, 2, 8, row_count), f32),
            pltpu.VMEM((share, 2, 8, row_count), f32),
            pltpu.VMEM((share, 2, 2, row_count, head_width), f32),
            pltpu.VMEM((share, row_count, head_width), bf16),
            pltpu.VMEM((n_z, row_count, head_width), bf16),
            pltpu.VMEM((share, 2, row_count, head_width), bf16),
            pltpu.VMEM((n_z, row_count, head_width), bf16),
            pltpu.VMEM((n_tp, n_ep, capacity, width), bf16),
            pltpu.VMEM(gate_weight.shape, bf16),
            pltpu.VMEM(up_weight.shape, bf16),
            pltpu.VMEM(down_weight.shape, bf16),
            pltpu.VMEM((2, slot_rows // 2, hidden_width), bf16),
            pltpu.VMEM((2, n_tp, slot_rows // 2, width), bf16),
            pltpu.VMEM((2, n_tp, slot_rows // 2, width), bf16),
            pltpu.VMEM((n_ep, capacity, width), bf16),
            pltpu.VMEM((n_ep, capacity, width), bf16),
            pltpu.VMEM(out_weight.shape, bf16),
            pltpu.VMEM((n_z, row_count, head_width), bf16),
            pltpu.VMEM((n_tp, 2, row_count // 2, width), bf16),
            pltpu.VMEM((3, 2, row_count // 2, width), bf16),
            pltpu.VMEM((2, row_count // 2, width), bf16),
            dma((5,)),
            dma((4,)),
            dma((3 + n_z,)),
            dma((n_ep,)),
            dma((n_ep,)),
            dma((3, n_ep)),
            dma((3, n_ep)),
            dma((2, n_tp)),
            dma((2, n_tp)),
            dma((n_ep,)),
            dma((n_ep,)),
            dma((2, share)),
            dma((2, share)),
            dma((2,)),
            dma((2,)),
            dma((2,)),
            dma((n_z,)),
            dma((2, share)),
            dma((share, 2)),
            dma((share,)),
            dma((share,)),
            dma((share, 2)),
            dma((share, 2)),
            dma((share,)),
            dma((n_z,)),
            dma((share, 2)),
            dma((n_z,)),
            dma((3, 2)),
            dma((3, 2)),
            pltpu.SemaphoreType.REGULAR,
        ],
        compiler_params=pltpu.CompilerParams(
            collective_id=0, has_side_effects=True, vmem_limit_bytes=60 * 1024 * 1024
        ),
        name="layer",
    )(
        expert_gain.reshape(1, model_width),
        routes.T,
        route_weights.T,
        offsets,
        head_lambda.reshape(1, n_z),
        head_gain.reshape(1, head_width),
        expert_rows,
        query_maps,
        key_maps,
        value_rows,
        turns,
        gate_weight,
        up_weight,
        down_weight,
        out_weight,
    )
    expert_out, mixed = pl.pallas_call(
        hand_over,
        out_shape=(
            jax.ShapeDtypeStruct((token_count, width), bf16),
            jax.ShapeDtypeStruct((row_count, width), bf16),
        ),
        in_specs=[vmem] * 2,
        out_specs=(vmem, vmem),
        name="hand_over",
    )(expert_out, mixed)
    return (mixed, expert_out)


def on_device(
    query_maps,
    key_maps,
    value_rows,
    head_lambda,
    head_gain,
    out_weight,
    expert_rows,
    expert_gain,
    routes,
    route_weights,
    gate_weight,
    up_weight,
    down_weight,
):
    n_ep = lax.axis_size("ep")
    head_count = head_lambda.shape[0]
    capacity = 3 * expert_rows.shape[0] * routes.shape[1] // (2 * n_ep)
    if (
        2 * head_count == n_ep
        and head_count == lax.axis_size("tp") == 4
        and capacity % 16 == 0
        and value_rows.shape[1] == query_maps.shape[1] == 256 * head_count
    ):
        return fused(
            query_maps,
            key_maps,
            value_rows,
            head_lambda,
            head_gain,
            out_weight,
            expert_rows,
            expert_gain,
            routes,
            route_weights,
            gate_weight,
            up_weight,
            down_weight,
        )
    mixed = mixer_half(query_maps, key_maps, value_rows, head_lambda, head_gain, out_weight)
    expert_out = expert_half(
        expert_rows, expert_gain, routes, route_weights, gate_weight, up_weight, down_weight
    )
    return (mixed, expert_out)


def solution(mesh):
    placed = (
        P("ep", "tp"),
        P("ep", "tp"),
        P("ep", "tp"),
        P("tp"),
        P(),
        P("tp", None),
        P("ep", None),
        P(),
        P("ep", None),
        P("ep", None),
        P("ep", None, "tp"),
        P("ep", None, "tp"),
        P("ep", "tp", None),
    )
    return jax.shard_map(
        on_device,
        mesh=mesh,
        in_specs=placed,
        out_specs=(P("ep", "tp"), P("ep", "tp")),
        check_vma=False,
    )
```

```python
import functools

import jax
import jax.numpy as jnp
import numpy as np
from jax import lax
from jax.experimental import pallas as pl
from jax.experimental.pallas import tpu as pltpu
from jax.sharding import PartitionSpec as P

norm_eps = 1e-06
rope_base = 10000.0


def rope_turn(inputs, positions):
    half_dim = inputs.shape[-1] // 2
    inverse = rope_base ** (-2.0 * jnp.arange(half_dim, dtype=jnp.float32) / inputs.shape[-1])
    angles = positions.astype(jnp.float32)[:, None] * inverse[None, :]
    cos_table = jnp.cos(angles)[:, None, None, :]
    sin_table = jnp.sin(angles)[:, None, None, :]
    first_half = inputs[..., :half_dim]
    second_half = inputs[..., half_dim:]
    return jnp.concatenate(
        [
            first_half * cos_table - second_half * sin_table,
            second_half * cos_table + first_half * sin_table,
        ],
        axis=-1,
    )


def mixer_half(query_maps, key_maps, value_rows, head_lambda, head_gain, out_weight):
    row_count = query_maps.shape[0]
    head_count = head_lambda.shape[0]
    head_dim = query_maps.shape[1] // (2 * head_count)
    value_dim = value_rows.shape[1] // head_count
    model_width = out_weight.shape[1]
    score_scale = head_dim ** (-0.5)
    offset = lax.axis_index("ep") * row_count
    positions = offset + jnp.arange(row_count, dtype=jnp.int32)
    last_row = offset + row_count - 1
    rotated_q = rope_turn(
        query_maps.astype(jnp.float32).reshape(row_count, head_count, 2, head_dim), positions
    ).astype(jnp.bfloat16)
    rotated_k = rope_turn(
        key_maps.astype(jnp.float32).reshape(row_count, head_count, 2, head_dim), positions
    ).astype(jnp.bfloat16)
    rotated_k = rotated_k.reshape(row_count, head_count * 2 * head_dim)
    initial = (
        jnp.full((head_count, 2, row_count), -1e30, jnp.float32),
        jnp.zeros((head_count, 2, row_count), jnp.float32),
        jnp.zeros((head_count, 2, row_count, value_dim), jnp.float32),
    )
    piece_k = lax.all_gather(rotated_k, "ep", axis=0, tiled=True)
    piece_v = lax.all_gather(value_rows, "ep", axis=0, tiled=True)
    piece_len = piece_k.shape[0]
    block_size = 1024

    def attend(state):

        def fold_step(inner, block_index):
            block_start = block_index * block_size
            block_k = lax.dynamic_slice_in_dim(piece_k, block_start, block_size, 0).reshape(
                block_size, head_count, 2, head_dim
            )
            block_v = lax.dynamic_slice_in_dim(piece_v, block_start, block_size, 0).reshape(
                block_size, head_count, value_dim
            )
            scores = (
                jnp.einsum(
                    "qhmd,khmd->hmqk", rotated_q, block_k, preferred_element_type=jnp.float32
                )
                * score_scale
            )
            key_pos = block_start + jnp.arange(block_size, dtype=jnp.int32)
            causal = key_pos[None, :] <= positions[:, None]
            masked = jnp.where(causal, scores, -1e30)
            run_max, run_sum, run_acc = inner
            new_max = jnp.maximum(run_max, jnp.max(masked, axis=-1))
            expd = jnp.where(causal, jnp.exp(masked - new_max[..., None]), 0.0)
            rescale = jnp.exp(run_max - new_max)
            new_sum = run_sum * rescale + jnp.sum(expd, axis=-1)
            new_acc = run_acc * rescale[..., None] + jnp.einsum(
                "hmqk,khe->hmqe",
                expd.astype(jnp.bfloat16),
                block_v,
                preferred_element_type=jnp.float32,
            )
            return ((new_max, new_sum, new_acc), None)

        result, _ = lax.scan(fold_step, state, jnp.arange(piece_len // block_size, dtype=jnp.int32))
        return result

    def skip_piece(state):
        return state

    run_max, run_sum, run_acc = lax.cond(jnp.int32(0) <= last_row, attend, skip_piece, initial)
    first_map = run_acc[:, 0] / run_sum[:, 0][..., None]
    second_map = run_acc[:, 1] / run_sum[:, 1][..., None]
    difference = first_map - head_lambda[:, None, None] * second_map
    head_out = (
        difference
        * lax.rsqrt(jnp.mean(difference * difference, axis=-1, keepdims=True) + norm_eps)
        * head_gain
    ).astype(jnp.bfloat16)
    partial_value = jnp.einsum(
        "hqe,hed->qd",
        head_out,
        out_weight.reshape(head_count, value_dim, model_width),
        preferred_element_type=jnp.float32,
    )
    return lax.psum_scatter(
        partial_value.astype(jnp.bfloat16), "tp", scatter_dimension=1, tiled=True
    )


def expert_half(
    expert_rows, expert_gain, routes, route_weights, gate_weight, up_weight, down_weight
):
    ep_count = lax.axis_size("ep")
    tp_count = lax.axis_size("tp")
    row_count, model_width = expert_rows.shape
    pick_count = routes.shape[1]
    capacity = 3 * row_count * pick_count // (2 * ep_count)
    column_count = model_width // tp_count
    inputs = expert_rows.astype(jnp.float32)
    normed = (
        inputs
        * lax.rsqrt(jnp.mean(inputs * inputs, axis=-1, keepdims=True) + norm_eps)
        * expert_gain
    ).astype(jnp.bfloat16)
    expert_ids = routes.reshape(-1)
    one_hot = (expert_ids[:, None] == jnp.arange(ep_count, dtype=jnp.int32)[None, :]).astype(
        jnp.int32
    )
    slot_index = jnp.sum((jnp.cumsum(one_hot, axis=0) - one_hot) * one_hot, axis=1)
    source_row = jnp.arange(row_count * pick_count, dtype=jnp.int32) // pick_count
    empty = jnp.zeros((ep_count, capacity, normed.shape[1]), jnp.bfloat16)
    arrived = lax.all_to_all(
        empty.at[expert_ids, slot_index].set(normed[source_row]),
        "ep",
        split_axis=0,
        concat_axis=0,
        tiled=True,
    )
    slot_count = arrived.shape[1]
    flat_rows = arrived.reshape(ep_count * slot_count, model_width)
    gate_values = jnp.dot(flat_rows, gate_weight[0], preferred_element_type=jnp.float32)
    up_values = jnp.dot(flat_rows, up_weight[0], preferred_element_type=jnp.float32)
    hidden = (jax.nn.silu(gate_values) * up_values).astype(jnp.bfloat16)
    partial_value = jnp.dot(hidden, down_weight[0], preferred_element_type=jnp.float32).reshape(
        ep_count, slot_count, model_width
    )
    summed = lax.psum_scatter(
        partial_value.astype(jnp.bfloat16), "tp", scatter_dimension=2, tiled=True
    )
    returned = lax.all_to_all(summed, "ep", split_axis=0, concat_axis=0, tiled=True)
    picked = returned[expert_ids, slot_index].reshape(row_count, pick_count, column_count)
    combined = jnp.sum(route_weights[..., None] * picked.astype(jnp.float32), axis=1)
    return combined.astype(jnp.bfloat16)


MESH = pl.DeviceIdType.MESH


def remote(source, target, send_sem, recv_sem, device):
    return pltpu.make_async_remote_copy(
        src_ref=source,
        dst_ref=target,
        send_sem=send_sem,
        recv_sem=recv_sem,
        device_id=device,
        device_id_type=MESH,
    )


def layer_kernel(
    n_ep,
    n_tp,
    norm_gain_ref,
    routes_ref,
    route_weights_ref,
    offset_ref,
    lambda_ref,
    gain_ref,
    rows_hbm,
    query_hbm,
    key_hbm,
    value_hbm,
    turn_hbm,
    gate_hbm,
    up_hbm,
    down_hbm,
    weight_hbm,
    expert_ref,
    mixed_ref,
    rows_ref,
    query_ref,
    key_ref,
    value_ref,
    turn_ref,
    slots_ref,
    packed_q,
    packed_kv,
    own_q,
    own_kv,
    below_kv,
    lower_kv,
    upper_q,
    own_stat,
    upper_stat,
    low_stat,
    back_stat,
    own_maps,
    own_part,
    own_diff,
    low_part,
    low_diff,
    gathered,
    gate_vmem,
    up_vmem,
    down_vmem,
    hidden,
    partial,
    arrived,
    summed,
    returned,
    weight_vmem,
    heads,
    mixed_partial,
    mixed_arrived,
    mixed_sum,
    input_sem,
    weight_sem,
    local_sem,
    disp_send,
    disp_recv,
    gath_send,
    gath_recv,
    part_send,
    part_recv,
    ret_send,
    ret_recv,
    swap_send,
    swap_recv,
    below_send,
    below_recv,
    lower_send,
    lower_recv,
    upper_send,
    upper_recv,
    stat_send,
    stat_recv,
    back_send,
    back_recv,
    diff_send,
    diff_recv,
    cross_send,
    cross_recv,
    mixed_send,
    mixed_recv,
    hold_sem,
):
    ep = lax.axis_index("ep")
    tp = lax.axis_index("tp")
    n_z = n_ep // 2
    middle = n_z // 2
    z, core = ep // 2, lax.rem(ep, 2)
    odd = lax.rem(z, 2)
    asks = [z >= middle, odd == 1]
    host = [middle - 1, z - 1]
    seat = [lax.rem(z, middle), 0]
    partner = {"ep": ep + 1 - 2 * core}
    capacity, width = slots_ref.shape[1:]
    rows = n_ep * capacity
    head_count, row_count, head_width = packed_q.shape
    share = head_count // 2
    half = head_width // 2
    first = core * share
    weights = [
        pltpu.make_async_copy(gate_hbm, gate_vmem, weight_sem.at[0]),
        pltpu.make_async_copy(up_hbm, up_vmem, weight_sem.at[1]),
        pltpu.make_async_copy(down_hbm, down_vmem, weight_sem.at[2]),
        pltpu.make_async_copy(weight_hbm, weight_vmem, weight_sem.at[3]),
    ]
    inputs = [
        pltpu.make_async_copy(rows_hbm, rows_ref, input_sem.at[0]),
        pltpu.make_async_copy(turn_hbm, turn_ref, input_sem.at[1]),
        pltpu.make_async_copy(query_hbm, query_ref, input_sem.at[2]),
        pltpu.make_async_copy(key_hbm, key_ref, input_sem.at[3]),
        pltpu.make_async_copy(value_hbm, value_ref, input_sem.at[4]),
    ]
    for copy in inputs:
        copy.start()
    peers = [{"ep": lax.rem(ep + d, n_ep)} for d in range(1, n_ep)]
    peers += [{"tp": lax.rem(tp + d, n_tp)} for d in range(1, n_tp)]
    barrier = pltpu.get_barrier_semaphore()
    for device in peers:
        pl.semaphore_signal(barrier, inc=1, device_id=device, device_id_type=MESH)

    token_count = rows_ref.shape[0]
    picks = routes_ref.shape[0]
    inputs[0].wait()
    for copy in weights:
        copy.start()
    entries = rows_ref[...].astype(jnp.float32)
    inverse_norm = lax.rsqrt(jnp.mean(entries * entries, axis=1, keepdims=True) + norm_eps)
    own = pl.ds(pl.multiple_of(tp * width, width), width)
    normed = rows_ref[:, own].astype(jnp.float32) * inverse_norm * norm_gain_ref[:, own]
    normed = normed.astype(jnp.bfloat16)
    named_rows = -(-n_ep // 16) * 16
    label = lax.broadcasted_iota(jnp.int32, (named_rows, token_count), 0)
    named = [
        jnp.where(label == routes_ref[k : k + 1, :], 1.0, 0.0).astype(jnp.float32)
        for k in range(picks)
    ]
    before = lax.broadcasted_iota(jnp.int32, (token_count, token_count), 0)
    after = lax.broadcasted_iota(jnp.int32, (token_count, token_count), 1)
    earlier = jnp.dot(
        sum(named).astype(jnp.bfloat16),
        jnp.where(before < after, 1.0, 0.0).astype(jnp.bfloat16),
        preferred_element_type=jnp.float32,
    )
    slot_of = lax.broadcasted_iota(jnp.int32, (rows, token_count), 0)
    select = []
    for k in range(picks):
        rank = jnp.sum(named[k] * earlier, axis=0, keepdims=True).astype(jnp.int32)
        place = routes_ref[k : k + 1, :] * capacity + rank
        select.append(jnp.where(slot_of == place, 1.0, 0.0).astype(jnp.float32))
    slots_ref[...] = (
        jnp.dot(
            sum(select).astype(jnp.bfloat16), normed, preferred_element_type=jnp.float32
        )
        .astype(jnp.bfloat16)
        .reshape(n_ep, capacity, width)
    )
    with jax.named_scope("barrier"):
        pl.semaphore_wait(barrier, len(peers))
    across, along = tp + 1 - 2 * lax.rem(tp, 2), lax.rem(tp + 2, n_tp)
    corner = n_tp - 1 - tp
    dispatch = [pltpu.make_async_copy(slots_ref.at[ep], gathered.at[tp, 0], local_sem.at[0])]
    for d in range(1, n_ep):
        target = lax.rem(ep + d, n_ep)
        dispatch.append(
            remote(
                slots_ref.at[target],
                gathered.at[tp, d],
                disp_send.at[d],
                disp_recv.at[d],
                {"ep": target},
            )
        )
    for copy in dispatch:
        copy.start()

    for copy in inputs[1:]:
        copy.wait()
    cos_off, sin_off = offset_ref[0, pl.ds(ep, 1), :], offset_ref[1, pl.ds(ep, 1), :]
    cosine = turn_ref[0] * cos_off - turn_ref[1] * sin_off
    sine = turn_ref[1] * cos_off + turn_ref[0] * sin_off
    sine = jnp.where(lax.broadcasted_iota(jnp.int32, sine.shape, 1) < half // 2, -sine, sine)
    for head in range(head_count):
        for m in range(2):
            at = head * head_width + m * half
            to = slice(m * half, (m + 1) * half)
            for ref, packed in ((query_ref, packed_q), (key_ref, packed_kv)):
                entry = ref[:, at : at + half].astype(jnp.float32)
                turned = entry * cosine + pltpu.roll(entry, half // 2, 1) * sine
                packed[head, :, to] = turned.astype(jnp.bfloat16)
        packed_kv[head, :, head_width:] = value_ref[
            :, head * head_width : (head + 1) * head_width
        ]
    other = share - first
    swaps = []
    for j in range(share):
        swaps += [
            remote(
                packed_q.at[other + j],
                own_q.at[j, core],
                swap_send.at[0, j],
                swap_recv.at[0, j],
                partner,
            ),
            remote(
                packed_kv.at[other + j],
                own_kv.at[j, core],
                swap_send.at[1, j],
                swap_recv.at[1, j],
                partner,
            ),
        ]
    keeps = []
    for j in range(share):
        keeps += [
            pltpu.make_async_copy(packed_q.at[first + j], own_q.at[j, core], local_sem.at[3 + j]),
            pltpu.make_async_copy(
                packed_kv.at[first + j], own_kv.at[j, core], local_sem.at[3 + share + j]
            ),
        ]
    for copy in swaps + keeps:
        copy.start()

    def lift(side):
        return remote(
            packed_kv.at[side * share],
            below_kv.at[0, core],
            below_send.at[side],
            below_recv.at[core],
            {"ep": lax.rem(ep - core + 2 + side, n_ep)},
        )

    def lift_far(side):
        return remote(
            packed_kv.at[side * share + 1],
            lower_kv.at[0, 2 * lax.rem(z, middle) + core],
            lower_send.at[side],
            lower_recv.at[2 * lax.rem(z, middle) + core],
            {"ep": 2 * middle + side},
        )

    def ask(side, j):
        return remote(
            packed_q.at[side * share + j],
            upper_q.at[seat[j], core],
            upper_send.at[side, j],
            upper_recv.at[seat[j], core],
            {"ep": 2 * host[j] + side},
        )

    def wait_landed(ref, sem):
        pltpu.make_async_copy(ref, ref, sem).wait()

    def leave():
        for j in range(share):
            for side in range(2):

                @pl.when(asks[j])
                def _():
                    ask(side, j).start()

        for side in range(2):

            @pl.when(odd == 0)
            def _():
                lift(side).start()

        for side in range(2):

            @pl.when(z < middle)
            def _():
                lift_far(side).start()

    spread = []
    with jax.named_scope("wait_disp"):
        for d in range(n_ep):
            if d == 5:
                leave()
            if d == 0:
                dispatch[0].wait()
            else:
                dispatch[d].wait_recv()
            slot = gathered.at[tp, d]
            for way, device in enumerate((across, along)):
                copy = remote(
                    slot, slot, gath_send.at[way, d], gath_recv.at[way, d], {"tp": device}
                )
                copy.start()
                spread.append(copy)

    row = lax.broadcasted_iota(jnp.int32, (row_count, row_count), 0)
    column = lax.broadcasted_iota(jnp.int32, (row_count, row_count), 1)
    causal = column <= row
    wide = lax.broadcasted_iota(jnp.int32, (row_count, 2 * row_count), 0) + row_count
    wide_causal = lax.broadcasted_iota(jnp.int32, (row_count, 2 * row_count), 1) <= wide
    diagonal = column == row
    scale = half ** (-0.5)
    stat_row = lax.broadcasted_iota(jnp.int32, (8, row_count), 0)

    def as_column(values):
        return jnp.sum(jnp.where(diagonal, values, 0.0), axis=1, keepdims=True)

    def as_row(values):
        return jnp.sum(jnp.where(diagonal, values, 0.0), axis=0, keepdims=True)

    def as_stats(levels):
        return jnp.where(stat_row == 0, as_row(levels[0]), as_row(levels[1]))

    def head_weight(j):
        lanes = lax.broadcasted_iota(jnp.int32, lambda_ref.shape, 1)
        return jnp.sum(
            jnp.where(lanes == first + j, lambda_ref[...], 0.0), axis=1, keepdims=True
        )

    def fold(query_of, pieces, m):
        scores = []
        for keys_of, values_of, mask in pieces:
            piece = lax.dot_general(
                query_of(m), keys_of(m), (((1,), (1,)), ((), ())), preferred_element_type=jnp.float32
            )
            piece = piece * scale
            if mask is not None:
                piece = jnp.where(mask, piece, -1e30)
            scores.append(piece)
        peak = functools.reduce(
            jnp.maximum, [jnp.max(piece, axis=1, keepdims=True) for piece in scores]
        )
        total = jnp.zeros((row_count, 1), jnp.float32)
        outcome = jnp.zeros((row_count, head_width), jnp.float32)
        for piece, (keys_of, values_of, mask) in zip(scores, pieces):
            expd = jnp.exp(piece - peak)
            total += jnp.sum(expd, axis=1, keepdims=True)
            outcome += jnp.dot(
                expd.astype(jnp.bfloat16), values_of(), preferred_element_type=jnp.float32
            )
        return peak, total, outcome

    def piece_of(ref, j, count, mask):
        def keys_of(m):
            keys = ref[j, :count, :, m * half : (m + 1) * half]
            return keys.reshape(count * row_count, half)

        def values_of():
            return ref[j, :count, :, head_width:].reshape(count * row_count, head_width)

        return keys_of, values_of, mask

    def keep_diff(j, block, difference):
        @pl.when(core == block)
        def _():
            own_diff[first + j] = difference.astype(jnp.bfloat16)

        @pl.when(core != block)
        def _():
            own_part[j] = difference.astype(jnp.bfloat16)
            send_diff(j).start()

    def send_diff(j):
        return remote(
            own_part.at[j], own_diff.at[first + j], diff_send.at[j], diff_recv.at[first + j], partner
        )

    def send_stat(j):
        return remote(
            own_stat.at[j],
            upper_stat.at[seat[j]],
            stat_send.at[j],
            stat_recv.at[seat[j]],
            {"ep": 2 * host[j] + core},
        )

    def wait_own(j):
        swaps[2 * j].wait_recv()
        swaps[2 * j + 1].wait_recv()
        keeps[2 * j].wait()
        keeps[2 * j + 1].wait()

    def local_head(j, pieces):
        for block in range(2):
            mask = wide_causal if block else causal
            parts = pieces + [piece_of(own_kv, j, block + 1, mask)]
            maps, levels = [], []
            for m in range(2):
                peak, total, outcome = fold(
                    lambda m: own_q[j, block, :, m * half : (m + 1) * half], parts, m
                )
                maps.append(outcome / total)
                levels.append(peak + jnp.log(total))

            @pl.when(asks[j])
            def _():
                own_maps[j, block, 0] = maps[0]
                own_maps[j, block, 1] = maps[1]
                own_stat[j, block] = as_stats(levels)

            @pl.when(jnp.logical_not(asks[j]))
            def _():
                keep_diff(j, block, maps[0] - head_weight(j) * maps[1])

        @pl.when(asks[j])
        def _():
            send_stat(j).start()

    def send_cross(up, j, block, target):
        return remote(
            low_part.at[up, block],
            low_diff.at[first + j],
            cross_send.at[up, block],
            cross_recv.at[first + j],
            {"ep": 2 * target + block},
        )

    def send_back(up, j, block, target):
        return remote(
            low_stat.at[up, block],
            back_stat.at[j, block],
            back_send.at[up, block],
            back_recv.at[j, block],
            {"ep": 2 * target + core},
        )

    def cross_head(j, count, base, pieces):
        def step(index, carry):
            up, block = index // 2, lax.rem(index, 2)
            target = base + up
            wait_landed(upper_q.at[up, block], upper_recv.at[up, block])

            @pl.when(block == 0)
            def _():
                wait_landed(upper_stat.at[up], stat_recv.at[up])

            maps, levels = [], []
            for m in range(2):
                peak, total, outcome = fold(
                    lambda m: upper_q[up, block, :, m * half : (m + 1) * half], pieces, m
                )
                level = peak + jnp.log(total)
                above = as_column(upper_stat[up, block, m : m + 1, :])
                whole = jnp.maximum(level, above) + jnp.log(1.0 + jnp.exp(-jnp.abs(level - above)))
                maps.append(outcome * jnp.exp(peak - whole))
                levels.append(level)
            low_stat[up, block] = as_stats(levels)
            send_back(up, j, block, target).start()
            low_part[up, block] = (maps[0] - head_weight(j) * maps[1]).astype(jnp.bfloat16)
            send_cross(up, j, block, target).start()
            return carry

        lax.fori_loop(0, 2 * count, step, 0)

    def finish_upper(j):
        for block in range(2):
            wait_landed(back_stat.at[j, block], back_recv.at[j, block])
            maps = []
            for m in range(2):
                below = as_column(back_stat[j, block, m : m + 1, :])
                level = as_column(own_stat[j, block, m : m + 1, :])
                maps.append(own_maps[j, block, m] / (1.0 + jnp.exp(below - level)))
            keep_diff(j, block, maps[0] - head_weight(j) * maps[1])

    below_piece = piece_of(below_kv, 0, 2, None)
    lower_piece = piece_of(lower_kv, 0, 2 * middle, None)

    @pl.when(z != middle)
    def _():
        with jax.named_scope("own1"):
            wait_own(1)
            local_head(1, [])

    @pl.when(odd == 0)
    def _():
        with jax.named_scope("own0"):
            wait_own(0)
            local_head(0, [])

    with jax.named_scope("forward"):
        for d in range(n_ep):
            way = d % 2
            slot = gathered.at[(across, along)[way], d]
            wait_landed(slot, gath_recv.at[way, d])
            copy = remote(
                slot, slot, gath_send.at[2, d], gath_recv.at[2, d], {"tp": (along, across)[way]}
            )
            copy.start()
            spread.append(copy)
    tile = 256
    part_count = n_ep // 2
    part_rows = part_count * capacity
    scatter = []
    for part in range(2):
        lead = part * part_count
        with jax.named_scope(f"wait_gath#p={part}"):
            for d in range(lead, lead + part_count):
                way = 1 - d % 2
                wait_landed(gathered.at[(across, along)[way], d], gath_recv.at[way, d])
                wait_landed(gathered.at[corner, d], gath_recv.at[2, d])
        if part == 0:
            weights[0].wait()
            weights[1].wait()

        def hidden_tile(j, carry):
            columns = pl.ds(pl.multiple_of(j * tile, tile), tile)
            gate = jnp.zeros((part_rows, tile), jnp.float32)
            up = jnp.zeros((part_rows, tile), jnp.float32)
            for i in range(n_tp):
                block = gathered[i, lead : lead + part_count].reshape(part_rows, width)
                gate += jnp.dot(
                    block,
                    gate_vmem[0, i * width : (i + 1) * width, columns],
                    preferred_element_type=jnp.float32,
                )
                up += jnp.dot(
                    block,
                    up_vmem[0, i * width : (i + 1) * width, columns],
                    preferred_element_type=jnp.float32,
                )
            hidden[part, :, columns] = (gate / (1.0 + jnp.exp(-gate)) * up).astype(jnp.bfloat16)
            return carry

        with jax.named_scope(f"gateup#p={part}"):
            lax.fori_loop(0, hidden.shape[2] // tile, hidden_tile, 0)
        if part == 0:
            weights[2].wait()
        with jax.named_scope(f"down#p={part}"):
            for d in list(range(1, n_tp)) + [0]:
                target = lax.rem(tp + d, n_tp)
                columns = pl.ds(pl.multiple_of(target * width, width), width)
                partial[part, d] = jnp.dot(
                    hidden[part], down_vmem[0, :, columns], preferred_element_type=jnp.float32
                ).astype(jnp.bfloat16)
                if d:
                    copy = remote(
                        partial.at[part, d],
                        arrived.at[part, d],
                        part_send.at[part, d],
                        part_recv.at[part, d],
                        {"tp": target},
                    )
                    copy.start()
                    scatter.append(copy)

    @pl.when(odd == 1)
    def _():
        with jax.named_scope("odd0"):
            for source in range(2):
                wait_landed(below_kv.at[0, source], below_recv.at[source])
            wait_own(0)
            local_head(0, [below_piece])

    @pl.when(z == 0)
    def _():
        with jax.named_scope("cross0"):
            cross_head(1, 1, 1, [piece_of(own_kv, 1, 2, None)])

    @pl.when(z == middle - 1)
    def _():
        with jax.named_scope("cross1"):
            cross_head(0, middle, middle, [below_piece, piece_of(own_kv, 0, 2, None)])

    def project():
        with jax.named_scope("wait_heads"):
            for j in range(share):
                wait_landed(own_diff.at[other + j], diff_recv.at[other + j])

                @pl.when(asks[j])
                def _():
                    for side in range(2):
                        at = side * share + j
                        wait_landed(low_diff.at[at], cross_recv.at[at])

        for head in range(head_count):
            difference = own_diff[head].astype(jnp.float32) + low_diff[head].astype(jnp.float32)
            mean = jnp.mean(difference * difference, axis=1, keepdims=True)
            heads[head] = (difference * lax.rsqrt(mean + norm_eps) * gain_ref[...]).astype(
                jnp.bfloat16
            )
        weights[3].wait()
        for role, target in ((3, corner), (1, across), (2, along), (0, tp)):
            columns = pl.ds(pl.multiple_of(target * width, width), width)
            product = jnp.zeros((row_count, width), jnp.float32)
            for h in range(head_count):
                product += jnp.dot(
                    heads[h],
                    weight_vmem[h * head_width : (h + 1) * head_width, columns],
                    preferred_element_type=jnp.float32,
                )
            mixed_partial[role] = product.astype(jnp.bfloat16).reshape(
                2, row_count // 2, width
            )
            for part in range(2):
                if role == 3:
                    mixed_copy(1, part).start()
                elif role == 1 + part:
                    mixed_copy(0, part).start()

    ways = (across, along)

    def mixed_copy(kind, part):
        return remote(
            (mixed_partial.at[1 + part, part], mixed_partial.at[3, part], mixed_sum.at[part])[kind],
            mixed_arrived.at[kind, part],
            mixed_send.at[kind, part],
            mixed_recv.at[kind, part],
            {"tp": ways[1 - part if kind == 2 else part]},
        )

    def mixed_forward():
        with jax.named_scope("mixed_forward"):
            for part in range(2):
                mixed_copy(1, part).wait_recv()
                both = mixed_partial[2 - part, part].astype(jnp.float32)
                both += mixed_arrived[1, part].astype(jnp.float32)
                mixed_sum[part] = both.astype(jnp.bfloat16)
                mixed_copy(2, part).start()

    back = []
    for d in range(n_ep):
        if d == 0:
            copy = pltpu.make_async_copy(summed.at[0], returned.at[ep], local_sem.at[2])
        else:
            copy = remote(
                summed.at[d],
                returned.at[ep],
                ret_send.at[d],
                ret_recv.at[d],
                {"ep": lax.rem(ep + n_ep - d, n_ep)},
            )
        back.append(copy)

    def sum_part(part):
        lead = part * part_count
        total = partial[part, 0].astype(jnp.float32)
        with jax.named_scope(f"wait_part#p={part}"):
            for d in range(1, n_tp):
                scatter[part * (n_tp - 1) + d - 1].wait_recv()
                total += arrived[part, d].astype(jnp.float32)
        summed[lead : lead + part_count] = total.astype(jnp.bfloat16).reshape(
            part_count, capacity, width
        )

    for j in range(share):

        @pl.when(jnp.logical_not(asks[j]))
        def _():
            for side in range(2):
                low_diff[side * share + j] = jnp.zeros((row_count, head_width), jnp.bfloat16)

    @pl.when(z == middle - 1)
    def _():
        with jax.named_scope("finish"):
            finish_upper(1)

    @pl.when(z < middle)
    def _():
        with jax.named_scope("project_low"):
            project()

    sum_part(0)

    @pl.when(z < middle)
    def _():
        mixed_forward()

    @pl.when(z >= middle)
    def _():
        for copy in back[:part_count]:
            copy.start()

    @pl.when(z == middle)
    def _():
        with jax.named_scope("cross2"):
            for source in range(2 * middle):
                wait_landed(lower_kv.at[0, source], lower_recv.at[source])
            wait_own(1)
            cross_head(1, 1, middle + 1, [lower_piece, piece_of(own_kv, 1, 2, None)])
            local_head(1, [lower_piece])

    sum_part(1)

    def release(steps):
        pl.semaphore_signal(
            hold_sem,
            inc=1,
            device_id={"ep": lax.rem(ep + n_ep - 2 * steps, n_ep)},
            device_id_type=MESH,
        )

    @pl.when(z < middle)
    def _():
        targets = [lax.rem(ep + n_ep - d, n_ep) for d in range(n_ep)]
        for target, copy in zip(targets, back):

            @pl.when(target < 2 * middle)
            def _():
                copy.start()

        with jax.named_scope("hold"):

            @pl.when(z == middle - 1)
            def _():
                for up in range(middle):
                    for side in range(2):
                        send_cross(up, 0, side, middle + up).wait_send()
                release(1)
                pl.semaphore_wait(hold_sem, 1)

            @pl.when(z != middle - 1)
            def _():
                pl.semaphore_wait(hold_sem, 2)

        for target, copy in zip(targets, back):

            @pl.when(target >= 2 * middle)
            def _():
                copy.start()

    @pl.when(z >= middle)
    def _():
        @pl.when(z != middle)
        def _():
            for copy in back[part_count:]:
                copy.start()

        with jax.named_scope("finish"):
            finish_upper(0)

        @pl.when(odd == 1)
        def _():
            with jax.named_scope("finish"):
                finish_upper(1)

        with jax.named_scope("project_up"):
            project()

        @pl.when(z == middle)
        def _():
            with jax.named_scope("held"):
                for side in range(2):
                    send_cross(0, 1, side, middle + 1).wait_send()
            release(1)
            release(2)
            for copy in back[part_count:]:
                copy.start()

        mixed_forward()

    with jax.named_scope("wait_back"):
        back[0].wait()
        for copy in back[1:]:
            copy.wait_recv()
    flat = returned[...].reshape(rows, width)
    result = jnp.zeros(expert_ref.shape, jnp.float32)
    for k in range(picks):
        picked = lax.dot_general(
            select[k].astype(jnp.bfloat16),
            flat,
            (((0,), (0,)), ((), ())),
            preferred_element_type=jnp.float32,
        )
        spread_out = jnp.where(before == after, route_weights_ref[k : k + 1, :], 0.0)
        result += jnp.sum(spread_out, axis=1, keepdims=True) * picked
    expert_ref[...] = result.astype(expert_ref.dtype)
    with jax.named_scope("wait_mixed"):
        for part in range(2):
            total = mixed_partial[0, part].astype(jnp.float32)
            for kind in (0, 2):
                mixed_copy(kind, part).wait_recv()
                total += mixed_arrived[kind, part].astype(jnp.float32)
            lines = slice(part * row_count // 2, (part + 1) * row_count // 2)
            mixed_ref[lines, :] = total.astype(jnp.bfloat16)
    for copy in dispatch[1:] + swaps + spread + scatter + back[1:]:
        copy.wait_send()
    for kind in range(3):
        for part in range(2):
            mixed_copy(kind, part).wait_send()
    for j in range(share):
        send_diff(j).wait_send()

        @pl.when(asks[j])
        def _():
            send_stat(j).wait_send()
            for side in range(2):
                ask(side, j).wait_send()

    for side in range(2):

        @pl.when(odd == 0)
        def _():
            lift(side).wait_send()

        @pl.when(z < middle)
        def _():
            lift_far(side).wait_send()

        @pl.when(z <= middle)
        def _():
            send_back(0, 0, side, z + 1).wait_send()

            @pl.when(z < middle - 1)
            def _():
                send_cross(0, 0, side, z + 1).wait_send()

        @pl.when(z == middle - 1)
        def _():
            send_back(1, 0, side, z + 2).wait_send()


def hand_over(expert_ref, mixed_ref, expert_out, mixed_out):
    expert_out[...] = expert_ref[...]
    mixed_out[...] = mixed_ref[...]


def fused(
    query_maps,
    key_maps,
    value_rows,
    head_lambda,
    head_gain,
    out_weight,
    expert_rows,
    expert_gain,
    routes,
    route_weights,
    gate_weight,
    up_weight,
    down_weight,
):
    n_ep = lax.axis_size("ep")
    n_tp = lax.axis_size("tp")
    n_z = n_ep // 2
    row_count = query_maps.shape[0]
    head_width = query_maps.shape[1] // n_z
    head_dim = head_width // 2
    token_count, model_width = expert_rows.shape
    capacity = 3 * token_count * routes.shape[1] // (2 * n_ep)
    width = model_width // n_tp
    hidden_width = gate_weight.shape[2]
    slot_rows = n_ep * capacity

    half_dim = head_dim // 2
    inverse = rope_base ** (-2.0 * np.arange(half_dim) / head_dim)
    inverse = np.concatenate([inverse, inverse])
    turns = np.arange(row_count)[:, None] * inverse
    offsets = (row_count * np.arange(n_ep))[:, None] * inverse
    turns = jnp.asarray(np.stack([np.cos(turns), np.sin(turns)]), jnp.float32)
    offsets = jnp.asarray(np.stack([np.cos(offsets), np.sin(offsets)]), jnp.float32)

    vmem = pl.BlockSpec(memory_space=pltpu.VMEM)
    hbm = pl.BlockSpec(memory_space=pl.ANY)
    dma = pltpu.SemaphoreType.DMA
    bf16, f32 = jnp.bfloat16, jnp.float32
    share = n_z // 2
    expert_out, mixed = pl.pallas_call(
        functools.partial(layer_kernel, n_ep, n_tp),
        out_shape=(
            jax.ShapeDtypeStruct((token_count, width), bf16),
            jax.ShapeDtypeStruct((row_count, width), bf16),
        ),
        in_specs=[vmem] * 6 + [hbm] * 9,
        out_specs=(vmem, vmem),
        scratch_shapes=[
            pltpu.VMEM(expert_rows.shape, bf16),
            pltpu.VMEM(query_maps.shape, bf16),
            pltpu.VMEM(key_maps.shape, bf16),
            pltpu.VMEM(value_rows.shape, bf16),
            pltpu.VMEM(turns.shape, f32),
            pltpu.VMEM((n_ep, capacity, width), bf16),
            pltpu.VMEM((n_z, row_count, head_width), bf16),
            pltpu.VMEM((n_z, row_count, 2 * head_width), bf16),
            pltpu.VMEM((share, 2, row_count, head_width), bf16),
            pltpu.VMEM((share, 2, row_count, 2 * head_width), bf16),
            pltpu.VMEM((1, 2, row_count, 2 * head_width), bf16),
            pltpu.VMEM((1, n_z, row_count, 2 * head_width), bf16),
            pltpu.VMEM((share, 2, row_count, head_width), bf16),
            pltpu.VMEM((share, 2, 8, row_count), f32),
            pltpu.VMEM((share, 2, 8, row_count), f32),
            pltpu.VMEM((share, 2, 8, row_count), f32),
            pltpu.VMEM((share, 2, 8, row_count), f32),
            pltpu.VMEM((share, 2, 2, row_count, head_width), f32),
            pltpu.VMEM((share, row_count, head_width), bf16),
            pltpu.VMEM((n_z, row_count, head_width), bf16),
            pltpu.VMEM((share, 2, row_count, head_width), bf16),
            pltpu.VMEM((n_z, row_count, head_width), bf16),
            pltpu.VMEM((n_tp, n_ep, capacity, width), bf16),
            pltpu.VMEM(gate_weight.shape, bf16),
            pltpu.VMEM(up_weight.shape, bf16),
            pltpu.VMEM(down_weight.shape, bf16),
            pltpu.VMEM((2, slot_rows // 2, hidden_width), bf16),
            pltpu.VMEM((2, n_tp, slot_rows // 2, width), bf16),
            pltpu.VMEM((2, n_tp, slot_rows // 2, width), bf16),
            pltpu.VMEM((n_ep, capacity, width), bf16),
            pltpu.VMEM((n_ep, capacity, width), bf16),
            pltpu.VMEM(out_weight.shape, bf16),
            pltpu.VMEM((n_z, row_count, head_width), bf16),
            pltpu.VMEM((n_tp, 2, row_count // 2, width), bf16),
            pltpu.VMEM((3, 2, row_count // 2, width), bf16),
            pltpu.VMEM((2, row_count // 2, width), bf16),
            dma((5,)),
            dma((4,)),
            dma((3 + n_z,)),
            dma((n_ep,)),
            dma((n_ep,)),
            dma((3, n_ep)),
            dma((3, n_ep)),
            dma((2, n_tp)),
            dma((2, n_tp)),
            dma((n_ep,)),
            dma((n_ep,)),
            dma((2, share)),
            dma((2, share)),
            dma((2,)),
            dma((2,)),
            dma((2,)),
            dma((n_z,)),
            dma((2, share)),
            dma((share, 2)),
            dma((share,)),
            dma((share,)),
            dma((share, 2)),
            dma((share, 2)),
            dma((share,)),
            dma((n_z,)),
            dma((share, 2)),
            dma((n_z,)),
            dma((3, 2)),
            dma((3, 2)),
            pltpu.SemaphoreType.REGULAR,
        ],
        compiler_params=pltpu.CompilerParams(
            collective_id=0, has_side_effects=True, vmem_limit_bytes=60 * 1024 * 1024
        ),
        name="layer",
    )(
        expert_gain.reshape(1, model_width),
        routes.T,
        route_weights.T,
        offsets,
        head_lambda.reshape(1, n_z),
        head_gain.reshape(1, head_width),
        expert_rows,
        query_maps,
        key_maps,
        value_rows,
        turns,
        gate_weight,
        up_weight,
        down_weight,
        out_weight,
    )
    expert_out, mixed = pl.pallas_call(
        hand_over,
        out_shape=(
            jax.ShapeDtypeStruct((token_count, width), bf16),
            jax.ShapeDtypeStruct((row_count, width), bf16),
        ),
        in_specs=[vmem] * 2,
        out_specs=(vmem, vmem),
        name="hand_over",
    )(expert_out, mixed)
    return (mixed, expert_out)


def on_device(
    query_maps,
    key_maps,
    value_rows,
    head_lambda,
    head_gain,
    out_weight,
    expert_rows,
    expert_gain,
    routes,
    route_weights,
    gate_weight,
    up_weight,
    down_weight,
):
    n_ep = lax.axis_size("ep")
    head_count = head_lambda.shape[0]
    capacity = 3 * expert_rows.shape[0] * routes.shape[1] // (2 * n_ep)
    if (
        2 * head_count == n_ep
        and head_count == lax.axis_size("tp") == 4
        and capacity % 16 == 0
        and value_rows.shape[1] == query_maps.shape[1] == 256 * head_count
    ):
        return fused(
            query_maps,
            key_maps,
            value_rows,
            head_lambda,
            head_gain,
            out_weight,
            expert_rows,
            expert_gain,
            routes,
            route_weights,
            gate_weight,
            up_weight,
            down_weight,
        )
    mixed = mixer_half(query_maps, key_maps, value_rows, head_lambda, head_gain, out_weight)
    expert_out = expert_half(
        expert_rows, expert_gain, routes, route_weights, gate_weight, up_weight, down_weight
    )
    return (mixed, expert_out)


def solution(mesh):
    placed = (
        P("ep", "tp"),
        P("ep", "tp"),
        P("ep", "tp"),
        P("tp"),
        P(),
        P("tp", None),
        P("ep", None),
        P(),
        P("ep", None),
        P("ep", None),
        P("ep", None, "tp"),
        P("ep", None, "tp"),
        P("ep", "tp", None),
    )
    return jax.shard_map(
        on_device,
        mesh=mesh,
        in_specs=placed,
        out_specs=(P("ep", "tp"), P("ep", "tp")),
        check_vma=False,
    )
```
